256 devices in a mesh: sp: 32 (over z, y), fs: 4 (over x), tp: 2 (over core).
Axes of the slice: x: 4, y: 4, z: 8, core: 2. Of those that a mesh axis runs over, the one named last changes fastest.
Arguments:
- tokens: bfloat16 [4, 4096, 2048], P('fs', ('sp', 'tp')), may hold values from -6 to 6
- norm_gain: float32 [2048], replicated, may hold values from 0.1 to 1.9
- drive_weight: bfloat16 [2048, 1024], P('fs', 'tp'), may hold values from -0.125 to 0.125
- query_weight: bfloat16 [2048, 1024], P('fs', 'tp'), may hold values from -1 to 1
- key_weight: bfloat16 [2048, 1024], P('fs', 'tp'), may hold values from -1 to 1
- value_weight: bfloat16 [2048, 1024], P('fs', 'tp'), may hold values from -0.5 to 0.5
- key_offset: bfloat16 [8, 4, 4096], P('tp', 'fs', 'sp'), may hold values from -16 to 0
- log_step: float32 [64], P('tp'), may hold values from -4.7 to -1.2
- lambda_real: float32 [64, 64], P('tp'), as said below
- lambda_imag: float32 [64, 64], P('tp'), may hold values from 1 to 201
- input_map: float32 [2, 64, 64, 16], P(None, 'tp'), may hold values from -2 to 2
- output_map: float32 [2, 64, 16, 64], P(None, 'tp'), may hold values from -0.5 to 0.5
- skip_gain: float32 [1024], P('tp'), may hold values from -5 to 5
- forget: float32 [64, 4, 4096], P('tp', 'fs', 'sp'), may hold values from -0.52 to 0
- initial_state: float32 [2, 4, 64, 64], P(None, 'fs', 'tp'), may hold values from -24 to 24
- scan_out_weight: bfloat16 [1024, 2048], P('tp', 'fs'), may hold values from -0.125 to 0.125
- attend_out_weight: bfloat16 [1024, 2048], P('tp', 'fs'), may hold values from -0.125 to 0.125
Outputs:
- layer_out: bfloat16 [4, 4096, 2048], P('fs', ('sp', 'tp'))
The draws below stay inside these ranges and needn't reach their ends.
Inputs may be any that keep to these rules, and one draw needn't show every extreme that they name: lambda_real[g, n] * exp(log_step[g]) lies between -1/30 and 0 for every group g and state n.
All inputs are finite; a program needn't handle non-finite values.
Results may differ from the reference program's by a relative error of at most 0.009.
Values may be sent and summed in bfloat16 or wider, within the bound.
No kernel may reach another device: no remote copies, remote signals or barrier semaphores. Data moves between devices by JAX's collectives and lax.ppermute only.
A program may use at most 128 MiB of HBM per device.

```python
import math
import jax
import jax.numpy as jnp
from jax import lax

D = 2048
BRANCH_W = 1024
HEAD_DIM = 128
HEADS = 8
GROUP_W = 16
GROUPS = 64
STATE_N = 64
TOK_DEV = 128
LENGTH = 4096
SEQUENCE_COUNT = 4
N_TP = 2


def spike_mask(key, leading_part, item_count):
    spots = jax.random.randint(key, leading_part + (item_count,), 0, LENGTH)
    places = jnp.arange(LENGTH, dtype=jnp.int32)
    return jnp.any(places[None, None, :, None] == spots[:, :, None, :], axis=-1)


def draw_tokens(key, part):
    key_sequence = jax.random.split(jax.random.fold_in(key, 11), 4)
    full_shape = (SEQUENCE_COUNT, LENGTH, D)
    noise = jnp.clip(jax.random.normal(key_sequence[0], full_shape, jnp.float32), -4.0, 4.0)
    direction = jnp.where(jax.random.bernoulli(key_sequence[1], 0.5, (SEQUENCE_COUNT, 1, D)), 1.0, -1.0)
    row_sign = jnp.where(jax.random.bernoulli(key_sequence[2], 0.5, (SEQUENCE_COUNT, LENGTH, 1)), 1.0, -1.0)
    block_total = LENGTH // TOK_DEV
    amplitude = jnp.exp(jax.random.uniform(key_sequence[3], (SEQUENCE_COUNT, block_total, 1), jnp.float32, math.log(0.15), math.log(2.0)))
    amplitude = jnp.repeat(amplitude, TOK_DEV, axis=1)
    return (noise + row_sign * amplitude * direction).astype(jnp.bfloat16)


def paired_weights(key):
    key_sequence = jax.random.split(jax.random.fold_in(key, 13), 2)
    first = jnp.clip(jax.random.normal(key_sequence[0], (D, BRANCH_W), jnp.float32), -6.0, 6.0) * D ** (-0.5)
    second = jnp.clip(jax.random.normal(key_sequence[1], (D, BRANCH_W), jnp.float32), -6.0, 6.0) * D ** (-0.5)
    return (first, 0.35 * first + 0.93675 * second)


def draw_query_weight(key, part):
    return paired_weights(key)[0].astype(jnp.bfloat16)


def draw_key_weight(key, part):
    return paired_weights(key)[1].astype(jnp.bfloat16)


def draw_key_offset(key, part):
    head_number = BRANCH_W // HEAD_DIM
    key_sequence = jax.random.split(jax.random.fold_in(key, 7), 7)
    fast_count = head_number // 2
    fast = jax.random.permutation(key_sequence[0], head_number) < fast_count
    quick_rate = jnp.exp(jax.random.uniform(key_sequence[1], (head_number,), jnp.float32, math.log(0.001), math.log(1.0 / 30.0)))
    slow_rate = jnp.exp(jax.random.uniform(key_sequence[2], (head_number,), jnp.float32, math.log(0.1), math.log(0.6))) / LENGTH
    ground_level = jnp.log(jnp.where(fast, quick_rate, slow_rate)) - 0.5
    block_total = LENGTH // TOK_DEV
    block_multiplier = jax.random.uniform(key_sequence[3], (head_number, SEQUENCE_COUNT, block_total), jnp.float32, math.log(0.5), math.log(2.0))
    block_multiplier = jnp.repeat(block_multiplier, TOK_DEV, axis=2)
    random_shake = jax.random.uniform(key_sequence[4], (head_number, SEQUENCE_COUNT, LENGTH), jnp.float32, -0.7, 0.7)
    struck_mask = spike_mask(key_sequence[5], (head_number, SEQUENCE_COUNT), 3)
    share_fraction = jax.random.uniform(key_sequence[6], (head_number, SEQUENCE_COUNT, LENGTH), jnp.float32, 0.2, 0.4)
    spike_level = jnp.log(share_fraction / (1.0 - share_fraction))
    value_gathered_full = jnp.where(struck_mask, spike_level, ground_level[:, None, None] + block_multiplier + random_shake)
    return value_gathered_full.astype(jnp.bfloat16)


def decay_pair(key):
    group_count_total = BRANCH_W // GROUP_W
    key_sequence = jax.random.split(jax.random.fold_in(key, 3), 4)
    log_steps = jax.random.uniform(key_sequence[0], (group_count_total,), jnp.float32, math.log(0.01), math.log(0.3))
    fast_count = group_count_total // 2
    fast = jax.random.permutation(key_sequence[1], group_count_total) < fast_count
    quick_rate = jnp.exp(jax.random.uniform(key_sequence[2], (group_count_total, STATE_N), jnp.float32, math.log(0.001), math.log(1.0 / 30.0)))
    slow_rate = jnp.exp(jax.random.uniform(key_sequence[3], (group_count_total, STATE_N), jnp.float32, math.log(0.05), math.log(0.4))) / LENGTH
    rate_all = jnp.where(fast[:, None], quick_rate, slow_rate)
    return (log_steps, -rate_all / jnp.exp(log_steps)[:, None])


def draw_log_step(key, part):
    return decay_pair(key)[0]


def draw_lambda_real(key, part):
    return decay_pair(key)[1]


def draw_forget(key, part):
    group_count_total = BRANCH_W // GROUP_W
    key_sequence = jax.random.split(jax.random.fold_in(key, 5), 4)
    base_rate = jax.random.uniform(key_sequence[0], (group_count_total, SEQUENCE_COUNT, LENGTH), jnp.float32, 0.05, 0.5) / LENGTH
    block_total = LENGTH // TOK_DEV
    block_multiplier = jnp.exp(jax.random.uniform(key_sequence[1], (group_count_total, SEQUENCE_COUNT, block_total), jnp.float32, math.log(0.5), math.log(2.0)))
    block_multiplier = jnp.repeat(block_multiplier, TOK_DEV, axis=2)
    struck_mask = spike_mask(key_sequence[2], (group_count_total, SEQUENCE_COUNT), 2)
    share_fraction = jax.random.uniform(key_sequence[3], (group_count_total, SEQUENCE_COUNT, LENGTH), jnp.float32, 0.2, 0.4)
    return jnp.where(struck_mask, jnp.log1p(-share_fraction), -base_rate * block_multiplier)


def block_scale(stream_key, extent, pieces, low, largest):
    def one(axis_at, blocks):
        draws = jax.random.uniform(jax.random.fold_in(jax.random.fold_in(stream_key, 6), axis_at), (blocks,), jnp.float32, low / len(pieces), largest / len(pieces))
        return jnp.repeat(jnp.exp(draws), extent[axis_at] // blocks).reshape((-1,) + (1,) * (len(extent) - axis_at - 1))

    level = one(*pieces[0])
    for cut in pieces[1:]:
        level = level * one(*cut)
    return level


def scatter_about(key, dims, spread, bound, cuts=(), kind=jnp.bfloat16):
    level = block_scale(key, dims, cuts, -0.22, 0.18) if cuts else 1.0
    array = jax.random.normal(key, dims, jnp.float32) * spread * level
    return jnp.minimum(jnp.maximum(array, -bound), bound).astype(kind)


def setup_inputs(seed: int = 0) -> dict:
    arg_keys = jax.random.split(jax.random.key(seed), 18)
    return {
        "tokens": draw_tokens(jax.random.fold_in(arg_keys[17], 71), 0),
        "norm_gain": jnp.clip(1.0 + 0.18 * jax.random.normal(arg_keys[1], (D,), jnp.float32), 0.1, 1.9),
        "drive_weight": scatter_about(arg_keys[2], (D, BRANCH_W), D ** -0.5, 0.125, ((0, 4), (1, 2))),
        "query_weight": draw_query_weight(jax.random.fold_in(arg_keys[17], 71), 0),
        "key_weight": draw_key_weight(jax.random.fold_in(arg_keys[17], 71), 0),
        "value_weight": scatter_about(arg_keys[5], (D, BRANCH_W), (D // 16) ** -0.5, 0.5, ((0, 4), (1, 2))),
        "key_offset": draw_key_offset(jax.random.fold_in(arg_keys[17], 71), 0),
        "log_step": draw_log_step(jax.random.fold_in(arg_keys[17], 71), 0),
        "lambda_real": draw_lambda_real(jax.random.fold_in(arg_keys[17], 71), 0),
        "lambda_imag": jnp.clip(1.0 + 200.0 * jax.random.uniform(arg_keys[9], (GROUPS, STATE_N), jnp.float32) ** block_scale(arg_keys[9], (GROUPS, STATE_N), ((0, 2),), -0.2, 0.2), 1.0, 201.0),
        "input_map": scatter_about(arg_keys[10], (2, GROUPS, STATE_N, GROUP_W), (GROUP_W // 2) ** -0.5, 2.0, ((1, 2),), jnp.float32),
        "output_map": scatter_about(arg_keys[11], (2, GROUPS, GROUP_W, STATE_N), (2 * STATE_N) ** -0.5, 0.5, ((1, 2),), jnp.float32),
        "skip_gain": scatter_about(arg_keys[12], (BRANCH_W,), 1.0, 5.0, ((0, 2),), jnp.float32),
        "forget": draw_forget(jax.random.fold_in(arg_keys[17], 71), 0),
        "initial_state": scatter_about(arg_keys[14], (2, SEQUENCE_COUNT, GROUPS, STATE_N), 4.0, 24.0, ((1, 4), (2, 2)), jnp.float32),
        "scan_out_weight": scatter_about(arg_keys[15], (BRANCH_W, D), (2 * BRANCH_W) ** -0.5, 0.125, ((0, 2), (1, 4))),
        "attend_out_weight": scatter_about(arg_keys[16], (BRANCH_W, D), (2 * BRANCH_W) ** -0.5, 0.125, ((0, 2), (1, 4))),
    }


epsilon = 1e-06

def reference(tokens, norm_gain, drive_weight, query_weight, key_weight, value_weight, key_offset, log_step, lambda_real, lambda_imag, input_map, output_map, skip_gain, forget, initial_state, scan_out_weight, attend_out_weight):
    highest = lax.Precision.HIGHEST
    flat_rows = tokens.reshape(SEQUENCE_COUNT * LENGTH, D).astype(jnp.float32)
    normed = (flat_rows * lax.rsqrt(lax.optimization_barrier(jnp.mean(flat_rows * flat_rows, axis=1, keepdims=True)) + epsilon) * norm_gain[None]).astype(jnp.bfloat16)

    def project(matrix):
        return jnp.dot(normed, matrix, preferred_element_type=jnp.float32).astype(jnp.bfloat16)
    drive_rows = project(drive_weight)
    queries = project(query_weight)
    keys_all = project(key_weight)
    values_all = project(value_weight)
    step_size = jnp.exp(log_step)[:, None]
    log_gain = lambda_real * step_size
    rotate = lambda_imag * step_size
    magnitude = jnp.exp(log_gain)
    bar_real = magnitude * jnp.cos(rotate)
    bar_imag = magnitude * jnp.sin(rotate)
    divisor = lambda_real * lambda_real + lambda_imag * lambda_imag
    shifted = bar_real - 1.0
    factor_real = (shifted * lambda_real + bar_imag * lambda_imag) / divisor
    factor_imag = (bar_imag * lambda_real - shifted * lambda_imag) / divisor
    map_real = factor_real[:, :, None] * input_map[0] - factor_imag[:, :, None] * input_map[1]
    map_imag = factor_real[:, :, None] * input_map[1] + factor_imag[:, :, None] * input_map[0]
    inputs = drive_rows.astype(jnp.float32).reshape(SEQUENCE_COUNT, LENGTH, GROUPS, GROUP_W)

    def one_sequence(element):
        seq_inputs, seq_forget, seq_init = element

        def advance(running, item_pair):
            in_now, forget_now = item_pair
            keep_rate = jnp.exp(forget_now)[:, None]
            new_real = keep_rate * (bar_real * running[0] - bar_imag * running[1]) + jnp.einsum('gc,gnc->gn', in_now, map_real, precision=highest)
            new_imag = keep_rate * (bar_real * running[1] + bar_imag * running[0]) + jnp.einsum('gc,gnc->gn', in_now, map_imag, precision=highest)
            readout = jnp.einsum('gn,gcn->gc', new_real, output_map[0], precision=highest) - jnp.einsum('gn,gcn->gc', new_imag, output_map[1], precision=highest)
            return ((new_real, new_imag), readout)
        _, read_rows = lax.scan(advance, (seq_init[0], seq_init[1]), (seq_inputs, seq_forget.T))
        return read_rows
    readouts = lax.map(one_sequence, (inputs, jnp.transpose(forget, (1, 0, 2)), jnp.transpose(initial_state, (1, 0, 2, 3))))
    readouts = readouts + skip_gain.reshape(GROUPS, GROUP_W)[None, None] * inputs
    scan_out = jax.nn.gelu(readouts).reshape(SEQUENCE_COUNT * LENGTH, BRANCH_W).astype(jnp.bfloat16)
    blocks = LENGTH // TOK_DEV
    shape_five = (SEQUENCE_COUNT, blocks, TOK_DEV, HEADS, HEAD_DIM)
    query_five = queries.reshape(shape_five)
    key_five = keys_all.reshape(shape_five)
    value_five = values_all.reshape(shape_five)
    offset_four = key_offset.reshape(HEADS, SEQUENCE_COUNT, blocks, TOK_DEV)
    ladder = jnp.arange(TOK_DEV, dtype=jnp.int32)

    def one_block(item_index):
        seq_id = item_index // blocks
        block_id = item_index % blocks
        query_block = query_five[seq_id, block_id].astype(jnp.float32)
        query_place = block_id * TOK_DEV + ladder

        def turn(distance, running):
            summed_now, fallen = running
            source = block_id - distance
            key_block = key_five[seq_id, source].astype(jnp.float32)
            value_block = value_five[seq_id, source].astype(jnp.float32)
            offset_block = offset_four[:, seq_id, source].astype(jnp.float32)
            scores = jnp.einsum('qhd,khd->qhk', query_block, key_block) * HEAD_DIM ** (-0.5) + offset_block[None]
            key_place = source * TOK_DEV + ladder
            visible = key_place[None, None, :] < query_place[:, None, None]
            escape_log = jnp.where(visible, jax.nn.log_sigmoid(-scores), 0.0)
            behind_log = lax.cumsum(escape_log, axis=2, reverse=True) - escape_log
            weight = jnp.where(visible, jnp.exp(jax.nn.log_sigmoid(scores) + behind_log), 0.0)
            weight = lax.optimization_barrier(weight.astype(jnp.bfloat16)).astype(jnp.float32)
            portion = jnp.einsum('qhk,khd->qhd', weight, value_block)
            return (summed_now + jnp.exp(fallen)[:, :, None] * portion, fallen + lax.optimization_barrier(jnp.sum(escape_log, axis=2)))
        empty_state = (jnp.zeros((TOK_DEV, HEADS, HEAD_DIM), jnp.float32), jnp.zeros((TOK_DEV, HEADS), jnp.float32))
        result_now, _ = lax.fori_loop(0, block_id + 1, turn, empty_state)
        return result_now.astype(jnp.bfloat16)
    attended = lax.map(one_block, jnp.arange(SEQUENCE_COUNT * blocks, dtype=jnp.int32))
    attend_out = attended.reshape(SEQUENCE_COUNT * LENGTH, BRANCH_W)
    share_width = BRANCH_W // N_TP
    summed = jnp.zeros((SEQUENCE_COUNT * LENGTH, D), jnp.float32)
    for part_index in range(N_TP):
        column_low = part_index * share_width
        column_high = column_low + share_width
        partial_value = jnp.dot(scan_out[:, column_low:column_high], scan_out_weight[column_low:column_high], preferred_element_type=jnp.float32)
        partial_value = partial_value + jnp.dot(attend_out[:, column_low:column_high], attend_out_weight[column_low:column_high], preferred_element_type=jnp.float32)
        rounded = lax.optimization_barrier(partial_value.astype(jnp.bfloat16))
        summed = summed + rounded.astype(jnp.float32)
    return summed.astype(jnp.bfloat16).reshape(SEQUENCE_COUNT, LENGTH, D)
```

```python
import math

import jax
import jax.numpy as jnp
from jax import lax
from jax.experimental import pallas as pl
from jax.experimental.pallas import tpu as pltpu
from jax.sharding import Mesh
from jax.sharding import PartitionSpec as P

HEAD_DIM = 128
BLOCK = 128
ROWS = 512
EXTRA = 16
SP = ("z", "y")
SP_TP = ("z", "y", "c")
LOG2E = 1.4426950408889634
SCORE = HEAD_DIM ** (-0.5) * LOG2E
epsilon = 1e-06
f32 = jnp.float32
bf16 = jnp.bfloat16
INTERPRET = False


def vmem(n):
    return [pl.BlockSpec(memory_space=pltpu.VMEM)] * n


def smem(n):
    return [pl.BlockSpec(memory_space=pltpu.SMEM)] * n


def call(body, out_shape, n_scalar, n_in, scratch=(), flops=0, name=None):
    many = isinstance(out_shape, (list, tuple))
    return pl.pallas_call(
        body,
        out_shape=out_shape,
        in_specs=smem(n_scalar) + vmem(n_in),
        out_specs=vmem(len(out_shape)) if many else vmem(1)[0],
        scratch_shapes=list(scratch),
        cost_estimate=pl.CostEstimate(flops=flops, transcendentals=0, bytes_accessed=1 << 20),
        compiler_params=pltpu.CompilerParams(vmem_limit_bytes=48 << 20),
        interpret=INTERPRET,
        name=name,
    )


def shape(dims, dtype):
    return jax.ShapeDtypeStruct(dims, dtype)


def split2(v):
    hi = v.astype(bf16)
    return hi, (v - hi.astype(f32)).astype(bf16)


def mm(a, b):
    return jnp.dot(a, b, preferred_element_type=f32)


def norm_body(tok_ref, gain_ref, forget_ref, off_ref, out_ref):
    v = tok_ref[...].astype(f32)
    scale = lax.rsqrt(jnp.mean(v * v, axis=1, keepdims=True) + epsilon)
    out_ref[EXTRA:, :] = (v * scale * gain_ref[...]).astype(bf16)
    hi, lo = split2(forget_ref[...])
    hi, lo = hi.astype(f32), lo.astype(f32)
    off = off_ref[...].astype(f32)
    blank = jnp.zeros((11, BLOCK), f32)
    for j in range(16):
        last = off[j : j + 1] if j < 4 else jnp.zeros((1, BLOCK), f32)
        tile = jnp.concatenate(
            [hi[j : j + 1], hi[16 + j : 17 + j], lo[j : j + 1], lo[16 + j : 17 + j], last, blank], axis=0
        )
        out_ref[:EXTRA, j * BLOCK : (j + 1) * BLOCK] = tile.astype(bf16)


def normalize(tokens, gain, forget, offset):
    return call(norm_body, shape((EXTRA + 64, 2048), bf16), 0, 4, flops=10**6, name="norm")(
        tokens, gain.reshape(1, -1), forget, offset
    )


def weight_rows(x, w_all, own, up, down, far0, far1):
    half = far0.shape[0]
    w_all[pl.ds(pl.multiple_of(x * ROWS, ROWS), ROWS), :] = own[...]
    w_all[pl.ds(pl.multiple_of(((x + 3) % 4) * ROWS, ROWS), ROWS), :] = up[...]
    w_all[pl.ds(pl.multiple_of(((x + 1) % 4) * ROWS, ROWS), ROWS), :] = down[...]
    far = pl.multiple_of(((x + 2) % 4) * ROWS, ROWS)
    w_all[pl.ds(far, half), :] = far0[...]
    w_all[pl.ds(far + half, half), :] = far1[...]


def kv_body(where, *refs):
    pieces, weights = refs[:10], refs[10:15]
    rows_ref, kv_ref, forget_ref, w_all = refs[15:]
    x, y, c = where[0], where[1], where[2]
    kv_ref[ROWS:, :] = jnp.zeros((EXTRA, 256), bf16)
    offs = [None] * 4
    for part in range(2):
        own, up, down, far0, far1 = pieces[part * 5 : part * 5 + 5]
        core = (c + part) % 2
        for piece, step in ((own, 0), (up, 3), (down, 1)):
            at = pl.multiple_of(((y + step) % 4) * BLOCK + core * 64, 64)
            rows_ref[pl.ds(at, 64), :] = piece[EXTRA:, :]
        at = pl.multiple_of(((y + 2) % 4) * BLOCK + core * 64, 64)
        rows_ref[pl.ds(at, 32), :] = far0[EXTRA:, :]
        rows_ref[pl.ds(at + 32, 32), :] = far1[...]
    own, up, down, far0 = pieces[:4]
    high = y // 2
    lane = pl.multiple_of((y % 2) * 8 * BLOCK, 8 * BLOCK)
    for piece, step in ((own, 0), (up, 3), (down, 1), (far0, 2)):
        block = (y + step) % 4
        tile = piece[:EXTRA, pl.ds(lane, 8 * BLOCK)].astype(f32)
        row = jnp.where(high == 1, tile[1:2] + tile[3:4], tile[0:1] + tile[2:3])
        rows8 = jnp.concatenate([row[:, g * BLOCK : (g + 1) * BLOCK] for g in range(8)], axis=0)
        forget_ref[:, pl.ds(pl.multiple_of(block * BLOCK, BLOCK), BLOCK)] = rows8
        off = piece[:EXTRA, pl.ds(pl.multiple_of(y * BLOCK, BLOCK), BLOCK)].astype(f32)[4:5]
        offs = [off if o is None else jnp.where(block == k, off, o) for k, o in enumerate(offs)]
    row0 = jnp.concatenate(offs[:2], axis=1)
    row1 = jnp.concatenate(offs[2:], axis=1)
    tail = jnp.concatenate([row0, row1, jnp.zeros((EXTRA - 2, 256), f32)], axis=0)
    kv_ref[ROWS:, :] = tail.astype(bf16)
    weight_rows(x, w_all, *weights)
    kv_ref[:ROWS, :] = mm(rows_ref[...], w_all[...]).astype(bf16)


def project_kv(where, pieces, weights):
    return call(
        kv_body,
        (shape((ROWS, 2048), bf16), shape((ROWS + EXTRA, 256), bf16), shape((8, ROWS), f32)),
        1,
        15,
        [pltpu.VMEM((2048, 256), bf16)],
        flops=2 * ROWS * 2048 * 256,
        name="project_kv",
    )(where, *pieces, *weights)


def qd_body(where, rows_ref, own, up, down, far0, far1, q_ref, d_ref, w_all):
    weight_rows(where[0], w_all, own, up, down, far0, far1)
    both = mm(rows_ref[...], w_all[...])
    q_ref[...] = both[:, :BLOCK].astype(bf16)
    d_ref[...] = both[:, BLOCK:].astype(bf16)


def project_qd(where, rows, weights):
    return call(
        qd_body,
        (shape((ROWS, BLOCK), bf16), shape((ROWS, BLOCK), bf16)),
        1,
        6,
        [pltpu.VMEM((2048, 256), bf16)],
        flops=2 * ROWS * 2048 * 256,
        name="project_qd",
    )(where, rows, *weights)


SPAN = 256
TILE = 64


def chunk(q_ref, kv_ref, tri_ref, acc_ref, fall_ref, scr, diagonal):
    s_ref, hi_ref, lo_ref, r_ref, w_ref = scr
    for blk in (1, 0):
        keys = kv_ref[blk * SPAN : (blk + 1) * SPAN, :BLOCK]
        vals = kv_ref[blk * SPAN : (blk + 1) * SPAN, BLOCK:]
        off = kv_ref[ROWS : ROWS + EXTRA, :].astype(f32)[blk : blk + 1] * LOG2E
        s_ref[...] = lax.dot_general(
            q_ref[...], keys, (((1,), (1,)), ((), ())), preferred_element_type=f32
        )

        def visible(i):
            t = lax.broadcasted_iota(jnp.int32, (TILE, SPAN), 0) + i * TILE
            s = lax.broadcasted_iota(jnp.int32, (TILE, SPAN), 1) + blk * SPAN
            return s < t

        def first(i, _):
            at = pl.ds(pl.multiple_of(i * TILE, TILE), TILE)
            z = s_ref[at, :] * SCORE + off
            soft = jnp.maximum(z, 0.0) + jnp.log2(1.0 + jnp.exp2(-jnp.abs(z)))
            s_ref[at, :] = z - soft
            if diagonal:
                soft = jnp.where(visible(i), soft, 0.0)
            hi, lo = split2(soft)
            hi_ref[at, :] = hi
            lo_ref[at, :] = lo
            return 0

        lax.fori_loop(0, ROWS // TILE, first, 0, unroll=2)
        r_ref[...] = mm(hi_ref[...], tri_ref[...]) + mm(lo_ref[...], tri_ref[...])

        def second(i, _):
            at = pl.ds(pl.multiple_of(i * TILE, TILE), TILE)
            fall = fall_ref[at, :]
            w = jnp.exp2(
                s_ref[at, :] - r_ref[at, :SPAN] - jnp.concatenate([fall, fall], axis=1)
            )
            if diagonal:
                w = jnp.where(visible(i), w, 0.0)
            w_ref[at, :] = w.astype(bf16)
            fall_ref[at, :] = fall + r_ref[at, SPAN:]
            return 0

        lax.fori_loop(0, ROWS // TILE, second, 0, unroll=2)
        acc_ref[...] += mm(w_ref[...], vals)


ATTEND_SCRATCH = [
    pltpu.VMEM((ROWS, SPAN), f32),
    pltpu.VMEM((ROWS, SPAN), bf16),
    pltpu.VMEM((ROWS, SPAN), bf16),
    pltpu.VMEM((ROWS, SPAN + BLOCK), f32),
    pltpu.VMEM((ROWS, SPAN), bf16),
]
PAIR = (shape((ROWS, BLOCK), f32), shape((ROWS, BLOCK), f32))
ATTEND_FLOPS = 8 * ROWS * ROWS * BLOCK


def own_body(q_ref, kv_ref, tri_ref, acc_ref, fall_ref, *scr):
    acc_ref[...] = jnp.zeros((ROWS, BLOCK), f32)
    fall_ref[...] = jnp.zeros((ROWS, BLOCK), f32)
    chunk(q_ref, kv_ref, tri_ref, acc_ref, fall_ref, scr, True)


def attend_own(q, kv, tri):
    return call(own_body, PAIR, 0, 3, ATTEND_SCRATCH, flops=ATTEND_FLOPS, name="attend_own")(q, kv, tri)


def up_body(where, q_ref, kv_ref, tri_ref, acc_in, fall_in, acc_ref, fall_ref, *scr, step):
    acc_ref[...] = acc_in[...]
    fall_ref[...] = fall_in[...]

    @pl.when(where[3] >= step)
    def _():
        chunk(q_ref, kv_ref, tri_ref, acc_ref, fall_ref, scr, False)


def attend_up(where, q, kv, tri, acc, fall, step):
    def body(*refs):
        up_body(*refs, step=step)

    return call(body, PAIR, 1, 5, ATTEND_SCRATCH, flops=ATTEND_FLOPS, name="attend_up")(
        where, q, kv, tri, acc, fall
    )


def attend_down(where, q, kv, tri, acc, step):
    def body(where, q_ref, kv_ref, tri_ref, acc_in, acc_ref, fall_ref, *scr):
        @pl.when(where[3] + step >= 8)
        def _():
            acc_ref[...] = jnp.zeros((ROWS, BLOCK), f32)
            fall_ref[...] = jnp.zeros((ROWS, BLOCK), f32)
            chunk(q_ref, kv_ref, tri_ref, acc_ref, fall_ref, scr, False)
            acc_ref[...] += jnp.exp2(-fall_ref[...]) * acc_in[...]

        @pl.when(where[3] + step < 8)
        def _():
            acc_ref[...] = acc_in[...]

    return call(
        body,
        PAIR[0],
        1,
        4,
        [pltpu.VMEM((ROWS, BLOCK), f32)] + ATTEND_SCRATCH,
        flops=ATTEND_FLOPS,
        name="attend_down",
    )(where, q, kv, tri, acc)


def attend_last(where, q, kv, tri, acc, fall, far, scan_out):
    def body(where, q_ref, kv_ref, tri_ref, acc_in, fall_in, far_ref, scan_ref, out_ref, acc_ref, fall_ref, *scr):
        up_body(where, q_ref, kv_ref, tri_ref, acc_in, fall_in, acc_ref, fall_ref, *scr, step=4)
        out_ref[:, :BLOCK] = scan_ref[...]
        out_ref[:, BLOCK:] = (acc_ref[...] + jnp.exp2(-fall_ref[...]) * far_ref[...]).astype(bf16)

    return call(
        body,
        shape((ROWS, 2 * BLOCK), bf16),
        1,
        7,
        [pltpu.VMEM((ROWS, BLOCK), f32)] * 2 + ATTEND_SCRATCH,
        flops=ATTEND_FLOPS,
        name="attend_last",
    )(where, q, kv, tri, acc, fall, far, scan_out)


N = 512


def cmul(ar, ai, br, bi):
    return ar * br - ai * bi, ar * bi + ai * br


def dot3(a_hi, a_lo, b_hi, b_lo):
    return mm(a_hi, b_hi) + mm(a_lo, b_hi) + mm(a_hi, b_lo)


def scan_body(
    u_ref, f_ref, lam_ref, b_hi, b_lo, c_hi, c_lo, sel_ref, skip_ref,
    y_ref, ef_ref, pow_ref, hop_ref, sum_ref, inv_ref,
):
    bar_r, bar_i, gain = lam_ref[0:1, :], lam_ref[1:2, :], lam_ref[2:3, :]
    count = lax.broadcasted_iota(jnp.int32, (BLOCK, N), 0) + 1
    pr = jnp.ones((BLOCK, N), f32)
    pi = jnp.zeros((BLOCK, N), f32)
    sr, si = bar_r, bar_i
    for bit in range(8):
        on = ((count >> bit) & 1) == 1
        nr, ni = cmul(pr, pi, sr, si)
        pr, pi = jnp.where(on, nr, pr), jnp.where(on, ni, pi)
        if bit < 7:
            sr, si = cmul(sr, si, sr, si)
    back = jnp.exp(-2.0 * count.astype(f32) * gain)
    pow_ref[:BLOCK, :] = pr
    pow_ref[BLOCK:, :] = pi
    inv_ref[:BLOCK, :] = pr * back
    inv_ref[BLOCK:, :] = -pi * back
    row = lax.broadcasted_iota(jnp.int32, (BLOCK, BLOCK), 0)
    col = lax.broadcasted_iota(jnp.int32, (BLOCK, BLOCK), 1)
    low = (col <= row).astype(bf16)
    low32 = (col <= row).astype(f32)
    carry_r = jnp.zeros((1, N), f32)
    carry_i = jnp.zeros((1, N), f32)
    hop_r = jnp.ones((1, N), f32)
    hop_i = jnp.zeros((1, N), f32)
    hops = []
    for b in range(ROWS // BLOCK):
        rows = slice(b * BLOCK, (b + 1) * BLOCK)
        f = f_ref[:, rows]
        f_all = jnp.concatenate([jnp.broadcast_to(f[g : g + 1], (16, BLOCK)) for g in range(8)], axis=0)
        cum_f = lax.dot_general(
            low32, f_all, (((1,), (1,)), ((), ())), precision=lax.Precision.HIGHEST, preferred_element_type=f32
        )
        ef = jnp.exp(cum_f)
        ef_ref[rows, :] = ef
        u = u_ref[rows, :].astype(f32)
        drive = dot3(*split2(u * jnp.exp(-cum_f)), b_hi[...], b_lo[...])
        dr, di = cmul(drive[:, :N], drive[:, N:], inv_ref[:BLOCK, :], inv_ref[BLOCK:, :])
        drh, drl = split2(dr)
        dih, dil = split2(di)
        tr = mm(low, drh) + mm(low, drl) + carry_r
        ti = mm(low, dih) + mm(low, dil) + carry_i
        st_r, st_i = cmul(pow_ref[:BLOCK, :], pow_ref[BLOCK:, :], tr, ti)
        rh, rl = split2(st_r)
        ih, il = split2(st_i)
        out = dot3(rh, rl, c_hi[:N, :], c_lo[:N, :]) + dot3(ih, il, c_hi[N:, :], c_lo[N:, :])
        y_ref[rows, :] = ef * out + skip_ref[...] * u
        last_f = jnp.dot(
            cum_f[BLOCK - 8 :, :], sel_ref[...], precision=lax.Precision.HIGHEST, preferred_element_type=f32
        )[7:8]
        keep = jnp.exp(last_f)
        carry_r = keep * st_r[BLOCK - 1 :, :]
        carry_i = keep * st_i[BLOCK - 1 :, :]
        hops += [hop_r, hop_i]
        nr, ni = cmul(hop_r, hop_i, pow_ref[BLOCK - 1 : BLOCK, :], pow_ref[2 * BLOCK - 1 :, :])
        hop_r, hop_i = keep * nr, keep * ni
    hop_ref[...] = jnp.concatenate(hops, axis=0)
    sum_ref[...] = jnp.concatenate(
        [carry_r, carry_i, hop_r, hop_i, jnp.zeros((4, N), f32)], axis=0
    )


def scan_local(u, forget, lam, b_hi, b_lo, c_hi, c_lo, sel, skip):
    return call(
        scan_body,
        (
            shape((ROWS, BLOCK), f32),
            shape((ROWS, BLOCK), f32),
            shape((2 * BLOCK, N), f32),
            shape((8, N), f32),
            shape((8, N), f32),
        ),
        0,
        9,
        [pltpu.VMEM((2 * BLOCK, N), f32)],
        flops=5 * 10**9,
        name="scan_local",
    )(u, forget, lam, b_hi, b_lo, c_hi, c_lo, sel, skip)


def finish_body(where, y_ref, ef_ref, pow_ref, hop_ref, all_ref, init_ref, c_hi, c_lo, out_ref):
    z = where[3]
    sr, si = init_ref[0:1, :], init_ref[1:2, :]
    for j in range(7):
        part = all_ref[j]
        nr, ni = cmul(part[2:3], part[3:4], sr, si)
        sr = jnp.where(j < z, nr + part[0:1], sr)
        si = jnp.where(j < z, ni + part[1:2], si)
    for b in range(ROWS // BLOCK):
        rows = slice(b * BLOCK, (b + 1) * BLOCK)
        er, ei = cmul(hop_ref[2 * b : 2 * b + 1, :], hop_ref[2 * b + 1 : 2 * b + 2, :], sr, si)
        gr, gi = cmul(pow_ref[:BLOCK, :], pow_ref[BLOCK:, :], er, ei)
        rh, rl = split2(gr)
        ih, il = split2(gi)
        more = dot3(rh, rl, c_hi[:N, :], c_lo[:N, :]) + dot3(ih, il, c_hi[N:, :], c_lo[N:, :])
        v = y_ref[rows, :] + ef_ref[rows, :] * more
        inner = math.sqrt(2.0 / math.pi) * (v + 0.044715 * v * v * v)
        out_ref[rows, :] = (0.5 * v * (1.0 + jnp.tanh(inner))).astype(bf16)


def scan_finish(where, y, ef, power, hop, everyone, init, c_hi, c_lo):
    return call(
        finish_body, shape((ROWS, BLOCK), bf16), 1, 8, flops=2 * 10**9, name="scan_finish"
    )(where, y, ef, power, hop, everyone, init, c_hi, c_lo)


def scan_weights(log_step, lambda_real, lambda_imag, input_map, output_map):
    step = jnp.exp(log_step)[:, None]
    log_gain = lambda_real * step
    rotate = lambda_imag * step
    magnitude = jnp.exp(log_gain)
    bar_real = magnitude * jnp.cos(rotate)
    bar_imag = magnitude * jnp.sin(rotate)
    divisor = lambda_real * lambda_real + lambda_imag * lambda_imag
    shifted = bar_real - 1.0
    factor_real = (shifted * lambda_real + bar_imag * lambda_imag) / divisor
    factor_imag = (bar_imag * lambda_real - shifted * lambda_imag) / divisor
    map_real = factor_real[:, :, None] * input_map[0] - factor_imag[:, :, None] * input_map[1]
    map_imag = factor_real[:, :, None] * input_map[1] + factor_imag[:, :, None] * input_map[0]
    eye = jnp.eye(8, dtype=f32)

    def spread(part):
        return (part.transpose(0, 2, 1)[:, :, None, :] * eye[:, None, :, None]).reshape(BLOCK, N)

    b = jnp.concatenate([spread(map_real), spread(map_imag)], axis=1)

    def gather(part):
        return (part.transpose(0, 2, 1)[:, :, None, :] * eye[:, None, :, None]).reshape(N, BLOCK)

    c = jnp.concatenate([gather(output_map[0]), -gather(output_map[1])], axis=0)
    lam = jnp.stack([bar_real, bar_imag, log_gain]).reshape(3, N)
    return (lam, *split2(b), *split2(c))


def out_body(where, recv_ref, *refs):
    pieces, out_ref, lhs_ref = refs[:10], refs[10], refs[11]
    x, c = where[0], where[2]
    for part in range(2):
        core = (c + part) % 2
        for k in range(4):
            got = recv_ref[2 * k + core]
            lhs_ref[part, :, k * BLOCK : (k + 1) * BLOCK] = got[:, :BLOCK]
            lhs_ref[part, :, ROWS + k * BLOCK : ROWS + (k + 1) * BLOCK] = got[:, BLOCK:]
    for k, step in enumerate((0, 3, 1, 2)):
        total = jnp.zeros((64, ROWS), f32)
        for part in range(2):
            group = pieces[5 * part : 5 * part + 5]
            if k < 3:
                total += mm(lhs_ref[part], group[k][...])
            else:
                total += mm(lhs_ref[part, :, :ROWS], group[3][...])
                total += mm(lhs_ref[part, :, ROWS:], group[4][...])
        at = pl.multiple_of(((x + step) % 4) * ROWS, ROWS)
        out_ref[:, pl.ds(at, ROWS)] = total.astype(bf16)


def project_out(where, recv, pieces):
    return call(
        out_body,
        shape((64, 2048), bf16),
        1,
        11,
        [pltpu.VMEM((2, 64, 1024), bf16)],
        flops=64 * 2048 * 2048 * 2,
        name="project_out",
    )(where, recv, *pieces)


def shift(a, axis, by):
    n = lax.axis_size(axis)
    return lax.ppermute(a, axis, [(i, (i + by) % n) for i in range(n)])


def ring4(a, axis, cut):
    up = shift(a, axis, 1)
    down = shift(a, axis, -1)
    far0 = shift(up[:cut], axis, 1)
    far1 = shift(down[cut:], axis, -1)
    return [a, up, down, far0, far1]


def after(a, b):
    return lax.optimization_barrier((a, b))[0]


def on_device(
    tokens,
    norm_gain,
    drive_weight,
    query_weight,
    key_weight,
    value_weight,
    key_offset,
    log_step,
    lambda_real,
    lambda_imag,
    input_map,
    output_map,
    skip_gain,
    forget,
    initial_state,
    scan_out_weight,
    attend_out_weight,
):
    z, y, x, c = (lax.axis_index(a) for a in ("z", "y", "x", "c"))
    where = jnp.stack([x, y, c, z]).astype(jnp.int32)

    def columns(w):
        return lax.dynamic_slice_in_dim(w, y * BLOCK, BLOCK, 1)

    w_kv = jnp.concatenate([columns(key_weight), columns(value_weight)], axis=1)
    w_qd = jnp.concatenate([columns(query_weight), columns(drive_weight)], axis=1)
    normed = normalize(tokens[0], norm_gain, forget[:, 0, :], key_offset[:, 0, :])
    mine = ring4(normed, "y", EXTRA + 32)
    theirs = [shift(a, "c", 1) for a in mine]
    kv_weights = ring4(w_kv, "x", 256)
    qd_weights = ring4(after(w_qd, kv_weights[4]), "x", 256)
    rows, kv, forget_all = project_kv(where, mine + theirs, kv_weights)

    ups, downs = [kv], [kv]
    for k in range(3):
        ups.append(shift(ups[-1], "z", 1))
        downs.append(shift(downs[-1], "z", -1))
    ups.append(shift(ups[-1], "z", 1))

    out_rows = jnp.concatenate([scan_out_weight, attend_out_weight], axis=0)
    own_out = ring4(after(out_rows, qd_weights[4]), "x", 512)
    other_out = [shift(a, "c", 1) for a in own_out]

    def groups(a, dim):
        return lax.dynamic_slice_in_dim(a, y * 8, 8, dim)

    lam, b_hi, b_lo, c_hi, c_lo = scan_weights(
        groups(log_step, 0),
        groups(lambda_real, 0),
        groups(lambda_imag, 0),
        groups(input_map, 1),
        groups(output_map, 1),
    )
    skip = lax.dynamic_slice_in_dim(skip_gain, y * BLOCK, BLOCK, 0).reshape(1, BLOCK)
    init = groups(initial_state[:, 0], 1).reshape(2, N)
    pick = jnp.arange(BLOCK)[:, None] == (jnp.arange(N)[None] // 64) * 16
    span = jnp.arange(SPAN)
    tri = jnp.concatenate(
        [(span[:, None] > span[None]).astype(bf16), jnp.ones((SPAN, BLOCK), bf16)], axis=1
    )

    q, drive = project_qd(where, rows, qd_weights)
    y_local, ef, power, hop, summary = scan_local(
        drive, forget_all, lam, b_hi, b_lo, c_hi, c_lo, pick.astype(f32), skip
    )
    everyone = lax.all_to_all(
        jnp.broadcast_to(summary[None], (8, 8, N)), "z", split_axis=0, concat_axis=0, tiled=True
    )
    acc, fall = attend_own(q, kv, tri)
    far = jnp.zeros((ROWS, BLOCK), f32)
    for k in range(1, 4):
        acc, fall = attend_up(where, q, ups[k], tri, acc, fall, k)
        far = attend_down(where, q, downs[k], tri, far, k)
    scan_out = scan_finish(where, y_local, ef, power, hop, everyone, init, c_hi, c_lo)
    both = attend_last(where, q, ups[4], tri, acc, fall, far, scan_out)
    recv = lax.all_to_all(
        both.reshape(8, 64, 2 * BLOCK), ("y", "c"), split_axis=0, concat_axis=0, tiled=True
    )
    return project_out(where, recv, own_out + other_out)[None]


def solution(mesh):
    split = Mesh(
        mesh.devices.reshape(8, 4, mesh.shape["fs"], mesh.shape["tp"]), ("z", "y", "x", "c")
    )
    in_specs = (
        P("x", SP_TP, None),
        P(),
        P("x", "c"),
        P("x", "c"),
        P("x", "c"),
        P("x", "c"),
        P("c", "x", SP),
        P("c"),
        P("c", None),
        P("c", None),
        P(None, "c", None, None),
        P(None, "c", None, None),
        P("c"),
        P("c", "x", SP),
        P(None, "x", "c", None),
        P("c", "x"),
        P("c", "x"),
    )
    out_specs = P("x", SP_TP, None)
    return jax.shard_map(
        on_device, mesh=split, in_specs=in_specs, out_specs=out_specs, check_vma=False
    )
```

```python
import math

import jax
import jax.numpy as jnp
from jax import lax
from jax.experimental import pallas as pl
from jax.experimental.pallas import tpu as pltpu
from jax.sharding import Mesh
from jax.sharding import PartitionSpec as P

HEAD_DIM = 128
BLOCK = 128
ROWS = 512
EXTRA = 16
MORE = 8
SP = ("z", "y")
SP_TP = ("z", "y", "c")
LOG2E = 1.4426950408889634
SCORE = HEAD_DIM ** (-0.5) * LOG2E
epsilon = 1e-06
f32 = jnp.float32
bf16 = jnp.bfloat16
INTERPRET = False


def vmem(n):
    return [pl.BlockSpec(memory_space=pltpu.VMEM)] * n


def call(body, out_shape, n_in, scratch=(), flops=0, name=None, limit=16):
    many = isinstance(out_shape, (list, tuple))
    return pl.pallas_call(
        body,
        out_shape=out_shape,
        in_specs=vmem(n_in),
        out_specs=vmem(len(out_shape)) if many else vmem(1)[0],
        scratch_shapes=list(scratch),
        cost_estimate=pl.CostEstimate(flops=flops, transcendentals=0, bytes_accessed=1 << 20),
        compiler_params=pltpu.CompilerParams(vmem_limit_bytes=limit << 20),
        interpret=INTERPRET,
        name=name,
    )


def whole(a):
    return pl.BlockSpec(a.shape, lambda i: (0,) * len(a.shape))


def fetched(body, out_shape, arrays, flops=0, name=None, limit=24):
    many = isinstance(out_shape, (list, tuple))
    return pl.pallas_call(
        body,
        out_shape=out_shape,
        grid=(1,),
        in_specs=[whole(a) for a in arrays],
        out_specs=[whole(a) for a in out_shape] if many else whole(out_shape),
        cost_estimate=pl.CostEstimate(flops=flops, transcendentals=0, bytes_accessed=1 << 20),
        compiler_params=pltpu.CompilerParams(vmem_limit_bytes=limit << 20),
        interpret=INTERPRET,
        name=name,
    )(*arrays)


def shape(dims, dtype):
    return jax.ShapeDtypeStruct(dims, dtype)


def split2(v):
    hi = v.astype(bf16)
    return hi, (v - hi.astype(f32)).astype(bf16)


def mm(a, b):
    return jnp.dot(a, b, preferred_element_type=f32)


def mm_t(a, b):
    return lax.dot_general(a, b, (((1,), (1,)), ((), ())), preferred_element_type=f32)


def norm_body(tok_ref, gain_ref, forget_ref, off_ref, out_ref):
    v = tok_ref[0].astype(f32)
    scale = lax.rsqrt(jnp.mean(v * v, axis=1, keepdims=True) + epsilon)
    normed = (v * scale * gain_ref[...]).astype(bf16)
    hi, lo = split2(forget_ref[...])
    hi, lo = hi.astype(f32), lo.astype(f32)
    off = off_ref[...].astype(f32)
    blank = jnp.zeros((6, BLOCK), f32)
    for k in range(4):
        out_ref[k, :64, :] = normed
        for j in range(16):
            row = hi[8 * k + j : 8 * k + j + 1] if j < 8 else lo[8 * k + j - 8 : 8 * k + j - 7]
            last = off[k : k + 1] if j == 0 else jnp.zeros((1, BLOCK), f32)
            tile = jnp.concatenate([row, last, blank], axis=0)
            out_ref[k, 64:, j * BLOCK : (j + 1) * BLOCK] = tile.astype(bf16)


def normalize(tokens, gain, forget, offset):
    return fetched(
        norm_body,
        shape((4, 64 + MORE, 2048), bf16),
        [tokens, gain.reshape(1, -1), forget, offset],
        flops=10**6,
        name="norm",
    )


def pack_body(left_ref, right_ref, out_ref, sems):
    at = pl.ds(pl.multiple_of(lax.axis_index("y") * BLOCK, BLOCK), BLOCK)
    copies = []
    for k in range(4):
        for h, ref in enumerate((left_ref, right_ref)):
            copies.append(
                pltpu.make_async_copy(
                    ref.at[:, at], out_ref.at[k, :, pl.ds(h * BLOCK, BLOCK)], sems.at[2 * k + h]
                )
            )
    for copy in copies:
        copy.start()
    for copy in copies:
        copy.wait()


def pack(left, right):
    anywhere = pl.BlockSpec(memory_space=pl.ANY)
    return pl.pallas_call(
        pack_body,
        out_shape=shape((4, ROWS, 2 * BLOCK), bf16),
        in_specs=[anywhere, anywhere],
        out_specs=anywhere,
        scratch_shapes=[pltpu.SemaphoreType.DMA((8,))],
        interpret=INTERPRET,
        name="pack",
    )(left, right)


def kv_body(mine_ref, theirs_ref, w_ref, rows_ref, kv_ref, forget_ref):
    c = lax.axis_index("c")
    offs = []
    for b in range(4):
        for part, ref in enumerate((mine_ref, theirs_ref)):
            at = pl.multiple_of(b * BLOCK + ((c + part) % 2) * 64, 64)
            rows_ref[pl.ds(at, 64), :] = ref[b, :64, :]
        tile = mine_ref[b, 64:, :].astype(f32)
        both = tile[0:1, : 8 * BLOCK] + tile[0:1, 8 * BLOCK :]
        forget_ref[:, b * BLOCK : (b + 1) * BLOCK] = jnp.concatenate(
            [both[:, g * BLOCK : (g + 1) * BLOCK] for g in range(8)], axis=0
        )
        offs.append(tile[1:2, :BLOCK])
    row0 = jnp.concatenate(offs[:2], axis=1)
    row1 = jnp.concatenate(offs[2:], axis=1)
    tail = jnp.concatenate([row0, row1, jnp.zeros((EXTRA - 2, 256), f32)], axis=0)
    kv_ref[ROWS:, :] = tail.astype(bf16)
    kv_ref[:ROWS, :] = mm(rows_ref[...], w_ref[...]).astype(bf16)


def project_kv(mine, theirs, weights):
    return call(
        kv_body,
        (shape((ROWS, 2048), bf16), shape((ROWS + EXTRA, 256), bf16), shape((8, ROWS), f32)),
        3,
        flops=2 * ROWS * 2048 * 256,
        name="project_kv",
    )(mine, theirs, weights)


def qd_body(rows_ref, w_ref, q_ref, d_ref):
    both = mm(rows_ref[...], w_ref[...])
    q_ref[...] = both[:, :BLOCK].astype(bf16)
    d_ref[...] = both[:, BLOCK:].astype(bf16)


def project_qd(rows, weights):
    return call(
        qd_body,
        (shape((ROWS, BLOCK), bf16), shape((ROWS, BLOCK), bf16)),
        2,
        flops=2 * ROWS * 2048 * 256,
        name="project_qd",
    )(rows, weights)


SPAN = 256
TILE = 64


def chunk(q_ref, kv_ref, acc_ref, fall_ref, scr, diagonal):
    s_ref, hi_ref, lo_ref, r_ref, w_ref, tri_ref = scr
    j = lax.broadcasted_iota(jnp.int32, (SPAN, SPAN + BLOCK), 0)
    k = lax.broadcasted_iota(jnp.int32, (SPAN, SPAN + BLOCK), 1)
    tri_ref[...] = jnp.where((j > k) | (k >= SPAN), 1.0, 0.0).astype(bf16)
    for blk in (1, 0):
        keys = kv_ref[blk * SPAN : (blk + 1) * SPAN, :BLOCK]
        vals = kv_ref[blk * SPAN : (blk + 1) * SPAN, BLOCK:]
        off = kv_ref[ROWS : ROWS + EXTRA, :].astype(f32)[blk : blk + 1] * LOG2E
        s_ref[...] = lax.dot_general(
            q_ref[...], keys, (((1,), (1,)), ((), ())), preferred_element_type=f32
        )

        def visible(i):
            t = lax.broadcasted_iota(jnp.int32, (TILE, SPAN), 0) + i * TILE
            s = lax.broadcasted_iota(jnp.int32, (TILE, SPAN), 1) + blk * SPAN
            return s < t

        def first(i, _):
            at = pl.ds(pl.multiple_of(i * TILE, TILE), TILE)
            z = s_ref[at, :] * SCORE + off
            soft = jnp.maximum(z, 0.0) + jnp.log2(1.0 + jnp.exp2(-jnp.abs(z)))
            s_ref[at, :] = z - soft
            if diagonal:
                soft = jnp.where(visible(i), soft, 0.0)
            hi, lo = split2(soft)
            hi_ref[at, :] = hi
            lo_ref[at, :] = lo
            return 0

        lax.fori_loop(0, ROWS // TILE, first, 0, unroll=2)
        r_ref[...] = mm(hi_ref[...], tri_ref[...]) + mm(lo_ref[...], tri_ref[...])

        def second(i, _):
            at = pl.ds(pl.multiple_of(i * TILE, TILE), TILE)
            fall = fall_ref[at, :]
            w = jnp.exp2(
                s_ref[at, :] - r_ref[at, :SPAN] - jnp.concatenate([fall, fall], axis=1)
            )
            if diagonal:
                w = jnp.where(visible(i), w, 0.0)
            w_ref[at, :] = w.astype(bf16)
            fall_ref[at, :] = fall + r_ref[at, SPAN:]
            return 0

        lax.fori_loop(0, ROWS // TILE, second, 0, unroll=2)
        acc_ref[...] += mm(w_ref[...], vals)


ATTEND_SCRATCH = [
    pltpu.VMEM((ROWS, SPAN), f32),
    pltpu.VMEM((ROWS, SPAN), bf16),
    pltpu.VMEM((ROWS, SPAN), bf16),
    pltpu.VMEM((ROWS, SPAN + BLOCK), f32),
    pltpu.VMEM((ROWS, SPAN), bf16),
    pltpu.VMEM((SPAN, SPAN + BLOCK), bf16),
]
PAIR = (shape((ROWS, BLOCK), f32), shape((ROWS, BLOCK), f32))
ATTEND_FLOPS = 8 * ROWS * ROWS * BLOCK


def own_body(q_ref, kv_ref, acc_ref, fall_ref, *scr):
    acc_ref[...] = jnp.zeros((ROWS, BLOCK), f32)
    fall_ref[...] = jnp.zeros((ROWS, BLOCK), f32)
    chunk(q_ref, kv_ref, acc_ref, fall_ref, scr, True)


def attend_own(q, kv):
    return call(own_body, PAIR, 2, ATTEND_SCRATCH, flops=ATTEND_FLOPS, name="attend_own")(q, kv)


def step_up(active, q_ref, kv_ref, acc_in, fall_in, acc_ref, fall_ref, scr):
    acc_ref[...] = acc_in[...]
    fall_ref[...] = fall_in[...]

    @pl.when(active)
    def _():
        chunk(q_ref, kv_ref, acc_ref, fall_ref, scr, False)


def attend_step(q, up, down, acc, fall, far, step):
    def body(
        q_ref, up_ref, down_ref, acc_in, fall_in, far_in,
        acc_ref, fall_ref, far_ref, low_ref, *scr,
    ):
        z = lax.axis_index("z")
        step_up(z >= step, q_ref, up_ref, acc_in, fall_in, acc_ref, fall_ref, scr)

        @pl.when(z + step >= 8)
        def _():
            far_ref[...] = jnp.zeros((ROWS, BLOCK), f32)
            low_ref[...] = jnp.zeros((ROWS, BLOCK), f32)
            chunk(q_ref, down_ref, far_ref, low_ref, scr, False)
            far_ref[...] += jnp.exp2(-low_ref[...]) * far_in[...]

        @pl.when(z + step < 8)
        def _():
            far_ref[...] = far_in[...]

    return call(
        body,
        PAIR + PAIR[:1],
        6,
        [pltpu.VMEM((ROWS, BLOCK), f32)] + ATTEND_SCRATCH,
        flops=2 * ATTEND_FLOPS,
        name="attend_step",
    )(q, up, down, acc, fall, far)


def attend_last(q, kv, acc, fall, far, scan_out):
    def body(q_ref, kv_ref, acc_in, fall_in, far_ref, scan_ref, out_ref, acc_ref, fall_ref, *scr):
        step_up(lax.axis_index("z") >= 4, q_ref, kv_ref, acc_in, fall_in, acc_ref, fall_ref, scr)
        out_ref[:, :BLOCK] = scan_ref[...]
        out_ref[:, BLOCK:] = (acc_ref[...] + jnp.exp2(-fall_ref[...]) * far_ref[...]).astype(bf16)

    return call(
        body,
        shape((ROWS, 2 * BLOCK), bf16),
        6,
        [pltpu.VMEM((ROWS, BLOCK), f32)] * 2 + ATTEND_SCRATCH,
        flops=ATTEND_FLOPS,
        name="attend_last",
    )(q, kv, acc, fall, far, scan_out)


N = 512


def cmul(ar, ai, br, bi):
    return ar * br - ai * bi, ar * bi + ai * br


def dot3(a_hi, a_lo, b_hi, b_lo):
    return mm_t(a_hi, b_hi) + mm_t(a_lo, b_hi) + mm_t(a_hi, b_lo)


def tables_body(
    in_ref, out_ref, rows_ref, skip_in,
    pow_ref, inv_ref, bt_hi, bt_lo, ct_hi, ct_lo, init_ref, skip_ref,
):
    y = lax.axis_index("y")
    rows = rows_ref[:, pl.ds(pl.multiple_of(y * N, N), N)]
    lam_r, lam_i, step = rows[0:1], rows[1:2], jnp.exp(rows[2:3])
    init_ref[...] = rows[3:5]
    skip_ref[...] = skip_in[:, pl.ds(pl.multiple_of(y * BLOCK, BLOCK), BLOCK)]
    gain = lam_r * step
    turn = lam_i * step
    size = jnp.exp(gain)
    bar_r = size * jnp.cos(turn)
    bar_i = size * jnp.sin(turn)
    over = lam_r * lam_r + lam_i * lam_i
    less = bar_r - 1.0
    factor_r = (less * lam_r + bar_i * lam_i) / over
    factor_i = (bar_i * lam_r - less * lam_i) / over
    count = lax.broadcasted_iota(jnp.int32, (BLOCK, N), 0) + 1
    pr = jnp.ones((BLOCK, N), f32)
    pi = jnp.zeros((BLOCK, N), f32)
    sr, si = bar_r, bar_i
    for bit in range(8):
        on = ((count >> bit) & 1) == 1
        nr, ni = cmul(pr, pi, sr, si)
        pr, pi = jnp.where(on, nr, pr), jnp.where(on, ni, pi)
        if bit < 7:
            sr, si = cmul(sr, si, sr, si)
    back = jnp.exp(-2.0 * count.astype(f32) * gain)
    pow_ref[:BLOCK, :] = pr
    pow_ref[BLOCK:, :] = pi
    br, bi = cmul(pr * back, -pi * back, factor_r, factor_i)
    inv_ref[:BLOCK, :] = br
    inv_ref[BLOCK:, :] = bi
    own = pl.ds(pl.multiple_of(y * 8, 8), 8)

    def tiled(a, width, height, rows_total, cols_total):
        n = lax.broadcasted_iota(jnp.int32, (width, cols_total), 0)
        j = lax.broadcasted_iota(jnp.int32, (width, cols_total), 1)
        copy = (j % width == n).astype(bf16)
        r = lax.broadcasted_iota(jnp.int32, (rows_total, cols_total), 0) // height
        k = lax.broadcasted_iota(jnp.int32, (rows_total, cols_total), 1) // width
        return [jnp.where(r == k, mm(part, copy), 0.0).astype(bf16) for part in split2(a)]

    for p in range(2):
        hi, lo = tiled(in_ref[p, own].reshape(N, 16), 16, 64, N, BLOCK)
        bt_hi[p * N : (p + 1) * N, :] = hi
        bt_lo[p * N : (p + 1) * N, :] = lo
        sign = 1.0 if p == 0 else -1.0
        hi, lo = tiled(sign * out_ref[p, own].reshape(BLOCK, 64), 64, 16, BLOCK, N)
        ct_hi[:, p * N : (p + 1) * N] = hi
        ct_lo[:, p * N : (p + 1) * N] = lo


def scan_tables(input_map, output_map, rows, skip):
    return fetched(
        tables_body,
        (
            shape((2 * BLOCK, N), f32),
            shape((2 * BLOCK, N), f32),
            shape((2 * N, BLOCK), bf16),
            shape((2 * N, BLOCK), bf16),
            shape((BLOCK, 2 * N), bf16),
            shape((BLOCK, 2 * N), bf16),
            shape((2, N), f32),
            shape((1, BLOCK), f32),
        ),
        [input_map, output_map, rows, skip],
        flops=10**9,
        name="scan_tables",
    )


def scan_body(
    u_ref, f_ref, pow_ref, inv_ref, bt_hi, bt_lo, ct_hi, ct_lo, skip_ref,
    y_ref, ef_ref, hop_ref, sum_ref,
):
    row = lax.broadcasted_iota(jnp.int32, (BLOCK, BLOCK), 0)
    col = lax.broadcasted_iota(jnp.int32, (BLOCK, BLOCK), 1)
    low = (col <= row).astype(bf16)
    low32 = (col <= row).astype(f32)
    pick = (
        lax.broadcasted_iota(jnp.int32, (BLOCK, N), 0)
        == (lax.broadcasted_iota(jnp.int32, (BLOCK, N), 1) // 64) * 16
    ).astype(f32)

    def block(b, state):
        carry_r, carry_i, hop_r, hop_i = state
        rows = pl.ds(pl.multiple_of(b * BLOCK, BLOCK), BLOCK)
        f = f_ref[:, rows]
        f_all = jnp.concatenate([jnp.broadcast_to(f[g : g + 1], (16, BLOCK)) for g in range(8)], axis=0)
        cum_f = lax.dot_general(
            low32, f_all, (((1,), (1,)), ((), ())), precision=lax.Precision.HIGHEST, preferred_element_type=f32
        )
        ef = jnp.exp(cum_f)
        ef_ref[rows, :] = ef
        u = u_ref[rows, :].astype(f32)
        drive = dot3(*split2(u * jnp.exp(-cum_f)), bt_hi[...], bt_lo[...])
        dr, di = cmul(drive[:, :N], drive[:, N:], inv_ref[:BLOCK, :], inv_ref[BLOCK:, :])
        drh, drl = split2(dr)
        dih, dil = split2(di)
        tr = mm(low, drh) + mm(low, drl) + carry_r
        ti = mm(low, dih) + mm(low, dil) + carry_i
        st_r, st_i = cmul(pow_ref[:BLOCK, :], pow_ref[BLOCK:, :], tr, ti)
        rh, rl = split2(st_r)
        ih, il = split2(st_i)
        out = dot3(rh, rl, ct_hi[:, :N], ct_lo[:, :N]) + dot3(ih, il, ct_hi[:, N:], ct_lo[:, N:])
        y_ref[rows, :] = ef * out + skip_ref[...] * u
        last_f = jnp.dot(
            cum_f[BLOCK - 8 :, :], pick, precision=lax.Precision.HIGHEST, preferred_element_type=f32
        )[7:8]
        keep = jnp.exp(last_f)
        hop_ref[pl.ds(pl.multiple_of(b * 8, 8), 8), :] = jnp.concatenate(
            [hop_r, hop_i, jnp.zeros((6, N), f32)], axis=0
        )
        nr, ni = cmul(hop_r, hop_i, pow_ref[BLOCK - 1 : BLOCK, :], pow_ref[2 * BLOCK - 1 :, :])
        return keep * st_r[BLOCK - 1 :, :], keep * st_i[BLOCK - 1 :, :], keep * nr, keep * ni

    zero = jnp.zeros((1, N), f32)
    carry_r, carry_i, hop_r, hop_i = lax.fori_loop(
        0, ROWS // BLOCK, block, (zero, zero, zero + 1.0, zero)
    )
    total = jnp.concatenate([carry_r, carry_i, hop_r, hop_i, jnp.zeros((4, N), f32)], axis=0)
    for k in range(8):
        sum_ref[k] = total


def scan_local(u, forget, power, inverse, bt_hi, bt_lo, ct_hi, ct_lo, skip):
    return call(
        scan_body,
        (
            shape((ROWS, BLOCK), f32),
            shape((ROWS, BLOCK), f32),
            shape((32, N), f32),
            shape((8, 8, N), f32),
        ),
        9,
        flops=5 * 10**9,
        name="scan_local",
    )(u, forget, power, inverse, bt_hi, bt_lo, ct_hi, ct_lo, skip)


def finish_body(y_ref, ef_ref, pow_ref, hop_ref, all_ref, init_ref, ct_hi, ct_lo, out_ref):
    z = lax.axis_index("z")
    sr, si = init_ref[0:1, :], init_ref[1:2, :]
    for j in range(7):
        part = all_ref[j]
        nr, ni = cmul(part[2:3], part[3:4], sr, si)
        sr = jnp.where(j < z, nr + part[0:1], sr)
        si = jnp.where(j < z, ni + part[1:2], si)

    def block(b, _):
        rows = pl.ds(pl.multiple_of(b * BLOCK, BLOCK), BLOCK)
        hop = hop_ref[pl.ds(pl.multiple_of(b * 8, 8), 8), :]
        er, ei = cmul(hop[0:1], hop[1:2], sr, si)
        gr, gi = cmul(pow_ref[:BLOCK, :], pow_ref[BLOCK:, :], er, ei)
        rh, rl = split2(gr)
        ih, il = split2(gi)
        more = dot3(rh, rl, ct_hi[:, :N], ct_lo[:, :N]) + dot3(ih, il, ct_hi[:, N:], ct_lo[:, N:])
        v = y_ref[rows, :] + ef_ref[rows, :] * more
        inner = math.sqrt(2.0 / math.pi) * (v + 0.044715 * v * v * v)
        out_ref[rows, :] = (0.5 * v * (1.0 + jnp.tanh(inner))).astype(bf16)
        return 0

    lax.fori_loop(0, ROWS // BLOCK, block, 0)


def scan_finish(y, ef, power, hop, everyone, init, ct_hi, ct_lo):
    return call(
        finish_body, shape((ROWS, BLOCK), bf16), 8, flops=2 * 10**9, name="scan_finish"
    )(y, ef, power, hop, everyone, init, ct_hi, ct_lo)


def out_body(recv_ref, own, up, down, far0, far1, keep_ref, send_ref, lhs_ref, sum_ref):
    x, c = lax.axis_index("x"), lax.axis_index("c")
    for k in range(4):
        lhs_ref[:, k * BLOCK : (k + 1) * BLOCK] = recv_ref[k, :, :BLOCK]
        lhs_ref[:, ROWS + k * BLOCK : ROWS + (k + 1) * BLOCK] = recv_ref[k, :, BLOCK:]
    for piece, step in ((own, 0), (up, 3), (down, 1), (None, 2)):
        if step == 2:
            total = mm(lhs_ref[:, :ROWS], far0[...]) + mm(lhs_ref[:, ROWS:], far1[...])
        else:
            total = mm(lhs_ref[...], piece[...])
        sum_ref[:, pl.ds(pl.multiple_of(((x + step) % 4) * ROWS, ROWS), ROWS)] = total
    keep_ref[...] = sum_ref[pl.ds(pl.multiple_of(c * 64, 64), 64), :]
    send_ref[...] = sum_ref[pl.ds(pl.multiple_of((1 - c) * 64, 64), 64), :].astype(bf16)


def project_out(recv, pieces):
    return call(
        out_body,
        (shape((64, 2048), f32), shape((64, 2048), bf16)),
        6,
        [pltpu.VMEM((BLOCK, 1024), bf16), pltpu.VMEM((BLOCK, 2048), f32)],
        flops=BLOCK * 1024 * 2048 * 2,
        name="project_out",
    )(recv, *pieces)


def shift(a, axis, by):
    n = lax.axis_size(axis)
    return lax.ppermute(a, axis, [(i, (i + by) % n) for i in range(n)])


def ring4(a, axis, cut):
    up = shift(a, axis, 1)
    down = shift(a, axis, -1)
    far0 = shift(up[:cut], axis, 1)
    far1 = shift(down[cut:], axis, -1)
    return [a, up, down, far0, far1]


def after(a, b):
    return lax.optimization_barrier((a, b))[0]


def on_device(
    tokens,
    norm_gain,
    drive_weight,
    query_weight,
    key_weight,
    value_weight,
    key_offset,
    log_step,
    lambda_real,
    lambda_imag,
    input_map,
    output_map,
    skip_gain,
    forget,
    initial_state,
    scan_out_weight,
    attend_out_weight,
):
    def exchange(a, axis):
        return lax.all_to_all(a, axis, split_axis=0, concat_axis=0, tiled=True)

    w_kv = exchange(pack(key_weight, value_weight), "x").reshape(2048, 2 * BLOCK)
    normed = normalize(tokens, norm_gain, forget[:, 0, :], key_offset[:, 0, :])
    mine = exchange(normed, "y")
    theirs = shift(mine, "c", 1)
    w_qd = exchange(after(pack(query_weight, drive_weight), w_kv), "x")
    rows, kv, forget_all = project_kv(mine, theirs, w_kv)

    ups, downs = [kv], [kv]
    for k in range(3):
        ups.append(shift(ups[-1], "z", 1))
        downs.append(shift(downs[-1], "z", -1))
    ups.append(shift(ups[-1], "z", 1))

    out_rows = jnp.concatenate([scan_out_weight, attend_out_weight], axis=0)
    out_pieces = ring4(after(out_rows, (w_qd, kv)), "x", 512)

    row_table = jnp.stack(
        [
            lambda_real,
            lambda_imag,
            jnp.broadcast_to(log_step[:, None], lambda_real.shape),
            initial_state[0, 0],
            initial_state[1, 0],
        ]
    ).reshape(5, -1)
    power, inverse, bt_hi, bt_lo, ct_hi, ct_lo, init, skip = scan_tables(
        input_map, output_map, row_table, skip_gain.reshape(1, -1)
    )
    q, drive = project_qd(rows, w_qd.reshape(2048, 2 * BLOCK))
    y_local, ef, hop, summary = scan_local(
        drive, forget_all, power, inverse, bt_hi, bt_lo, ct_hi, ct_lo, skip
    )
    everyone = exchange(summary, "z")
    acc, fall = attend_own(q, kv)
    far = jnp.zeros((ROWS, BLOCK), f32)
    for k in range(1, 4):
        acc, fall, far = attend_step(q, ups[k], downs[k], acc, fall, far, k)
    scan_out = scan_finish(y_local, ef, power, hop, everyone, init, ct_hi, ct_lo)
    both = attend_last(q, ups[4], acc, fall, far, scan_out)
    recv = exchange(both.reshape(4, BLOCK, 2 * BLOCK), "y")
    keep, send = project_out(recv, out_pieces)
    return (keep + shift(send, "c", 1).astype(f32)).astype(bf16)[None]


def solution(mesh):
    split = Mesh(
        mesh.devices.reshape(8, 4, mesh.shape["fs"], mesh.shape["tp"]), ("z", "y", "x", "c")
    )
    in_specs = (
        P("x", SP_TP, None),
        P(),
        P("x", "c"),
        P("x", "c"),
        P("x", "c"),
        P("x", "c"),
        P("c", "x", SP),
        P("c"),
        P("c", None),
        P("c", None),
        P(None, "c", None, None),
        P(None, "c", None, None),
        P("c"),
        P("c", "x", SP),
        P(None, "x", "c", None),
        P("c", "x"),
        P("c", "x"),
    )
    out_specs = P("x", SP_TP, None)
    return jax.shard_map(
        on_device, mesh=split, in_specs=in_specs, out_specs=out_specs, check_vma=False
    )
```

```python
import math

import jax
import jax.numpy as jnp
from jax import lax
from jax.experimental import pallas as pl
from jax.experimental.pallas import tpu as pltpu
from jax.sharding import Mesh
from jax.sharding import PartitionSpec as P


HEAD_DIM = 128
BLOCK = 128
ROWS = 512
EXTRA = 16
MORE = 8
SP = ("z", "y")
SP_TP = ("z", "y", "c")
LOG2E = 1.4426950408889634
SCORE = HEAD_DIM ** (-0.5) * LOG2E
epsilon = 1e-06
f32 = jnp.float32
bf16 = jnp.bfloat16
INTERPRET = False


def staged(body, outs, arrays, scratch=(), flops=0, limit=20, lazy=False, raw=(), free=()):
    n, m = len(arrays), len(outs)
    kept = [i for i in range(n) if i not in raw]

    def kernel(*refs):
        src, dst = refs[:n], refs[n : n + m]
        refs = refs[n + m :]
        bufs = dict(zip(kept, refs[: len(kept)]))
        results = refs[len(kept) : len(kept) + m]
        sems, rest = refs[len(kept) + m], refs[len(kept) + m + 1 :]
        copies = {i: pltpu.make_async_copy(src[i], bufs[i], sems.at[i]) for i in kept}
        for i in kept:
            copies[i].start()
        leaving = {}

        def ready(*which):
            for i in which:
                copies[i].wait()

        def send(i):
            leaving[i] = pltpu.make_async_copy(results[i], dst[i], sems.at[n + i])
            leaving[i].start()

        ins = [bufs.get(i, src[i]) for i in range(n)]
        if lazy:
            body(ready, send, *ins, *results, *rest)
        else:
            ready(*kept)
            body(*ins, *results, *rest)
        for i in range(m):
            if i not in leaving:
                send(i)
        for i in range(m):
            leaving[i].wait()

    hbm = pl.BlockSpec(memory_space=pltpu.HBM)
    got = pl.pallas_call(
        kernel,
        out_shape=tuple(pltpu.HBM(o.shape, o.dtype) for o in outs),
        in_specs=[hbm] * n,
        out_specs=(hbm,) * m,
        scratch_shapes=[pltpu.VMEM(arrays[i].shape, arrays[i].dtype) for i in kept]
        + [pltpu.VMEM(o.shape, o.dtype) for o in outs]
        + [pltpu.SemaphoreType.DMA((n + m,))]
        + list(scratch),
        cost_estimate=pl.CostEstimate(flops=flops, transcendentals=0, bytes_accessed=1 << 20),
        compiler_params=pltpu.CompilerParams(vmem_limit_bytes=limit << 20),
        interpret=INTERPRET,
    )(*(a if i in free else pltpu.with_memory_space_constraint(a, pltpu.HBM) for i, a in enumerate(arrays)))
    return got if m > 1 else got[0]


def shape(dims, dtype):
    return jax.ShapeDtypeStruct(dims, dtype)


def split2(v):
    hi = v.astype(bf16)
    return hi, (v - hi.astype(f32)).astype(bf16)


def mm(a, b):
    return jnp.dot(a, b, preferred_element_type=f32)


def mm_t(a, b):
    return lax.dot_general(a, b, (((1,), (1,)), ((), ())), preferred_element_type=f32)


def norm_body(tok_ref, gain_ref, forget_ref, off_ref, out_ref):
    v = tok_ref[0].astype(f32)
    scale = lax.rsqrt(jnp.mean(v * v, axis=1, keepdims=True) + epsilon)
    normed = (v * scale * gain_ref[...]).astype(bf16)
    hi, lo = split2(forget_ref[...])
    hi, lo = hi.astype(f32), lo.astype(f32)
    off = off_ref[...].astype(f32)
    blank = jnp.zeros((6, BLOCK), f32)
    for k in range(4):
        out_ref[k, :64, :] = normed
        for j in range(16):
            row = hi[8 * k + j : 8 * k + j + 1] if j < 8 else lo[8 * k + j - 8 : 8 * k + j - 7]
            last = off[k : k + 1] if j == 0 else jnp.zeros((1, BLOCK), f32)
            tile = jnp.concatenate([row, last, blank], axis=0)
            out_ref[k, 64:, j * BLOCK : (j + 1) * BLOCK] = tile.astype(bf16)


def normalize(tokens, gain, forget, offset):
    return staged(
        norm_body,
        [shape((4, 64 + MORE, 2048), bf16)],
        [tokens, gain.reshape(1, -1), forget, offset],
        flops=10**6,
    )


def pack_body(k_ref, v_ref, q_ref, d_ref, kv_out, qd_out, kv_buf, qd_buf, sems):
    at = pl.ds(pl.multiple_of(lax.axis_index("y") * BLOCK, BLOCK), BLOCK)
    arrive = []
    for n, (ref, buf, h) in enumerate(
        ((k_ref, kv_buf, 0), (v_ref, kv_buf, 1), (q_ref, qd_buf, 0), (d_ref, qd_buf, 1))
    ):
        arrive.append(
            pltpu.make_async_copy(ref.at[:, at], buf.at[:, pl.ds(h * BLOCK, BLOCK)], sems.at[n])
        )
    for copy in arrive:
        copy.start()
    leave = []
    for part, (buf, out) in enumerate(((kv_buf, kv_out), (qd_buf, qd_out))):
        arrive[2 * part].wait()
        arrive[2 * part + 1].wait()
        for k in range(4):
            copy = pltpu.make_async_copy(buf, out.at[k], sems.at[4 + 4 * part + k])
            copy.start()
            leave.append(copy)
    for copy in leave:
        copy.wait()


def pack(*weights):
    anywhere = pl.BlockSpec(memory_space=pltpu.HBM)
    packed = pltpu.HBM((4, ROWS, 2 * BLOCK), bf16)
    return pl.pallas_call(
        pack_body,
        out_shape=(packed, packed),
        in_specs=[anywhere] * 4,
        out_specs=(anywhere, anywhere),
        scratch_shapes=[pltpu.VMEM((ROWS, 2 * BLOCK), bf16)] * 2 + [pltpu.SemaphoreType.DMA((12,))],
        interpret=INTERPRET,
        name="pack",
    )(*(pltpu.with_memory_space_constraint(a, pltpu.HBM) for a in weights))


def rows_copies(mine, theirs, rows, sems):
    c = lax.axis_index("c")
    copies = []
    for b in range(4):
        for part, ref in enumerate((mine, theirs)):
            at = pl.multiple_of(b * BLOCK + ((c + part) % 2) * 64, 64)
            copies.append(
                pltpu.make_async_copy(ref.at[b, pl.ds(0, 64)], rows.at[pl.ds(at, 64)], sems.at[2 * b + part])
            )
    return copies


ROWS_SCRATCH = [pltpu.VMEM((ROWS, 2048), bf16), pltpu.SemaphoreType.DMA((12,)), pltpu.VMEM((4, MORE, 2048), bf16)]


def kv_body(ready, send, mine, theirs, w_ref, kv_ref, rows, sems, more):
    copies = rows_copies(mine, theirs, rows, sems)
    for b in range(4):
        copies.append(
            pltpu.make_async_copy(mine.at[b, pl.ds(64, MORE)], more.at[b], sems.at[8 + b])
        )
    for copy in copies:
        copy.start()
    for copy in copies:
        copy.wait()
    ready(2)
    offs = [more[b].astype(f32)[1:2, :BLOCK] for b in range(4)]
    row0 = jnp.concatenate(offs[:2], axis=1)
    row1 = jnp.concatenate(offs[2:], axis=1)
    tail = jnp.concatenate([row0, row1, jnp.zeros((EXTRA - 2, 256), f32)], axis=0)
    kv_ref[ROWS:, :] = tail.astype(bf16)
    kv_ref[:ROWS, :] = mm(rows[...], w_ref[...]).astype(bf16)


def project_kv(mine, theirs, weights):
    return staged(
        kv_body,
        [shape((ROWS + EXTRA, 256), bf16)],
        [mine, theirs, weights],
        ROWS_SCRATCH,
        flops=2 * ROWS * 2048 * 256,
        lazy=True,
        raw=(0, 1),
        free=(0, 1, 2),
    )


SPAN = 256
TILE = 32
WIDE = SPAN + BLOCK


def chunk(q_ref, kv_ref, acc_ref, fall_ref, scr, diagonal):
    s_ref, soft_ref, r_ref, w_ref, tri_ref = scr
    j = lax.broadcasted_iota(jnp.int32, (SPAN, WIDE), 0)
    k = lax.broadcasted_iota(jnp.int32, (SPAN, WIDE), 1)
    tri_ref[...] = jnp.where((j > k) | (k >= SPAN), 1.0, 0.0).astype(bf16)
    offs = kv_ref[ROWS : ROWS + EXTRA, :].astype(f32)
    off = jnp.concatenate([offs[0:1], offs[1:2]], axis=1) * LOG2E
    s_ref[...] = mm_t(q_ref[...], kv_ref[:ROWS, :BLOCK])

    def visible(i):
        t = lax.broadcasted_iota(jnp.int32, (TILE, ROWS), 0) + i * TILE
        s = lax.broadcasted_iota(jnp.int32, (TILE, ROWS), 1)
        return s < t

    def first(i, _):
        at = pl.ds(pl.multiple_of(i * TILE, TILE), TILE)
        z = s_ref[at, :] * SCORE + off
        soft = jnp.maximum(z, 0.0) + jnp.log2(1.0 + jnp.exp2(-jnp.abs(z)))
        s_ref[at, :] = z - soft
        if diagonal:
            soft = jnp.where(visible(i), soft, 0.0)
        soft_ref[at, :] = soft.astype(bf16)
        return 0

    lax.fori_loop(0, ROWS // TILE, first, 0, unroll=2)
    for blk in range(2):
        r_ref[:, blk * WIDE : (blk + 1) * WIDE] = mm(
            soft_ref[:, blk * SPAN : (blk + 1) * SPAN], tri_ref[...]
        )

    def second(i, _):
        at = pl.ds(pl.multiple_of(i * TILE, TILE), TILE)
        fall1 = fall_ref[at, :]
        fall0 = fall1 + r_ref[at, WIDE + SPAN :]
        fall_ref[at, :] = fall0 + r_ref[at, SPAN:WIDE]
        behind = jnp.concatenate(
            [
                r_ref[at, :BLOCK] + fall0,
                r_ref[at, BLOCK:SPAN] + fall0,
                r_ref[at, WIDE : WIDE + BLOCK] + fall1,
                r_ref[at, WIDE + BLOCK : WIDE + SPAN] + fall1,
            ],
            axis=1,
        )
        w = jnp.exp2(s_ref[at, :] - behind)
        if diagonal:
            w = jnp.where(visible(i), w, 0.0)
        w_ref[at, :] = w.astype(bf16)
        return 0

    lax.fori_loop(0, ROWS // TILE, second, 0, unroll=2)
    acc_ref[...] += mm(w_ref[...], kv_ref[:ROWS, BLOCK:])


ATTEND_SCRATCH = [
    pltpu.VMEM((ROWS, ROWS), f32),
    pltpu.VMEM((ROWS, ROWS), bf16),
    pltpu.VMEM((ROWS, 2 * WIDE), f32),
    pltpu.VMEM((ROWS, ROWS), bf16),
    pltpu.VMEM((SPAN, WIDE), bf16),
]
PAIR = (shape((ROWS, BLOCK), f32), shape((ROWS, BLOCK), f32))
ATTEND_FLOPS = 8 * ROWS * ROWS * BLOCK


def attend_near(q, kv, up, down):
    def body(ready, send, q_ref, kv_ref, up_ref, down_ref, acc_ref, fall_ref, far_ref, low_ref, *scr):
        z = lax.axis_index("z")
        acc_ref[...] = jnp.zeros((ROWS, BLOCK), f32)
        fall_ref[...] = jnp.zeros((ROWS, BLOCK), f32)
        far_ref[...] = jnp.zeros((ROWS, BLOCK), f32)
        ready(0, 1)
        chunk(q_ref, kv_ref, acc_ref, fall_ref, scr, True)
        ready(2, 3)

        @pl.when(z >= 1)
        def _():
            chunk(q_ref, up_ref, acc_ref, fall_ref, scr, False)

        @pl.when(z >= 7)
        def _():
            low_ref[...] = jnp.zeros((ROWS, BLOCK), f32)
            chunk(q_ref, down_ref, far_ref, low_ref, scr, False)

    return staged(
        body,
        PAIR + PAIR[:1],
        [q, kv, up, down],
        [pltpu.VMEM((ROWS, BLOCK), f32)] + ATTEND_SCRATCH,
        flops=3 * ATTEND_FLOPS,
        lazy=True,
        free=(2, 3),
    )


def attend_middle(q, acc, fall, far, ups, downs):
    def body(
        ready, send, q_ref, acc_in, fall_in, far_in, up2, down2, up3, down3,
        acc_ref, fall_ref, far_ref, low_ref, *scr,
    ):
        z = lax.axis_index("z")
        ready(0, 1, 2, 3)
        acc_ref[...] = acc_in[...]
        fall_ref[...] = fall_in[...]
        for k, (up_ref, down_ref) in ((2, (up2, down2)), (3, (up3, down3))):
            ready(2 * k, 2 * k + 1)

            @pl.when(z >= k)
            def _(up_ref=up_ref):
                chunk(q_ref, up_ref, acc_ref, fall_ref, scr, False)

            before = far_in if k == 2 else far_ref

            @pl.when(z + k >= 8)
            def _(down_ref=down_ref, before=before):
                low_ref[...] = jnp.zeros((ROWS, BLOCK), f32)
                part_ref = acc_in
                part_ref[...] = jnp.zeros((ROWS, BLOCK), f32)
                chunk(q_ref, down_ref, part_ref, low_ref, scr, False)
                far_ref[...] = part_ref[...] + jnp.exp2(-low_ref[...]) * before[...]

            if k == 2:

                @pl.when(z + k < 8)
                def _():
                    far_ref[...] = far_in[...]

    return staged(
        body,
        PAIR + PAIR[:1],
        [q, acc, fall, far, ups[2], downs[2], ups[3], downs[3]],
        [pltpu.VMEM((ROWS, BLOCK), f32)] + ATTEND_SCRATCH,
        flops=4 * ATTEND_FLOPS,
        lazy=True,
        free=(4, 5, 6, 7),
    )


def attend_last(q, kv, acc, fall, far, scan_out):
    def body(q_ref, kv_ref, acc_ref, fall_ref, far_ref, scan_ref, out_ref, *scr):
        @pl.when(lax.axis_index("z") >= 4)
        def _():
            chunk(q_ref, kv_ref, acc_ref, fall_ref, scr, False)

        out_ref[:, :BLOCK] = scan_ref[...]
        out_ref[:, BLOCK:] = (acc_ref[...] + jnp.exp2(-fall_ref[...]) * far_ref[...]).astype(bf16)

    return staged(
        body,
        [shape((ROWS, 2 * BLOCK), bf16)],
        [q, kv, acc, fall, far, scan_out],
        ATTEND_SCRATCH,
        flops=ATTEND_FLOPS,
        free=(1,),
    )


N = 512


def cmul(ar, ai, br, bi):
    return ar * br - ai * bi, ar * bi + ai * br


def tables_body(
    in_ref, out_ref, lam_r_ref, lam_i_ref, step_ref, start_ref, skip_in,
    pow_ref, inv_ref, b_ref, ct_ref, init_ref, skip_ref,
):
    y = lax.axis_index("y")
    own = pl.ds(pl.multiple_of(y * 8, 8), 8)
    copy = (
        lax.broadcasted_iota(jnp.int32, (64, N), 1) % 64 == lax.broadcasted_iota(jnp.int32, (64, N), 0)
    ).astype(f32)

    def tiled(a, height):
        rows, width = a.shape
        r = lax.broadcasted_iota(jnp.int32, (rows, N), 0) // height
        k = lax.broadcasted_iota(jnp.int32, (rows, N), 1) // width
        spread = jnp.dot(a, copy, precision=lax.Precision.HIGHEST, preferred_element_type=f32)
        return jnp.where(r == k, spread, 0.0)

    def line(a):
        return jnp.sum(tiled(a, 1), axis=0, keepdims=True)

    lam_r, lam_i, step = line(lam_r_ref[own]), line(lam_i_ref[own]), jnp.exp(line(step_ref[own]))
    init_ref[0:1, :] = line(start_ref[0, 0, own])
    init_ref[1:2, :] = line(start_ref[1, 0, own])
    skip_ref[...] = skip_in[:, pl.ds(pl.multiple_of(y * BLOCK, BLOCK), BLOCK)]
    gain = lam_r * step
    turn = lam_i * step
    size = jnp.exp(gain)
    bar_r = size * jnp.cos(turn)
    bar_i = size * jnp.sin(turn)
    over = lam_r * lam_r + lam_i * lam_i
    less = bar_r - 1.0
    factor_r = (less * lam_r + bar_i * lam_i) / over
    factor_i = (bar_i * lam_r - less * lam_i) / over
    count = lax.broadcasted_iota(jnp.int32, (BLOCK, N), 0) + 1
    pr = jnp.ones((BLOCK, N), f32)
    pi = jnp.zeros((BLOCK, N), f32)
    sr, si = bar_r, bar_i
    for bit in range(8):
        on = ((count >> bit) & 1) == 1
        nr, ni = cmul(pr, pi, sr, si)
        pr, pi = jnp.where(on, nr, pr), jnp.where(on, ni, pi)
        if bit < 7:
            sr, si = cmul(sr, si, sr, si)
    back = jnp.exp(-2.0 * count.astype(f32) * gain)
    pow_ref[:BLOCK, :] = pr
    pow_ref[BLOCK:, :] = pi
    br, bi = cmul(pr * back, -pi * back, factor_r, factor_i)
    inv_ref[:BLOCK, :] = br
    inv_ref[BLOCK:, :] = bi
    for p in range(2):
        b_ref[:, p * N : (p + 1) * N] = tiled(in_ref[p, own].reshape(BLOCK, 64), 16).astype(bf16)
        sign = 1.0 if p == 0 else -1.0
        ct_ref[:, p * N : (p + 1) * N] = (sign * tiled(out_ref[p, own].reshape(BLOCK, 64), 16)).astype(bf16)


def scan_tables(*arrays):
    return staged(
        tables_body,
        (
            shape((2 * BLOCK, N), f32),
            shape((2 * BLOCK, N), f32),
            shape((BLOCK, 2 * N), bf16),
            shape((BLOCK, 2 * N), bf16),
            shape((2, N), f32),
            shape((1, BLOCK), f32),
        ),
        arrays,
        flops=10**9,
    )


def scan_body(
    ready, send, mine, theirs, w_ref, pow_ref, inv_ref, b_ref, ct_ref, skip_ref,
    q_ref, y_ref, ef_ref, hop_ref, sum_ref, all_rows, sems, more, u_ref, f_ref,
):
    copies = rows_copies(mine, theirs, all_rows, sems)
    for b in range(4):
        copies.append(
            pltpu.make_async_copy(mine.at[b, pl.ds(64, MORE)], more.at[b], sems.at[8 + b])
        )
    for copy in copies:
        copy.start()
    for copy in copies:
        copy.wait()
    ready(2)
    both = mm(all_rows[...], w_ref[...])
    q_ref[...] = both[:, :BLOCK].astype(bf16)
    u_ref[...] = both[:, BLOCK:].astype(bf16)
    send(0)
    for b in range(4):
        part = more[b].astype(f32)
        part = part[0:1, : 8 * BLOCK] + part[0:1, 8 * BLOCK :]
        f_ref[:, b * BLOCK : (b + 1) * BLOCK] = jnp.concatenate(
            [part[:, g * BLOCK : (g + 1) * BLOCK] for g in range(8)], axis=0
        )
    ready(3, 4, 5, 6, 7)
    row = lax.broadcasted_iota(jnp.int32, (BLOCK, BLOCK), 0)
    col = lax.broadcasted_iota(jnp.int32, (BLOCK, BLOCK), 1)
    low = (col <= row).astype(bf16)
    low32 = (col <= row).astype(f32)
    even = lax.broadcasted_iota(jnp.int32, (1, BLOCK), 1) < 64

    def block(b, state):
        carry_r, carry_i, hop_r, hop_i = state
        rows = pl.ds(pl.multiple_of(b * BLOCK, BLOCK), BLOCK)
        f = f_ref[:, rows]
        f_all = jnp.concatenate([jnp.broadcast_to(f[g : g + 1], (16, BLOCK)) for g in range(8)], axis=0)
        cum_f = lax.dot_general(
            low32, f_all, (((1,), (1,)), ((), ())), precision=lax.Precision.HIGHEST, preferred_element_type=f32
        )
        ef = jnp.exp(cum_f)
        ef_ref[rows, :] = ef
        u = u_ref[rows, :].astype(f32)
        drive = mm((u * jnp.exp(-cum_f)).astype(bf16), b_ref[...])
        dr, di = cmul(drive[:, :N], drive[:, N:], inv_ref[:BLOCK, :], inv_ref[BLOCK:, :])
        tr = mm(low, dr.astype(bf16)) + carry_r
        ti = mm(low, di.astype(bf16)) + carry_i
        st_r, st_i = cmul(pow_ref[:BLOCK, :], pow_ref[BLOCK:, :], tr, ti)
        out = mm_t(st_r.astype(bf16), ct_ref[:, :N]) + mm_t(st_i.astype(bf16), ct_ref[:, N:])
        y_ref[rows, :] = ef * out + skip_ref[...] * u
        total = jnp.exp(jnp.broadcast_to(jnp.sum(f, axis=1, keepdims=True), (8, BLOCK)))
        keep = jnp.concatenate(
            [jnp.where(even, total[2 * g : 2 * g + 1], total[2 * g + 1 : 2 * g + 2]) for g in range(4)], axis=1
        )
        hop_ref[pl.ds(pl.multiple_of(b * 8, 8), 8), :] = jnp.concatenate(
            [hop_r, hop_i, jnp.zeros((6, N), f32)], axis=0
        )
        nr, ni = cmul(hop_r, hop_i, pow_ref[BLOCK - 1 : BLOCK, :], pow_ref[2 * BLOCK - 1 :, :])
        return keep * st_r[BLOCK - 1 :, :], keep * st_i[BLOCK - 1 :, :], keep * nr, keep * ni

    zero = jnp.zeros((1, N), f32)
    carry_r, carry_i, hop_r, hop_i = lax.fori_loop(
        0, ROWS // BLOCK, block, (zero, zero, zero + 1.0, zero)
    )
    total = jnp.concatenate([carry_r, carry_i, hop_r, hop_i, jnp.zeros((4, N), f32)], axis=0)
    for k in range(8):
        sum_ref[k] = total


def scan_local(*arrays):
    return staged(
        scan_body,
        (
            shape((ROWS, BLOCK), bf16),
            shape((ROWS, BLOCK), f32),
            shape((ROWS, BLOCK), f32),
            shape((32, N), f32),
            shape((8, 8, N), f32),
        ),
        arrays,
        ROWS_SCRATCH + [pltpu.VMEM((ROWS, BLOCK), bf16), pltpu.VMEM((8, ROWS), f32)],
        flops=5 * 10**9,
        lazy=True,
        raw=(0, 1),
        free=(0, 1, 2),
    )


def finish_body(y_ref, ef_ref, pow_ref, hop_ref, all_ref, init_ref, ct_ref, out_ref):
    z = lax.axis_index("z")
    sr, si = init_ref[0:1, :], init_ref[1:2, :]
    for j in range(7):
        part = all_ref[j]
        nr, ni = cmul(part[2:3], part[3:4], sr, si)
        sr = jnp.where(j < z, nr + part[0:1], sr)
        si = jnp.where(j < z, ni + part[1:2], si)

    def block(b, _):
        rows = pl.ds(pl.multiple_of(b * BLOCK, BLOCK), BLOCK)
        hop = hop_ref[pl.ds(pl.multiple_of(b * 8, 8), 8), :]
        er, ei = cmul(hop[0:1], hop[1:2], sr, si)
        gr, gi = cmul(pow_ref[:BLOCK, :], pow_ref[BLOCK:, :], er, ei)
        more = mm_t(gr.astype(bf16), ct_ref[:, :N]) + mm_t(gi.astype(bf16), ct_ref[:, N:])
        v = y_ref[rows, :] + ef_ref[rows, :] * more
        inner = math.sqrt(2.0 / math.pi) * (v + 0.044715 * v * v * v)
        out_ref[rows, :] = (0.5 * v * (1.0 + jnp.tanh(inner))).astype(bf16)
        return 0

    lax.fori_loop(0, ROWS // BLOCK, block, 0)


def scan_finish(*arrays):
    return staged(finish_body, [shape((ROWS, BLOCK), bf16)], arrays, flops=2 * 10**9, free=(4,))


def out_body(recv_ref, own, up, down, far0, far1, keep_ref, send_ref, lhs_ref, sum_ref):
    x, c = lax.axis_index("x"), lax.axis_index("c")
    for k in range(4):
        lhs_ref[:, k * BLOCK : (k + 1) * BLOCK] = recv_ref[k, :, :BLOCK]
        lhs_ref[:, ROWS + k * BLOCK : ROWS + (k + 1) * BLOCK] = recv_ref[k, :, BLOCK:]
    for piece, step in ((own, 0), (up, 3), (down, 1), (None, 2)):
        if step == 2:
            total = mm(lhs_ref[:, :ROWS], far0[...]) + mm(lhs_ref[:, ROWS:], far1[...])
        else:
            total = mm(lhs_ref[...], piece[...])
        sum_ref[:, pl.ds(pl.multiple_of(((x + step) % 4) * ROWS, ROWS), ROWS)] = total
    keep_ref[...] = sum_ref[pl.ds(pl.multiple_of(c * 64, 64), 64), :]
    send_ref[...] = sum_ref[pl.ds(pl.multiple_of((1 - c) * 64, 64), 64), :].astype(bf16)


def project_out(recv, pieces):
    return staged(
        out_body,
        (shape((64, 2048), f32), shape((64, 2048), bf16)),
        [recv, *pieces],
        [pltpu.VMEM((BLOCK, 1024), bf16), pltpu.VMEM((BLOCK, 2048), f32)],
        flops=BLOCK * 1024 * 2048 * 2,
        free=range(6),
    )


def shift(a, axis, by):
    n = lax.axis_size(axis)
    return lax.ppermute(a, axis, [(i, (i + by) % n) for i in range(n)])


def ring4(a, axis, cut):
    up = shift(a, axis, 1)
    down = shift(a, axis, -1)
    far0 = shift(up[:cut], axis, 1)
    far1 = shift(down[cut:], axis, -1)
    return [a, up, down, far0, far1]


def after(a, b):
    return lax.optimization_barrier((a, b))[0]


def on_device(
    tokens,
    norm_gain,
    drive_weight,
    query_weight,
    key_weight,
    value_weight,
    key_offset,
    log_step,
    lambda_real,
    lambda_imag,
    input_map,
    output_map,
    skip_gain,
    forget,
    initial_state,
    scan_out_weight,
    attend_out_weight,
):
    def exchange(a, axis):
        return lax.all_to_all(a, axis, split_axis=0, concat_axis=0, tiled=True)

    kv_columns, qd_columns = pack(key_weight, value_weight, query_weight, drive_weight)
    w_kv = exchange(kv_columns, "x").reshape(2048, 2 * BLOCK)
    normed = normalize(tokens, norm_gain, forget[:, 0, :], key_offset[:, 0, :])
    mine = exchange(normed, "y")
    theirs = shift(mine, "c", 1)
    w_qd = exchange(after(qd_columns, w_kv), "x")
    tables = scan_tables(
        input_map.transpose(0, 1, 3, 2),
        output_map,
        lambda_real,
        lambda_imag,
        jnp.broadcast_to(log_step[:, None], lambda_real.shape),
        initial_state,
        skip_gain.reshape(1, -1),
    )
    out_rows = jnp.concatenate([scan_out_weight, attend_out_weight], axis=0)
    theirs, tables, out_rows = lax.optimization_barrier((theirs, tables, out_rows))
    power, inverse, b_map, c_map, init, skip = tables
    kv = project_kv(mine, theirs, w_kv)

    ups, downs = [kv], [kv]
    for k in range(1, 5):
        ups.append(shift(ups[-1], "z", 1))
        if k < 4:
            downs.append(shift(downs[-1], "z", -1))

    q, y_local, ef, hop, summary = scan_local(
        mine, theirs, w_qd.reshape(2048, 2 * BLOCK), power, inverse, b_map, c_map, skip
    )
    out_pieces = ring4(after(out_rows, q), "x", 512)
    everyone = exchange(summary, "z")
    acc, fall, far = attend_near(q, kv, ups[1], downs[1])
    scan_out = scan_finish(y_local, ef, power, hop, everyone, init, c_map)
    acc, fall, far = attend_middle(q, acc, fall, far, ups, downs)
    both = attend_last(q, ups[4], acc, fall, far, scan_out)
    recv = exchange(both.reshape(4, BLOCK, 2 * BLOCK), "y")
    keep, send = project_out(recv, out_pieces)
    return (keep + shift(send, "c", 1).astype(f32)).astype(bf16)[None]


def solution(mesh):
    split = Mesh(
        mesh.devices.reshape(8, 4, mesh.shape["fs"], mesh.shape["tp"]), ("z", "y", "x", "c")
    )
    in_specs = (
        P("x", SP_TP, None),
        P(),
        P("x", "c"),
        P("x", "c"),
        P("x", "c"),
        P("x", "c"),
        P("c", "x", SP),
        P("c"),
        P("c", None),
        P("c", None),
        P(None, "c", None, None),
        P(None, "c", None, None),
        P("c"),
        P("c", "x", SP),
        P(None, "x", "c", None),
        P("c", "x"),
        P("c", "x"),
    )
    out_specs = P("x", SP_TP, None)

    return jax.shard_map(
        on_device, mesh=split, in_specs=in_specs, out_specs=out_specs, check_vma=False
    )
```

```python
import math

import jax
import jax.numpy as jnp
from jax import lax
from jax.experimental import pallas as pl
from jax.experimental.pallas import tpu as pltpu
from jax.sharding import Mesh
from jax.sharding import PartitionSpec as P


HEAD_DIM = 128
BLOCK = 128
ROWS = 512
EXTRA = 16
MORE = 8
SP = ("z", "y")
SP_TP = ("z", "y", "c")
LOG2E = 1.4426950408889634
SCORE = HEAD_DIM ** (-0.5) * LOG2E
epsilon = 1e-06
f32 = jnp.float32
bf16 = jnp.bfloat16
INTERPRET = False


def staged(body, outs, arrays, scratch=(), flops=0, limit=20, lazy=False, raw=(), free=(), vin=(), vout=(), alias=()):
    n, m = len(arrays), len(outs)
    kept = [i for i in range(n) if i not in raw]

    def kernel(*refs):
        nv, mv = len(vin), len(vout)
        src, near_in = refs[:n], refs[n : n + nv]
        refs = refs[n + nv :]
        dst, near_out = refs[:m], refs[m : m + mv]
        refs = refs[m + mv :]
        bufs = dict(zip(kept, refs[: len(kept)]))
        results = refs[len(kept) : len(kept) + m]
        sems, rest = refs[len(kept) + m], refs[len(kept) + m + 1 :]
        copies = {i: pltpu.make_async_copy(src[i], bufs[i], sems.at[i]) for i in kept}
        for i in kept:
            copies[i].start()
        leaving = {}

        def ready(*which):
            for i in which:
                copies[i].wait()

        def send(i):
            leaving[i] = pltpu.make_async_copy(results[i], dst[i], sems.at[n + i])
            leaving[i].start()

        ins = [bufs.get(i, src[i]) for i in range(n)]
        if lazy:
            body(ready, send, *ins, *near_in, *results, *near_out, *rest)
        else:
            ready(*kept)
            body(*ins, *near_in, *results, *near_out, *rest)
        for i in range(m):
            if i not in leaving:
                send(i)
        for i in range(m):
            leaving[i].wait()

    hbm = pl.BlockSpec(memory_space=pltpu.HBM)
    near = pl.BlockSpec(memory_space=pltpu.VMEM)
    got = pl.pallas_call(
        kernel,
        out_shape=tuple(pltpu.HBM(o.shape, o.dtype) for o in outs) + tuple(vout),
        in_specs=[hbm] * n + [near] * len(vin),
        out_specs=(hbm,) * m + (near,) * len(vout),
        input_output_aliases={n + i: m + o for i, o in alias},
        scratch_shapes=[pltpu.VMEM(arrays[i].shape, arrays[i].dtype) for i in kept]
        + [pltpu.VMEM(o.shape, o.dtype) for o in outs]
        + [pltpu.SemaphoreType.DMA((n + m,))]
        + list(scratch),
        cost_estimate=pl.CostEstimate(flops=flops, transcendentals=0, bytes_accessed=1 << 20),
        compiler_params=pltpu.CompilerParams(vmem_limit_bytes=limit << 20),
        interpret=INTERPRET,
    )(*(a if i in free else pltpu.with_memory_space_constraint(a, pltpu.HBM) for i, a in enumerate(arrays)), *vin)
    return got if len(got) > 1 else got[0]


def shape(dims, dtype):
    return jax.ShapeDtypeStruct(dims, dtype)


def split2(v):
    hi = v.astype(bf16)
    return hi, (v - hi.astype(f32)).astype(bf16)


def mm(a, b):
    return jnp.dot(a, b, preferred_element_type=f32)


def mm_t(a, b):
    return lax.dot_general(a, b, (((1,), (1,)), ((), ())), preferred_element_type=f32)


def norm_body(
    ready, send, tok_ref, gain_ref, forget_ref, off_ref, k_ref, v_ref, q_ref, d_ref, out_ref, a_ref, b_ref, sems
):
    at = pl.ds(pl.multiple_of(lax.axis_index("y") * BLOCK, BLOCK), BLOCK)
    copies = []
    for n, (ref, to, h) in enumerate(((k_ref, a_ref, 0), (v_ref, a_ref, 1), (q_ref, b_ref, 0), (d_ref, b_ref, 1))):
        copies.append(pltpu.make_async_copy(ref.at[:, at], to.at[:, pl.ds(h * BLOCK, BLOCK)], sems.at[n]))
    for copy in copies:
        copy.start()
    ready(0, 1, 2, 3)
    v = tok_ref[0].astype(f32)
    scale = lax.rsqrt(jnp.mean(v * v, axis=1, keepdims=True) + epsilon)
    normed = (v * scale * gain_ref[...]).astype(bf16)
    hi, lo = split2(forget_ref[...])
    hi, lo = hi.astype(f32), lo.astype(f32)
    off = off_ref[...].astype(f32)
    blank = jnp.zeros((6, BLOCK), f32)
    for k in range(4):
        out_ref[k, :64, :] = normed
        for j in range(16):
            row = hi[8 * k + j : 8 * k + j + 1] if j < 8 else lo[8 * k + j - 8 : 8 * k + j - 7]
            last = off[k : k + 1] if j == 0 else jnp.zeros((1, BLOCK), f32)
            tile = jnp.concatenate([row, last, blank], axis=0)
            out_ref[k, 64:, j * BLOCK : (j + 1) * BLOCK] = tile.astype(bf16)
    send(0)
    for copy in copies:
        copy.wait()


def normalize(tokens, gain, forget, offset, *weights):
    return staged(
        norm_body,
        [shape((4, 64 + MORE, 2048), bf16), shape((ROWS, 256), bf16), shape((ROWS, 256), bf16)],
        [tokens, gain.reshape(1, -1), forget, offset, *weights],
        [pltpu.SemaphoreType.DMA((4,))],
        flops=10**6,
        lazy=True,
        raw=(4, 5, 6, 7),
    )


SPAN = 256
TILE = 32
WIDE = SPAN + BLOCK


def chunk(q_ref, kv_ref, acc_ref, fall_ref, scr, diagonal):
    s_ref, soft_ref, r_ref, w_ref, tri_ref = scr
    j = lax.broadcasted_iota(jnp.int32, (SPAN, WIDE), 0)
    k = lax.broadcasted_iota(jnp.int32, (SPAN, WIDE), 1)
    tri_ref[...] = jnp.where((j > k) | (k >= SPAN), 1.0, 0.0).astype(bf16)
    offs = kv_ref[ROWS : ROWS + EXTRA, :].astype(f32)
    off = jnp.concatenate([offs[0:1], offs[1:2]], axis=1) * LOG2E
    s_ref[...] = mm_t(q_ref[...], kv_ref[:ROWS, :BLOCK])

    def visible(i):
        t = lax.broadcasted_iota(jnp.int32, (TILE, ROWS), 0) + i * TILE
        s = lax.broadcasted_iota(jnp.int32, (TILE, ROWS), 1)
        return s < t

    def first(i, _):
        at = pl.ds(pl.multiple_of(i * TILE, TILE), TILE)
        z = s_ref[at, :] * SCORE + off
        soft = jnp.maximum(z, 0.0) + jnp.log2(1.0 + jnp.exp2(-jnp.abs(z)))
        s_ref[at, :] = z - soft
        if diagonal:
            soft = jnp.where(visible(i), soft, 0.0)
        soft_ref[at, :] = soft.astype(bf16)
        return 0

    lax.fori_loop(0, ROWS // TILE, first, 0, unroll=2)
    for blk in range(2):
        r_ref[:, blk * WIDE : (blk + 1) * WIDE] = mm(
            soft_ref[:, blk * SPAN : (blk + 1) * SPAN], tri_ref[...]
        )

    def second(i, _):
        at = pl.ds(pl.multiple_of(i * TILE, TILE), TILE)
        fall1 = fall_ref[at, :]
        fall0 = fall1 + r_ref[at, WIDE + SPAN :]
        fall_ref[at, :] = fall0 + r_ref[at, SPAN:WIDE]
        behind = jnp.concatenate(
            [
                r_ref[at, :BLOCK] + fall0,
                r_ref[at, BLOCK:SPAN] + fall0,
                r_ref[at, WIDE : WIDE + BLOCK] + fall1,
                r_ref[at, WIDE + BLOCK : WIDE + SPAN] + fall1,
            ],
            axis=1,
        )
        w = jnp.exp2(s_ref[at, :] - behind)
        if diagonal:
            w = jnp.where(visible(i), w, 0.0)
        w_ref[at, :] = w.astype(bf16)
        return 0

    lax.fori_loop(0, ROWS // TILE, second, 0, unroll=2)
    acc_ref[...] += mm(w_ref[...], kv_ref[:ROWS, BLOCK:])


ATTEND_SCRATCH = [
    pltpu.VMEM((ROWS, ROWS), f32),
    pltpu.VMEM((ROWS, ROWS), bf16),
    pltpu.VMEM((ROWS, 2 * WIDE), f32),
    pltpu.VMEM((ROWS, ROWS), bf16),
    pltpu.VMEM((SPAN, WIDE), bf16),
]
PAIR = (shape((ROWS, BLOCK), f32), shape((ROWS, BLOCK), f32))
ATTEND_FLOPS = 8 * ROWS * ROWS * BLOCK


def zero(ref):
    ref[...] = jnp.zeros(ref.shape, ref.dtype)


def attend_near(q, kv, up, down):
    def body(ready, send, kv_ref, up_ref, down_ref, q_ref, acc_ref, fall_ref, far_ref, low_ref, *scr):
        z = lax.axis_index("z")
        zero(acc_ref)
        zero(fall_ref)
        zero(far_ref)
        ready(0)
        chunk(q_ref, kv_ref, acc_ref, fall_ref, scr, True)
        ready(1, 2)

        @pl.when(z >= 1)
        def _():
            chunk(q_ref, up_ref, acc_ref, fall_ref, scr, False)

        @pl.when(z >= 7)
        def _():
            zero(low_ref)
            chunk(q_ref, down_ref, far_ref, low_ref, scr, False)

    return staged(
        body,
        (),
        [kv, up, down],
        [pltpu.VMEM((ROWS, BLOCK), f32)] + ATTEND_SCRATCH,
        flops=3 * ATTEND_FLOPS,
        lazy=True,
        free=(1, 2),
        vin=(q,),
        vout=PAIR + PAIR[:1],
    )


def attend_step(q, acc, fall, far, up, down, k):
    def body(ready, send, up_ref, down_ref, q_ref, _a, _b, _c, acc_ref, fall_ref, far_ref, low_ref, part_ref, *scr):
        z = lax.axis_index("z")
        ready(0, 1)

        @pl.when(z >= k)
        def _():
            chunk(q_ref, up_ref, acc_ref, fall_ref, scr, False)

        @pl.when(z + k >= 8)
        def _():
            zero(low_ref)
            zero(part_ref)
            chunk(q_ref, down_ref, part_ref, low_ref, scr, False)
            far_ref[...] = part_ref[...] + jnp.exp2(-low_ref[...]) * far_ref[...]

    return staged(
        body,
        (),
        [up, down],
        [pltpu.VMEM((ROWS, BLOCK), f32)] * 2 + ATTEND_SCRATCH,
        flops=2 * ATTEND_FLOPS,
        lazy=True,
        free=(0, 1),
        vin=(q, acc, fall, far),
        vout=PAIR + PAIR[:1],
        alias=((1, 0), (2, 1), (3, 2)),
    )


def attend_last(q, acc, fall, far, ups, downs, y, ef, power, hop, init, c_map):
    def body(
        ready, send, up4, y_ref, ef_ref, pow_ref, hop_ref, init_ref, ct_ref, *refs,
    ):
        heads = refs[:6]
        refs = refs[6:]
        q_ref, acc_in, fall_in, far_ref, out_ref, acc_ref, fall_ref, g_ref, head_ref, head_sem = refs[:10]
        scr = refs[10:]
        tails = [
            pltpu.make_async_copy(ref.at[pl.ds(ROWS + EXTRA, EXTRA)], head_ref.at[n], head_sem.at[n])
            for n, ref in enumerate(heads)
        ]
        for copy in tails:
            copy.start()
        acc_ref[...] = acc_in[...]
        fall_ref[...] = fall_in[...]
        ready(0)

        @pl.when(lax.axis_index("z") >= 4)
        def _():
            chunk(q_ref, up4, acc_ref, fall_ref, scr, False)

        for copy in tails:
            copy.wait()
        ready(1, 2, 3, 4, 5, 6)
        out_ref[:, BLOCK:] = (acc_ref[...] + jnp.exp2(-fall_ref[...]) * far_ref[...]).astype(bf16)

        def chunks(z):
            for n, k in enumerate((1, 2, 3)):
                yield head_ref[n], z + k >= 8
            yield up4[ROWS + EXTRA :, :], z >= 4
            for n, k in ((3, 3), (4, 2), (5, 1)):
                yield head_ref[n], z >= k

        out_ref[:, :BLOCK] = finish(chunks, y_ref, ef_ref, pow_ref, hop_ref, init_ref, ct_ref, g_ref)

    return staged(
        body,
        [shape((ROWS, 2 * BLOCK), bf16)],
        [ups[4], y, ef, power, hop, init, c_map, downs[1], downs[2], downs[3], ups[3], ups[2], ups[1]],
        [
            pltpu.VMEM((ROWS, BLOCK), f32),
            pltpu.VMEM((ROWS, BLOCK), f32),
            pltpu.VMEM((ROWS, 2 * N), bf16),
            pltpu.VMEM((6, EXTRA, 256), bf16),
            pltpu.SemaphoreType.DMA((6,)),
        ]
        + ATTEND_SCRATCH,
        flops=2 * ATTEND_FLOPS,
        lazy=True,
        raw=range(7, 13),
        free=(0,) + tuple(range(7, 13)),
        vin=(q, acc, fall, far),
    )


N = 512


def cmul(ar, ai, br, bi):
    return ar * br - ai * bi, ar * bi + ai * br


def tables_body(
    in_ref, out_ref, lam_r_ref, lam_i_ref, step_ref, start_ref, skip_in,
    pow_ref, inv_ref, b_ref, ct_ref, init_ref, skip_ref,
):
    y = lax.axis_index("y")
    own = pl.ds(pl.multiple_of(y * 8, 8), 8)
    copy = (
        lax.broadcasted_iota(jnp.int32, (64, N), 1) % 64 == lax.broadcasted_iota(jnp.int32, (64, N), 0)
    ).astype(f32)

    def tiled(a, height):
        rows, width = a.shape
        r = lax.broadcasted_iota(jnp.int32, (rows, N), 0) // height
        k = lax.broadcasted_iota(jnp.int32, (rows, N), 1) // width
        spread = jnp.dot(a, copy, precision=lax.Precision.HIGHEST, preferred_element_type=f32)
        return jnp.where(r == k, spread, 0.0)

    def line(a):
        return jnp.sum(tiled(a, 1), axis=0, keepdims=True)

    lam_r, lam_i, step = line(lam_r_ref[own]), line(lam_i_ref[own]), jnp.exp(line(step_ref[own]))
    init_ref[0:1, :] = line(start_ref[0, 0, own])
    init_ref[1:2, :] = line(start_ref[1, 0, own])
    skip_ref[...] = skip_in[:, pl.ds(pl.multiple_of(y * BLOCK, BLOCK), BLOCK)]
    gain = lam_r * step
    turn = lam_i * step
    size = jnp.exp(gain)
    bar_r = size * jnp.cos(turn)
    bar_i = size * jnp.sin(turn)
    over = lam_r * lam_r + lam_i * lam_i
    less = bar_r - 1.0
    factor_r = (less * lam_r + bar_i * lam_i) / over
    factor_i = (bar_i * lam_r - less * lam_i) / over
    count = lax.broadcasted_iota(jnp.int32, (BLOCK, N), 0) + 1
    pr = jnp.ones((BLOCK, N), f32)
    pi = jnp.zeros((BLOCK, N), f32)
    sr, si = bar_r, bar_i
    for bit in range(8):
        on = ((count >> bit) & 1) == 1
        nr, ni = cmul(pr, pi, sr, si)
        pr, pi = jnp.where(on, nr, pr), jnp.where(on, ni, pi)
        if bit < 7:
            sr, si = cmul(sr, si, sr, si)
    back = jnp.exp(-2.0 * count.astype(f32) * gain)
    pow_ref[:BLOCK, :] = pr
    pow_ref[BLOCK:, :] = pi
    br, bi = cmul(pr * back, -pi * back, factor_r, factor_i)
    inv_ref[:BLOCK, :] = br
    inv_ref[BLOCK:, :] = bi
    for p in range(2):
        b_ref[:, p * N : (p + 1) * N] = tiled(in_ref[p, own].reshape(BLOCK, 64), 16).astype(bf16)
        sign = 1.0 if p == 0 else -1.0
        ct_ref[:, p * N : (p + 1) * N] = (sign * tiled(out_ref[p, own].reshape(BLOCK, 64), 16)).astype(bf16)


def scan_tables(*arrays):
    return staged(
        tables_body,
        (
            shape((2 * BLOCK, N), f32),
            shape((2 * BLOCK, N), f32),
            shape((BLOCK, 2 * N), bf16),
            shape((BLOCK, 2 * N), bf16),
            shape((2, N), f32),
            shape((1, BLOCK), f32),
        ),
        arrays,
        flops=10**9,
    )


DEEP = ROWS + 2 * EXTRA


def project_body(
    ready, send, mine, theirs, a0, a3, a1, a2, b0, b3, b1, b2, pow_ref, inv_ref, b_ref, ct_ref, skip_ref,
    kv_ref, y_ref, ef_ref, hop_ref, q_ref,
    rows, sems, more, u_ref, f_ref, x_ref, st_ref, w_ref,
):
    c = lax.axis_index("c")
    x = lax.axis_index("x")
    copies = []
    for n, (step, ref) in enumerate(((0, a0), (3, a3), (1, a1), (2, a2), (0, b0), (3, b3), (1, b1), (2, b2))):
        at = pl.multiple_of(((x + step) % 4) * ROWS, ROWS)
        to = w_ref.at[pl.ds(at, ROWS), pl.ds(256 * (n // 4), 256)]
        copies.append(pltpu.make_async_copy(ref, to, sems.at[12 + n]))
    for b in range(4):
        for part, ref in enumerate((mine, theirs)):
            at = pl.multiple_of(b * BLOCK + ((c + part) % 2) * 64, 64)
            copies.append(
                pltpu.make_async_copy(ref.at[b, pl.ds(0, 64)], rows.at[pl.ds(at, 64)], sems.at[2 * b + part])
            )
    for b in range(4):
        copies.append(
            pltpu.make_async_copy(mine.at[b, pl.ds(64, MORE)], more.at[b], sems.at[8 + b])
        )
    for copy in copies:
        copy.start()
    for copy in copies:
        copy.wait()
    both = mm(rows[...], w_ref[...])
    kv_ref[:ROWS, :] = both[:, :256].astype(bf16)
    q_ref[...] = both[:, 256:384].astype(bf16)
    u_ref[...] = both[:, 384:].astype(bf16)
    offs = [more[b].astype(f32)[1:2, :BLOCK] for b in range(4)]
    row0 = jnp.concatenate(offs[:2], axis=1)
    row1 = jnp.concatenate(offs[2:], axis=1)
    tail = jnp.concatenate([row0, row1, jnp.zeros((EXTRA - 2, 256), f32)], axis=0)
    kv_ref[ROWS : ROWS + EXTRA, :] = tail.astype(bf16)
    for b in range(4):
        part = more[b].astype(f32)
        part = part[0:1, : 8 * BLOCK] + part[0:1, 8 * BLOCK :]
        f_ref[:, b * BLOCK : (b + 1) * BLOCK] = jnp.concatenate(
            [part[:, g * BLOCK : (g + 1) * BLOCK] for g in range(8)], axis=0
        )
    ready(10, 11, 12, 13, 14)
    row = lax.broadcasted_iota(jnp.int32, (BLOCK, BLOCK), 0)
    col = lax.broadcasted_iota(jnp.int32, (BLOCK, BLOCK), 1)
    low = (col <= row).astype(bf16)
    low32 = (col <= row).astype(f32)
    even = lax.broadcasted_iota(jnp.int32, (1, BLOCK), 1) < 64
    keeps = []
    blocks = [slice(b * BLOCK, (b + 1) * BLOCK) for b in range(4)]
    for at in blocks:
        f = f_ref[:, at]
        f_all = jnp.concatenate([jnp.broadcast_to(f[g : g + 1], (16, BLOCK)) for g in range(8)], axis=0)
        cum_f = lax.dot_general(
            low32, f_all, (((1,), (1,)), ((), ())), precision=lax.Precision.HIGHEST, preferred_element_type=f32
        )
        ef_ref[at, :] = jnp.exp(cum_f)
        x_ref[at, :BLOCK] = u_ref[at, :].astype(f32) * jnp.exp(-cum_f)
        total = jnp.exp(jnp.broadcast_to(jnp.sum(f, axis=1, keepdims=True), (8, BLOCK)))
        keeps.append(
            jnp.concatenate(
                [jnp.where(even, total[2 * g : 2 * g + 1], total[2 * g + 1 : 2 * g + 2]) for g in range(4)],
                axis=1,
            )
        )
    x_ref[...] = mm(x_ref[:, :BLOCK].astype(bf16), b_ref[...])
    carry_r = jnp.zeros((1, N), f32)
    carry_i = jnp.zeros((1, N), f32)
    hop_r = jnp.ones((1, N), f32)
    hop_i = jnp.zeros((1, N), f32)
    end_r, end_i = pow_ref[BLOCK - 1 : BLOCK, :], pow_ref[2 * BLOCK - 1 :, :]
    hops = []
    for at, keep in zip(blocks, keeps):
        dr, di = cmul(x_ref[at, :N], x_ref[at, N:], inv_ref[:BLOCK, :], inv_ref[BLOCK:, :])
        tr = mm(low, dr.astype(bf16)) + carry_r
        ti = mm(low, di.astype(bf16)) + carry_i
        st_r, st_i = cmul(pow_ref[:BLOCK, :], pow_ref[BLOCK:, :], tr, ti)
        st_ref[at, :N] = st_r.astype(bf16)
        st_ref[at, N:] = st_i.astype(bf16)
        carry_r, carry_i = keep * st_r[BLOCK - 1 :, :], keep * st_i[BLOCK - 1 :, :]
        hops += [hop_r, hop_i]
        nr, ni = cmul(hop_r, hop_i, end_r, end_i)
        hop_r, hop_i = keep * nr, keep * ni
    hop_ref[...] = jnp.concatenate(hops, axis=0)
    hi, lo = split2(jnp.concatenate([carry_r, carry_i, hop_r, hop_i], axis=0))
    hi, lo = hi.astype(f32), lo.astype(f32)
    kv_ref[ROWS + EXTRA :, :] = jnp.concatenate(
        [hi[:, :256], hi[:, 256:], lo[:, :256], lo[:, 256:]], axis=0
    ).astype(bf16)
    send(0)
    y_ref[...] = ef_ref[...] * mm_t(st_ref[...], ct_ref[...]) + skip_ref[...] * u_ref[...].astype(f32)


def project(*arrays):
    return staged(
        project_body,
        (
            shape((DEEP, 256), bf16),
            shape((ROWS, BLOCK), f32),
            shape((ROWS, BLOCK), f32),
            shape((8, N), f32),
        ),
        arrays,
        [
            pltpu.VMEM((ROWS, 2048), bf16),
            pltpu.SemaphoreType.DMA((20,)),
            pltpu.VMEM((4, MORE, 2048), bf16),
            pltpu.VMEM((ROWS, BLOCK), bf16),
            pltpu.VMEM((8, ROWS), f32),
            pltpu.VMEM((ROWS, 2 * N), f32),
            pltpu.VMEM((ROWS, 2 * N), bf16),
            pltpu.VMEM((2048, ROWS), bf16),
        ],
        flops=3 * 10**9,
        lazy=True,
        raw=range(10),
        free=range(10),
        vout=(shape((ROWS, BLOCK), bf16),),
        limit=32,
    )


def finish(chunks, y_ref, ef_ref, pow_ref, hop_ref, init_ref, ct_ref, g_ref):
    z = lax.axis_index("z")
    sr, si = init_ref[0:1, :], init_ref[1:2, :]
    for ref, active in chunks(z):
        part = ref.astype(f32)
        part = part[:8] + part[8:]
        part = jnp.concatenate([part[:4], part[4:]], axis=1)
        nr, ni = cmul(part[2:3], part[3:4], sr, si)
        sr = jnp.where(active, nr + part[0:1], sr)
        si = jnp.where(active, ni + part[1:2], si)
    for b in range(ROWS // BLOCK):
        at = slice(b * BLOCK, (b + 1) * BLOCK)
        er, ei = cmul(hop_ref[2 * b : 2 * b + 1, :], hop_ref[2 * b + 1 : 2 * b + 2, :], sr, si)
        gr, gi = cmul(pow_ref[:BLOCK, :], pow_ref[BLOCK:, :], er, ei)
        g_ref[at, :N] = gr.astype(bf16)
        g_ref[at, N:] = gi.astype(bf16)
    v = y_ref[...] + ef_ref[...] * mm_t(g_ref[...], ct_ref[...])
    inner = math.sqrt(2.0 / math.pi) * (v + 0.044715 * v * v * v)
    return (0.5 * v * (1.0 + jnp.tanh(inner))).astype(bf16)


def out_body(recv_ref, own, up, down, far0, far1, keep_ref, send_ref, lhs_ref, sum_ref):
    x, c = lax.axis_index("x"), lax.axis_index("c")
    for k in range(4):
        lhs_ref[:, k * BLOCK : (k + 1) * BLOCK] = recv_ref[k, :, :BLOCK]
        lhs_ref[:, ROWS + k * BLOCK : ROWS + (k + 1) * BLOCK] = recv_ref[k, :, BLOCK:]
    for piece, step in ((own, 0), (up, 3), (down, 1), (None, 2)):
        if step == 2:
            total = mm(lhs_ref[:, :ROWS], far0[...]) + mm(lhs_ref[:, ROWS:], far1[...])
        else:
            total = mm(lhs_ref[...], piece[...])
        sum_ref[:, pl.ds(pl.multiple_of(((x + step) % 4) * ROWS, ROWS), ROWS)] = total
    keep_ref[...] = sum_ref[pl.ds(pl.multiple_of(c * 64, 64), 64), :]
    send_ref[...] = sum_ref[pl.ds(pl.multiple_of((1 - c) * 64, 64), 64), :].astype(bf16)


def project_out(recv, pieces):
    return staged(
        out_body,
        (shape((64, 2048), f32), shape((64, 2048), bf16)),
        [recv, *pieces],
        [pltpu.VMEM((BLOCK, 1024), bf16), pltpu.VMEM((BLOCK, 2048), f32)],
        flops=BLOCK * 1024 * 2048 * 2,
        free=range(6),
    )


def shift(a, axis, by):
    n = lax.axis_size(axis)
    return lax.ppermute(a, axis, [(i, (i + by) % n) for i in range(n)])


def ring4(a, axis, cut):
    up = shift(a, axis, 1)
    down = shift(a, axis, -1)
    far0 = shift(up[:cut], axis, 1)
    far1 = shift(down[cut:], axis, -1)
    return [a, up, down, far0, far1]


def after(a, b):
    return lax.optimization_barrier((a, b))[0]


def on_device(
    tokens,
    norm_gain,
    drive_weight,
    query_weight,
    key_weight,
    value_weight,
    key_offset,
    log_step,
    lambda_real,
    lambda_imag,
    input_map,
    output_map,
    skip_gain,
    forget,
    initial_state,
    scan_out_weight,
    attend_out_weight,
):
    def exchange(a, axis):
        return lax.all_to_all(a, axis, split_axis=0, concat_axis=0, tiled=True)

    normed, w_a, w_b = normalize(
        tokens,
        norm_gain,
        forget[:, 0, :],
        key_offset[:, 0, :],
        key_weight,
        value_weight,
        query_weight,
        drive_weight,
    )
    a_up = shift(w_a, "x", 1)
    b_down = shift(w_b, "x", -1)
    b_up = shift(w_b, "x", 1)
    a_down = shift(w_a, "x", -1)
    a_far = shift(a_up, "x", 1)
    b_far = shift(b_down, "x", -1)
    weights = (w_a, a_up, a_down, a_far, w_b, b_up, b_down, b_far)
    mine = exchange(normed, "y")
    theirs = shift(mine, "c", 1)
    tables = scan_tables(
        input_map.transpose(0, 1, 3, 2),
        output_map,
        lambda_real,
        lambda_imag,
        jnp.broadcast_to(log_step[:, None], lambda_real.shape),
        initial_state,
        skip_gain.reshape(1, -1),
    )
    out_rows = jnp.concatenate([scan_out_weight, attend_out_weight], axis=0)
    theirs, tables, out_rows = lax.optimization_barrier((theirs, tables, out_rows))
    power, inverse, b_map, c_map, init, skip = tables
    kv, y_local, ef, hop, q = project(
        mine, theirs, *weights, power, inverse, b_map, c_map, skip
    )
    ups, downs = [kv], [kv]
    for k in range(1, 5):
        ups.append(shift(ups[-1], "z", 1))
        if k < 4:
            downs.append(shift(downs[-1], "z", -1))
    out_pieces = ring4(after(out_rows, kv), "x", 512)
    acc, fall, far = attend_near(q, kv, ups[1], downs[1])
    for k in (2, 3):
        acc, fall, far = attend_step(q, acc, fall, far, ups[k], downs[k], k)
    both = attend_last(q, acc, fall, far, ups, downs, y_local, ef, power, hop, init, c_map)
    recv = exchange(both.reshape(4, BLOCK, 2 * BLOCK), "y")
    keep, send = project_out(recv, out_pieces)
    return (keep + shift(send, "c", 1).astype(f32)).astype(bf16)[None]


def solution(mesh):
    split = Mesh(
        mesh.devices.reshape(8, 4, mesh.shape["fs"], mesh.shape["tp"]), ("z", "y", "x", "c")
    )
    in_specs = (
        P("x", SP_TP, None),
        P(),
        P("x", "c"),
        P("x", "c"),
        P("x", "c"),
        P("x", "c"),
        P("c", "x", SP),
        P("c"),
        P("c", None),
        P("c", None),
        P(None, "c", None, None),
        P(None, "c", None, None),
        P("c"),
        P("c", "x", SP),
        P(None, "x", "c", None),
        P("c", "x"),
        P("c", "x"),
    )
    out_specs = P("x", SP_TP, None)

    return jax.shard_map(on_device, mesh=split, in_specs=in_specs, out_specs=out_specs, check_vma=False)
```

```python
import math

import jax
import jax.numpy as jnp
from jax import lax
from jax.experimental import pallas as pl
from jax.experimental.pallas import tpu as pltpu
from jax.sharding import Mesh
from jax.sharding import PartitionSpec as P


HEAD_DIM = 128
BLOCK = 128
ROWS = 512
EXTRA = 16
MORE = 8
SP = ("z", "y")
SP_TP = ("z", "y", "c")
LOG2E = 1.4426950408889634
SCORE = HEAD_DIM ** (-0.5) * LOG2E
epsilon = 1e-06
f32 = jnp.float32
bf16 = jnp.bfloat16
INTERPRET = False


def staged(body, outs, arrays, scratch=(), flops=0, limit=20, lazy=False, raw=(), free=(), vin=(), vout=(), alias=()):
    n, m = len(arrays), len(outs)
    kept = [i for i in range(n) if i not in raw]

    def kernel(*refs):
        nv, mv = len(vin), len(vout)
        src, near_in = refs[:n], refs[n : n + nv]
        refs = refs[n + nv :]
        dst, near_out = refs[:m], refs[m : m + mv]
        refs = refs[m + mv :]
        bufs = dict(zip(kept, refs[: len(kept)]))
        results = refs[len(kept) : len(kept) + m]
        sems, rest = refs[len(kept) + m], refs[len(kept) + m + 1 :]
        copies = {i: pltpu.make_async_copy(src[i], bufs[i], sems.at[i]) for i in kept}
        for i in kept:
            copies[i].start()
        leaving = {}

        def ready(*which):
            for i in which:
                copies[i].wait()

        def send(i):
            leaving[i] = pltpu.make_async_copy(results[i], dst[i], sems.at[n + i])
            leaving[i].start()

        ins = [bufs.get(i, src[i]) for i in range(n)]
        if lazy:
            body(ready, send, *ins, *near_in, *results, *near_out, *rest)
        else:
            ready(*kept)
            body(*ins, *near_in, *results, *near_out, *rest)
        for i in range(m):
            if i not in leaving:
                send(i)
        for i in range(m):
            leaving[i].wait()

    hbm = pl.BlockSpec(memory_space=pltpu.HBM)
    near = pl.BlockSpec(memory_space=pltpu.VMEM)
    got = pl.pallas_call(
        kernel,
        out_shape=tuple(pltpu.HBM(o.shape, o.dtype) for o in outs) + tuple(vout),
        in_specs=[hbm] * n + [near] * len(vin),
        out_specs=(hbm,) * m + (near,) * len(vout),
        input_output_aliases={n + i: m + o for i, o in alias},
        scratch_shapes=[pltpu.VMEM(arrays[i].shape, arrays[i].dtype) for i in kept]
        + [pltpu.VMEM(o.shape, o.dtype) for o in outs]
        + [pltpu.SemaphoreType.DMA((n + m,))]
        + list(scratch),
        cost_estimate=pl.CostEstimate(flops=flops, transcendentals=0, bytes_accessed=1 << 20),
        compiler_params=pltpu.CompilerParams(vmem_limit_bytes=limit << 20),
        interpret=INTERPRET,
    )(*(a if i in free else pltpu.with_memory_space_constraint(a, pltpu.HBM) for i, a in enumerate(arrays)), *vin)
    return got if len(got) > 1 else got[0]


def shape(dims, dtype):
    return jax.ShapeDtypeStruct(dims, dtype)


def split2(v):
    hi = v.astype(bf16)
    return hi, (v - hi.astype(f32)).astype(bf16)


def mm(a, b):
    return jnp.dot(a, b, preferred_element_type=f32)


def mm_t(a, b):
    return lax.dot_general(a, b, (((1,), (1,)), ((), ())), preferred_element_type=f32)


def norm_body(
    ready, send, tok_ref, gain_ref, forget_ref, off_ref, k_ref, v_ref, q_ref, d_ref, out_ref, a_ref, b_ref, sems
):
    at = pl.ds(pl.multiple_of(lax.axis_index("y") * BLOCK, BLOCK), BLOCK)
    copies = []
    for n, (ref, to, h) in enumerate(((k_ref, a_ref, 0), (v_ref, a_ref, 1), (q_ref, b_ref, 0), (d_ref, b_ref, 1))):
        copies.append(pltpu.make_async_copy(ref.at[:, at], to.at[:, pl.ds(h * BLOCK, BLOCK)], sems.at[n]))
    for copy in copies:
        copy.start()
    ready(0, 1, 2, 3)
    v = tok_ref[0].astype(f32)
    scale = lax.rsqrt(jnp.mean(v * v, axis=1, keepdims=True) + epsilon)
    normed = (v * scale * gain_ref[...]).astype(bf16)
    hi, lo = split2(forget_ref[...])
    hi, lo = hi.astype(f32), lo.astype(f32)
    off = off_ref[...].astype(f32)
    blank = jnp.zeros((6, BLOCK), f32)
    for k in range(4):
        out_ref[k, :64, :] = normed
        for j in range(16):
            row = hi[8 * k + j : 8 * k + j + 1] if j < 8 else lo[8 * k + j - 8 : 8 * k + j - 7]
            last = off[k : k + 1] if j == 0 else jnp.zeros((1, BLOCK), f32)
            tile = jnp.concatenate([row, last, blank], axis=0)
            out_ref[k, 64:, j * BLOCK : (j + 1) * BLOCK] = tile.astype(bf16)
    send(0)
    for copy in copies:
        copy.wait()


def normalize(tokens, gain, forget, offset, *weights):
    return staged(
        norm_body,
        [shape((4, 64 + MORE, 2048), bf16), shape((ROWS, 256), bf16), shape((ROWS, 256), bf16)],
        [tokens, gain.reshape(1, -1), forget, offset, *weights],
        [pltpu.SemaphoreType.DMA((4,))],
        flops=10**6,
        lazy=True,
        raw=(4, 5, 6, 7),
    )


SPAN = 256
TILE = 32
WIDE = SPAN + BLOCK


def chunk(q_ref, kv_ref, acc_ref, fall_ref, scr, diagonal):
    s_ref, soft_ref, r_ref, w_ref, tri_ref = scr
    j = lax.broadcasted_iota(jnp.int32, (SPAN, WIDE), 0)
    k = lax.broadcasted_iota(jnp.int32, (SPAN, WIDE), 1)
    tri_ref[...] = jnp.where((j > k) | (k >= SPAN), 1.0, 0.0).astype(bf16)
    offs = kv_ref[ROWS : ROWS + EXTRA, :].astype(f32)
    off = jnp.concatenate([offs[0:1], offs[1:2]], axis=1) * LOG2E
    s_ref[...] = mm_t(q_ref[...], kv_ref[:ROWS, :BLOCK])

    def visible(i):
        t = lax.broadcasted_iota(jnp.int32, (TILE, ROWS), 0) + i * TILE
        s = lax.broadcasted_iota(jnp.int32, (TILE, ROWS), 1)
        return s < t

    def first(i, _):
        at = pl.ds(pl.multiple_of(i * TILE, TILE), TILE)
        z = s_ref[at, :] * SCORE + off
        soft = jnp.maximum(z, 0.0) + jnp.log2(1.0 + jnp.exp2(-jnp.abs(z)))
        s_ref[at, :] = z - soft
        if diagonal:
            soft = jnp.where(visible(i), soft, 0.0)
        soft_ref[at, :] = soft.astype(bf16)
        return 0

    lax.fori_loop(0, ROWS // TILE, first, 0, unroll=2)
    for blk in range(2):
        r_ref[:, blk * WIDE : (blk + 1) * WIDE] = mm(
            soft_ref[:, blk * SPAN : (blk + 1) * SPAN], tri_ref[...]
        )

    def second(i, _):
        at = pl.ds(pl.multiple_of(i * TILE, TILE), TILE)
        fall1 = fall_ref[at, :]
        fall0 = fall1 + r_ref[at, WIDE + SPAN :]
        fall_ref[at, :] = fall0 + r_ref[at, SPAN:WIDE]
        behind = jnp.concatenate(
            [
                r_ref[at, :BLOCK] + fall0,
                r_ref[at, BLOCK:SPAN] + fall0,
                r_ref[at, WIDE : WIDE + BLOCK] + fall1,
                r_ref[at, WIDE + BLOCK : WIDE + SPAN] + fall1,
            ],
            axis=1,
        )
        w = jnp.exp2(s_ref[at, :] - behind)
        if diagonal:
            w = jnp.where(visible(i), w, 0.0)
        w_ref[at, :] = w.astype(bf16)
        return 0

    lax.fori_loop(0, ROWS // TILE, second, 0, unroll=2)
    acc_ref[...] += mm(w_ref[...], kv_ref[:ROWS, BLOCK:])


ATTEND_SCRATCH = [
    pltpu.VMEM((ROWS, ROWS), f32),
    pltpu.VMEM((ROWS, ROWS), bf16),
    pltpu.VMEM((ROWS, 2 * WIDE), f32),
    pltpu.VMEM((ROWS, ROWS), bf16),
    pltpu.VMEM((SPAN, WIDE), bf16),
]
PAIR = (shape((ROWS, BLOCK), f32), shape((ROWS, BLOCK), f32))
ATTEND_FLOPS = 8 * ROWS * ROWS * BLOCK


def zero(ref):
    ref[...] = jnp.zeros(ref.shape, ref.dtype)


def attend_own(q, kv):
    def body(kv_ref, q_ref, acc_ref, fall_ref, far_ref, *scr):
        zero(acc_ref)
        zero(fall_ref)
        zero(far_ref)
        chunk(q_ref, kv_ref, acc_ref, fall_ref, scr, True)

    return staged(body, (), [kv], ATTEND_SCRATCH, flops=ATTEND_FLOPS, vin=(q,), vout=PAIR + PAIR[:1])


def attend_step(q, acc, fall, far, up, down, k):
    def body(ready, send, up_ref, down_ref, q_ref, _a, _b, _c, acc_ref, fall_ref, far_ref, low_ref, part_ref, *scr):
        z = lax.axis_index("z")
        ready(0, 1)

        @pl.when(z >= k)
        def _():
            chunk(q_ref, up_ref, acc_ref, fall_ref, scr, False)

        @pl.when(z + k >= 8)
        def _():
            zero(low_ref)
            zero(part_ref)
            chunk(q_ref, down_ref, part_ref, low_ref, scr, False)
            far_ref[...] = part_ref[...] + jnp.exp2(-low_ref[...]) * far_ref[...]

    return staged(
        body,
        (),
        [up, down],
        [pltpu.VMEM((ROWS, BLOCK), f32)] * 2 + ATTEND_SCRATCH,
        flops=2 * ATTEND_FLOPS,
        lazy=True,
        free=(0, 1),
        vin=(q, acc, fall, far),
        vout=PAIR + PAIR[:1],
        alias=((1, 0), (2, 1), (3, 2)),
    )


def attend_last(q, acc, fall, far, ups, downs, y, ef, power, hop, init, c_map):
    def body(
        ready, send, up4, y_ref, ef_ref, pow_ref, hop_ref, init_ref, ct_ref, *refs,
    ):
        heads = refs[:6]
        refs = refs[6:]
        q_ref, acc_in, fall_in, far_ref, *parts = refs[:8]
        out_ref, acc_ref, fall_ref, g_ref, head_ref, head_sem = refs[8:14]
        scr = refs[14:]
        tails = [
            pltpu.make_async_copy(ref.at[pl.ds(ROWS + EXTRA, EXTRA)], head_ref.at[n], head_sem.at[n])
            for n, ref in enumerate(heads)
        ]
        for copy in tails:
            copy.start()
        acc_ref[...] = acc_in[...]
        fall_ref[...] = fall_in[...]
        ready(0)

        @pl.when(lax.axis_index("z") >= 4)
        def _():
            chunk(q_ref, up4, acc_ref, fall_ref, scr, False)

        for copy in tails:
            copy.wait()
        ready(1, 2, 3, 4, 5, 6)
        out_ref[:, BLOCK:] = (acc_ref[...] + jnp.exp2(-fall_ref[...]) * far_ref[...]).astype(bf16)

        def chunks(z):
            for n, k in enumerate((1, 2, 3)):
                yield head_ref[n], z + k >= 8
            yield up4[ROWS + EXTRA :, :], z >= 4
            for n, k in ((3, 3), (4, 2), (5, 1)):
                yield head_ref[n], z >= k

        out_ref[:, :BLOCK] = finish(chunks, y_ref, ef_ref, pow_ref, hop_ref, init_ref, ct_ref, g_ref)
        mine = lax.axis_index("y")
        for k, part in enumerate(parts):
            part[...] = out_ref[pl.ds(pl.multiple_of(((mine + k) % 4) * BLOCK, BLOCK), BLOCK), :]

    return staged(
        body,
        [],
        [ups[4], y, ef, power, hop, init, c_map, downs[1], downs[2], downs[3], ups[3], ups[2], ups[1]],
        [
            pltpu.VMEM((ROWS, 2 * BLOCK), bf16),
            pltpu.VMEM((ROWS, BLOCK), f32),
            pltpu.VMEM((ROWS, BLOCK), f32),
            pltpu.VMEM((ROWS, 2 * N), bf16),
            pltpu.VMEM((6, EXTRA, 256), bf16),
            pltpu.SemaphoreType.DMA((6,)),
        ]
        + ATTEND_SCRATCH,
        flops=2 * ATTEND_FLOPS,
        lazy=True,
        raw=range(7, 13),
        free=(0,) + tuple(range(7, 13)),
        vin=(q, acc, fall, far),
        vout=(shape((BLOCK, 2 * BLOCK), bf16),) * 4,
    )


N = 512


def cmul(ar, ai, br, bi):
    return ar * br - ai * bi, ar * bi + ai * br


def tables_body(
    in_ref, out_ref, lam_r_ref, lam_i_ref, step_ref, start_ref, skip_in,
    pow_ref, inv_ref, b_ref, ct_ref, init_ref, skip_ref,
):
    y = lax.axis_index("y")
    own = pl.ds(pl.multiple_of(y * 8, 8), 8)
    copy = (
        lax.broadcasted_iota(jnp.int32, (64, N), 1) % 64 == lax.broadcasted_iota(jnp.int32, (64, N), 0)
    ).astype(f32)

    def tiled(a, height):
        rows, width = a.shape
        r = lax.broadcasted_iota(jnp.int32, (rows, N), 0) // height
        k = lax.broadcasted_iota(jnp.int32, (rows, N), 1) // width
        spread = jnp.dot(a, copy, precision=lax.Precision.HIGHEST, preferred_element_type=f32)
        return jnp.where(r == k, spread, 0.0)

    def line(a):
        return jnp.sum(tiled(a, 1), axis=0, keepdims=True)

    lam_r, lam_i, step = line(lam_r_ref[own]), line(lam_i_ref[own]), jnp.exp(line(step_ref[own]))
    init_ref[0:1, :] = line(start_ref[0, 0, own])
    init_ref[1:2, :] = line(start_ref[1, 0, own])
    skip_ref[...] = skip_in[:, pl.ds(pl.multiple_of(y * BLOCK, BLOCK), BLOCK)]
    gain = lam_r * step
    turn = lam_i * step
    size = jnp.exp(gain)
    bar_r = size * jnp.cos(turn)
    bar_i = size * jnp.sin(turn)
    over = lam_r * lam_r + lam_i * lam_i
    less = bar_r - 1.0
    factor_r = (less * lam_r + bar_i * lam_i) / over
    factor_i = (bar_i * lam_r - less * lam_i) / over
    count = lax.broadcasted_iota(jnp.int32, (BLOCK, N), 0) + 1
    pr = jnp.ones((BLOCK, N), f32)
    pi = jnp.zeros((BLOCK, N), f32)
    sr, si = bar_r, bar_i
    for bit in range(8):
        on = ((count >> bit) & 1) == 1
        nr, ni = cmul(pr, pi, sr, si)
        pr, pi = jnp.where(on, nr, pr), jnp.where(on, ni, pi)
        if bit < 7:
            sr, si = cmul(sr, si, sr, si)
    back = jnp.exp(-2.0 * count.astype(f32) * gain)
    pow_ref[:BLOCK, :] = pr
    pow_ref[BLOCK:, :] = pi
    br, bi = cmul(pr * back, -pi * back, factor_r, factor_i)
    inv_ref[:BLOCK, :] = br
    inv_ref[BLOCK:, :] = bi
    for p in range(2):
        b_ref[:, p * N : (p + 1) * N] = tiled(in_ref[p, own].reshape(BLOCK, 64), 16).astype(bf16)
        sign = 1.0 if p == 0 else -1.0
        ct_ref[:, p * N : (p + 1) * N] = (sign * tiled(out_ref[p, own].reshape(BLOCK, 64), 16)).astype(bf16)


def scan_tables(*arrays):
    return staged(
        tables_body,
        (
            shape((2 * BLOCK, N), f32),
            shape((2 * BLOCK, N), f32),
            shape((BLOCK, 2 * N), bf16),
            shape((BLOCK, 2 * N), bf16),
            shape((2, N), f32),
            shape((1, BLOCK), f32),
        ),
        arrays,
        flops=10**9,
    )


DEEP = ROWS + 2 * EXTRA


def project_body(
    ready, send, mine, theirs, a0, a3, a1, a2, b0, b3, b1, b2, pow_ref, inv_ref, b_ref, ct_ref, skip_ref,
    kv_ref, y_ref, ef_ref, hop_ref, q_ref,
    rows, sems, more, u_ref, f_ref, x_ref, st_ref, w_ref,
):
    c = lax.axis_index("c")
    x = lax.axis_index("x")
    copies = []
    both = None
    for n, (step, ref) in enumerate(((0, a0), (3, a3), (1, a1), (2, a2), (0, b0), (3, b3), (1, b1), (2, b2))):
        at = pl.multiple_of(((x + step) % 4) * ROWS, ROWS)
        to = w_ref.at[pl.ds(at, ROWS), pl.ds(256 * (n // 4), 256)]
        copies.append(pltpu.make_async_copy(ref, to, sems.at[12 + n]))
    for b in range(4):
        for part, ref in enumerate((mine, theirs)):
            at = pl.multiple_of(b * BLOCK + ((c + part) % 2) * 64, 64)
            copies.append(
                pltpu.make_async_copy(ref.at[b, pl.ds(0, 64)], rows.at[pl.ds(at, 64)], sems.at[2 * b + part])
            )
    for b in range(4):
        copies.append(
            pltpu.make_async_copy(mine.at[b, pl.ds(64, MORE)], more.at[b], sems.at[8 + b])
        )
    for copy in copies:
        copy.start()
    for copy in copies:
        copy.wait()
    both = mm(rows[...], w_ref[...])
    kv_ref[:ROWS, :] = both[:, :256].astype(bf16)
    q_ref[...] = both[:, 256:384].astype(bf16)
    u_ref[...] = both[:, 384:].astype(bf16)
    offs = [more[b].astype(f32)[1:2, :BLOCK] for b in range(4)]
    row0 = jnp.concatenate(offs[:2], axis=1)
    row1 = jnp.concatenate(offs[2:], axis=1)
    tail = jnp.concatenate([row0, row1, jnp.zeros((EXTRA - 2, 256), f32)], axis=0)
    kv_ref[ROWS : ROWS + EXTRA, :] = tail.astype(bf16)
    for b in range(4):
        part = more[b].astype(f32)
        part = part[0:1, : 8 * BLOCK] + part[0:1, 8 * BLOCK :]
        f_ref[:, b * BLOCK : (b + 1) * BLOCK] = jnp.concatenate(
            [part[:, g * BLOCK : (g + 1) * BLOCK] for g in range(8)], axis=0
        )
    ready(10, 11, 12, 13, 14)
    row = lax.broadcasted_iota(jnp.int32, (BLOCK, BLOCK), 0)
    col = lax.broadcasted_iota(jnp.int32, (BLOCK, BLOCK), 1)
    low = (col <= row).astype(bf16)
    low32 = (col <= row).astype(f32)
    even = lax.broadcasted_iota(jnp.int32, (1, BLOCK), 1) < 64
    keeps = []
    blocks = [slice(b * BLOCK, (b + 1) * BLOCK) for b in range(4)]
    for at in blocks:
        f = f_ref[:, at]
        f_all = jnp.concatenate([jnp.broadcast_to(f[g : g + 1], (16, BLOCK)) for g in range(8)], axis=0)
        cum_f = lax.dot_general(
            low32, f_all, (((1,), (1,)), ((), ())), precision=lax.Precision.HIGHEST, preferred_element_type=f32
        )
        ef_ref[at, :] = jnp.exp(cum_f)
        x_ref[at, :BLOCK] = u_ref[at, :].astype(f32) * jnp.exp(-cum_f)
        total = jnp.exp(jnp.broadcast_to(jnp.sum(f, axis=1, keepdims=True), (8, BLOCK)))
        keeps.append(
            jnp.concatenate(
                [jnp.where(even, total[2 * g : 2 * g + 1], total[2 * g + 1 : 2 * g + 2]) for g in range(4)],
                axis=1,
            )
        )
    x_ref[...] = mm(x_ref[:, :BLOCK].astype(bf16), b_ref[...])
    carry_r = jnp.zeros((1, N), f32)
    carry_i = jnp.zeros((1, N), f32)
    hop_r = jnp.ones((1, N), f32)
    hop_i = jnp.zeros((1, N), f32)
    end_r, end_i = pow_ref[BLOCK - 1 : BLOCK, :], pow_ref[2 * BLOCK - 1 :, :]
    hops = []
    for at, keep in zip(blocks, keeps):
        dr, di = cmul(x_ref[at, :N], x_ref[at, N:], inv_ref[:BLOCK, :], inv_ref[BLOCK:, :])
        tr = mm(low, dr.astype(bf16)) + carry_r
        ti = mm(low, di.astype(bf16)) + carry_i
        st_r, st_i = cmul(pow_ref[:BLOCK, :], pow_ref[BLOCK:, :], tr, ti)
        st_ref[at, :N] = st_r.astype(bf16)
        st_ref[at, N:] = st_i.astype(bf16)
        carry_r, carry_i = keep * st_r[BLOCK - 1 :, :], keep * st_i[BLOCK - 1 :, :]
        hops += [hop_r, hop_i]
        nr, ni = cmul(hop_r, hop_i, end_r, end_i)
        hop_r, hop_i = keep * nr, keep * ni
    hop_ref[...] = jnp.concatenate(hops, axis=0)
    hi, lo = split2(jnp.concatenate([carry_r, carry_i, hop_r, hop_i], axis=0))
    hi, lo = hi.astype(f32), lo.astype(f32)
    kv_ref[ROWS + EXTRA :, :] = jnp.concatenate(
        [hi[:, :256], hi[:, 256:], lo[:, :256], lo[:, 256:]], axis=0
    ).astype(bf16)
    send(0)
    y_ref[...] = ef_ref[...] * mm_t(st_ref[...], ct_ref[...]) + skip_ref[...] * u_ref[...].astype(f32)


def project(*arrays):
    return staged(
        project_body,
        (
            shape((DEEP, 256), bf16),
            shape((ROWS, BLOCK), f32),
            shape((ROWS, BLOCK), f32),
            shape((8, N), f32),
        ),
        arrays,
        [
            pltpu.VMEM((ROWS, 2048), bf16),
            pltpu.SemaphoreType.DMA((20,)),
            pltpu.VMEM((4, MORE, 2048), bf16),
            pltpu.VMEM((ROWS, BLOCK), bf16),
            pltpu.VMEM((8, ROWS), f32),
            pltpu.VMEM((ROWS, 2 * N), f32),
            pltpu.VMEM((ROWS, 2 * N), bf16),
            pltpu.VMEM((2048, ROWS), bf16),
        ],
        flops=3 * 10**9,
        lazy=True,
        raw=range(10),
        free=range(10),
        vout=(shape((ROWS, BLOCK), bf16),),
        limit=32,
    )


def finish(chunks, y_ref, ef_ref, pow_ref, hop_ref, init_ref, ct_ref, g_ref):
    z = lax.axis_index("z")
    sr, si = init_ref[0:1, :], init_ref[1:2, :]
    for ref, active in chunks(z):
        part = ref.astype(f32)
        part = part[:8] + part[8:]
        part = jnp.concatenate([part[:4], part[4:]], axis=1)
        nr, ni = cmul(part[2:3], part[3:4], sr, si)
        sr = jnp.where(active, nr + part[0:1], sr)
        si = jnp.where(active, ni + part[1:2], si)
    for b in range(ROWS // BLOCK):
        at = slice(b * BLOCK, (b + 1) * BLOCK)
        er, ei = cmul(hop_ref[2 * b : 2 * b + 1, :], hop_ref[2 * b + 1 : 2 * b + 2, :], sr, si)
        gr, gi = cmul(pow_ref[:BLOCK, :], pow_ref[BLOCK:, :], er, ei)
        g_ref[at, :N] = gr.astype(bf16)
        g_ref[at, N:] = gi.astype(bf16)
    v = y_ref[...] + ef_ref[...] * mm_t(g_ref[...], ct_ref[...])
    inner = math.sqrt(2.0 / math.pi) * (v + 0.044715 * v * v * v)
    return (0.5 * v * (1.0 + jnp.tanh(inner))).astype(bf16)


def out_body(
    ready, send, a0, a3, a1, a2, b0, b1, b3, b2, r0, r3, r1, r2, send_ref, keep_ref, lhs_ref, sum_ref
):
    x, y, c = lax.axis_index("x"), lax.axis_index("y"), lax.axis_index("c")
    for step, ref in ((0, r0), (3, r3), (1, r1), (2, r2)):
        at = pl.multiple_of(((y + step) % 4) * BLOCK, BLOCK)
        lhs_ref[:, pl.ds(at, BLOCK)] = ref[:, :BLOCK]
        lhs_ref[:, pl.ds(ROWS + at, BLOCK)] = ref[:, BLOCK:]
    ready(*range(8))
    for step, scan_w, attend_w in ((0, a0, b0), (3, a3, b3), (1, a1, b1), (2, a2, b2)):
        total = mm(lhs_ref[:, :ROWS], scan_w[...]) + mm(lhs_ref[:, ROWS:], attend_w[...])
        sum_ref[:, pl.ds(pl.multiple_of(((x + step) % 4) * ROWS, ROWS), ROWS)] = total
    keep_ref[...] = sum_ref[pl.ds(pl.multiple_of(c * 64, 64), 64), :]
    send_ref[...] = sum_ref[pl.ds(pl.multiple_of((1 - c) * 64, 64), 64), :].astype(bf16)


def project_out(recv, pieces):
    return staged(
        out_body,
        [shape((64, 2048), bf16)],
        list(pieces),
        [pltpu.VMEM((BLOCK, 1024), bf16), pltpu.VMEM((BLOCK, 2048), f32)],
        flops=BLOCK * 1024 * 2048 * 2,
        lazy=True,
        free=(1, 2, 3, 5, 6, 7),
        vin=tuple(recv),
        vout=(shape((64, 2048), f32),),
    )


def shift(a, axis, by):
    n = lax.axis_size(axis)
    return lax.ppermute(a, axis, [(i, (i + by) % n) for i in range(n)])


def after(a, b):
    return lax.optimization_barrier((a, b))[0]


def on_device(
    tokens,
    norm_gain,
    drive_weight,
    query_weight,
    key_weight,
    value_weight,
    key_offset,
    log_step,
    lambda_real,
    lambda_imag,
    input_map,
    output_map,
    skip_gain,
    forget,
    initial_state,
    scan_out_weight,
    attend_out_weight,
):
    def exchange(a, axis):
        return lax.all_to_all(a, axis, split_axis=0, concat_axis=0, tiled=True)

    normed, w_a, w_b = normalize(
        tokens,
        norm_gain,
        forget[:, 0, :],
        key_offset[:, 0, :],
        key_weight,
        value_weight,
        query_weight,
        drive_weight,
    )
    a_up = shift(w_a, "x", 1)
    b_down = shift(w_b, "x", -1)
    b_up = shift(w_b, "x", 1)
    a_down = shift(w_a, "x", -1)
    a_far = shift(a_up, "x", 1)
    b_far = shift(b_down, "x", -1)
    weights = (w_a, a_up, a_down, a_far, w_b, b_up, b_down, b_far)
    mine = exchange(normed, "y")
    theirs = shift(mine, "c", 1)
    wide = jnp.broadcast_to(log_step[:, None], lambda_real.shape)
    tables = scan_tables(
        input_map.transpose(0, 1, 3, 2),
        output_map,
        lambda_real,
        lambda_imag,
        wide,
        initial_state,
        skip_gain.reshape(1, -1),
    )
    theirs, tables = lax.optimization_barrier((theirs, tables))
    power, inverse, b_map, c_map, init, skip = tables
    kv, y_local, ef, hop, q = project(
        mine, theirs, *weights, power, inverse, b_map, c_map, skip
    )
    ups, downs = [kv], [kv]
    for k in range(1, 5):
        ups.append(shift(ups[-1], "z", 1))
        if k < 4:
            downs.append(shift(downs[-1], "z", -1))
    out_pieces = []
    for w, way in ((scan_out_weight, 1), (attend_out_weight, -1)):
        w = after(w, kv)
        first = shift(w, "x", way)
        second = shift(w, "x", -way)
        far_piece = shift(first, "x", way)
        out_pieces += [w, first, second, far_piece]
    acc, fall, far = attend_own(q, kv)
    for k in (1, 2, 3):
        acc, fall, far = attend_step(q, acc, fall, far, ups[k], downs[k], k)
    both = attend_last(q, acc, fall, far, ups, downs, y_local, ef, power, hop, init, c_map)
    got = [both[0]]
    for k in (1, 3, 2):
        got.append(shift(both[k], "y", k))
    send, keep = project_out(got, out_pieces)
    return (keep + shift(send, "c", 1).astype(f32)).astype(bf16)[None]


def solution(mesh):
    split = Mesh(
        mesh.devices.reshape(8, 4, mesh.shape["fs"], mesh.shape["tp"]), ("z", "y", "x", "c")
    )
    in_specs = (
        P("x", SP_TP, None),
        P(),
        P("x", "c"),
        P("x", "c"),
        P("x", "c"),
        P("x", "c"),
        P("c", "x", SP),
        P("c"),
        P("c", None),
        P("c", None),
        P(None, "c", None, None),
        P(None, "c", None, None),
        P("c"),
        P("c", "x", SP),
        P(None, "x", "c", None),
        P("c", "x"),
        P("c", "x"),
    )
    out_specs = P("x", SP_TP, None)

    return jax.shard_map(on_device, mesh=split, in_specs=in_specs, out_specs=out_specs, check_vma=False)
```

```python
import math

import jax
import jax.numpy as jnp
from jax import lax
from jax.experimental import pallas as pl
from jax.experimental.pallas import tpu as pltpu
from jax.sharding import Mesh
from jax.sharding import PartitionSpec as P


HEAD_DIM = 128
BLOCK = 128
ROWS = 512
EXTRA = 16
MORE = 8
SP = ("z", "y")
SP_TP = ("z", "y", "c")
LOG2E = 1.4426950408889634
SCORE = HEAD_DIM ** (-0.5) * LOG2E
epsilon = 1e-06
f32 = jnp.float32
bf16 = jnp.bfloat16
INTERPRET = False


def staged(body, outs, arrays, scratch=(), flops=0, limit=20, lazy=False, raw=(), free=(), vin=(), vout=(), alias=()):
    n, m = len(arrays), len(outs)
    kept = [i for i in range(n) if i not in raw]

    def kernel(*refs):
        nv, mv = len(vin), len(vout)
        src, near_in = refs[:n], refs[n : n + nv]
        refs = refs[n + nv :]
        dst, near_out = refs[:m], refs[m : m + mv]
        refs = refs[m + mv :]
        bufs = dict(zip(kept, refs[: len(kept)]))
        results = refs[len(kept) : len(kept) + m]
        sems, rest = refs[len(kept) + m], refs[len(kept) + m + 1 :]
        copies = {i: pltpu.make_async_copy(src[i], bufs[i], sems.at[i]) for i in kept}
        for i in kept:
            copies[i].start()
        leaving = {}

        def ready(*which):
            for i in which:
                copies[i].wait()

        def send(i):
            leaving[i] = pltpu.make_async_copy(results[i], dst[i], sems.at[n + i])
            leaving[i].start()

        ins = [bufs.get(i, src[i]) for i in range(n)]
        if lazy:
            body(ready, send, *ins, *near_in, *results, *near_out, *rest)
        else:
            ready(*kept)
            body(*ins, *near_in, *results, *near_out, *rest)
        for i in range(m):
            if i not in leaving:
                send(i)
        for i in range(m):
            leaving[i].wait()

    hbm = pl.BlockSpec(memory_space=pltpu.HBM)
    near = pl.BlockSpec(memory_space=pltpu.VMEM)
    got = pl.pallas_call(
        kernel,
        out_shape=tuple(pltpu.HBM(o.shape, o.dtype) for o in outs) + tuple(vout),
        in_specs=[hbm] * n + [near] * len(vin),
        out_specs=(hbm,) * m + (near,) * len(vout),
        input_output_aliases={n + i: m + o for i, o in alias},
        scratch_shapes=[pltpu.VMEM(arrays[i].shape, arrays[i].dtype) for i in kept]
        + [pltpu.VMEM(o.shape, o.dtype) for o in outs]
        + [pltpu.SemaphoreType.DMA((n + m,))]
        + list(scratch),
        cost_estimate=pl.CostEstimate(flops=flops, transcendentals=0, bytes_accessed=1 << 20),
        compiler_params=pltpu.CompilerParams(vmem_limit_bytes=limit << 20),
        interpret=INTERPRET,
    )(*(a if i in free else pltpu.with_memory_space_constraint(a, pltpu.HBM) for i, a in enumerate(arrays)), *vin)
    return got if len(got) > 1 else got[0]


def shape(dims, dtype):
    return jax.ShapeDtypeStruct(dims, dtype)


def split2(v):
    hi = v.astype(bf16)
    return hi, (v - hi.astype(f32)).astype(bf16)


def mm(a, b):
    return jnp.dot(a, b, preferred_element_type=f32)


def mm_t(a, b):
    return lax.dot_general(a, b, (((1,), (1,)), ((), ())), preferred_element_type=f32)


def norm_body(
    ready, send, tok_ref, gain_ref, forget_ref, off_ref, k_ref, v_ref, q_ref, d_ref, out_ref, a_ref, b_ref, sems
):
    at = pl.ds(pl.multiple_of(lax.axis_index("y") * BLOCK, BLOCK), BLOCK)
    copies = []
    for n, (ref, to, h) in enumerate(((k_ref, a_ref, 0), (v_ref, a_ref, 1), (q_ref, b_ref, 0), (d_ref, b_ref, 1))):
        copies.append(pltpu.make_async_copy(ref.at[:, at], to.at[:, pl.ds(h * BLOCK, BLOCK)], sems.at[n]))
    for copy in copies:
        copy.start()
    ready(0, 1, 2, 3)
    v = tok_ref[0].astype(f32)
    scale = lax.rsqrt(jnp.mean(v * v, axis=1, keepdims=True) + epsilon)
    normed = (v * scale * gain_ref[...]).astype(bf16)
    hi, lo = split2(forget_ref[...])
    hi, lo = hi.astype(f32), lo.astype(f32)
    off = off_ref[...].astype(f32)
    blank = jnp.zeros((6, BLOCK), f32)
    for k in range(4):
        out_ref[k, :64, :] = normed
        for j in range(16):
            row = hi[8 * k + j : 8 * k + j + 1] if j < 8 else lo[8 * k + j - 8 : 8 * k + j - 7]
            last = off[k : k + 1] if j == 0 else jnp.zeros((1, BLOCK), f32)
            tile = jnp.concatenate([row, last, blank], axis=0)
            out_ref[k, 64:, j * BLOCK : (j + 1) * BLOCK] = tile.astype(bf16)
    send(0)
    for copy in copies:
        copy.wait()


def normalize(tokens, gain, forget, offset, *weights):
    return staged(
        norm_body,
        [shape((4, 64 + MORE, 2048), bf16), shape((ROWS, 256), bf16), shape((ROWS, 256), bf16)],
        [tokens, gain.reshape(1, -1), forget, offset, *weights],
        [pltpu.SemaphoreType.DMA((4,))],
        flops=10**6,
        lazy=True,
        raw=(4, 5, 6, 7),
    )


SPAN = 256
TILE = 32
WIDE = SPAN + BLOCK


def chunk(q_ref, kv_ref, acc_ref, fall_ref, scr, diagonal):
    s_ref, soft_ref, r_ref, w_ref, tri_ref = scr
    j = lax.broadcasted_iota(jnp.int32, (SPAN, WIDE), 0)
    k = lax.broadcasted_iota(jnp.int32, (SPAN, WIDE), 1)
    tri_ref[...] = jnp.where((j > k) | (k >= SPAN), 1.0, 0.0).astype(bf16)
    offs = kv_ref[ROWS : ROWS + EXTRA, :].astype(f32)
    off = jnp.concatenate([offs[0:1], offs[1:2]], axis=1) * LOG2E
    s_ref[...] = mm_t(q_ref[...], kv_ref[:ROWS, :BLOCK])

    def visible(i):
        t = lax.broadcasted_iota(jnp.int32, (TILE, ROWS), 0) + i * TILE
        s = lax.broadcasted_iota(jnp.int32, (TILE, ROWS), 1)
        return s < t

    def first(i, _):
        at = pl.ds(pl.multiple_of(i * TILE, TILE), TILE)
        z = s_ref[at, :] * SCORE + off
        soft = jnp.maximum(z, 0.0) + jnp.log2(1.0 + jnp.exp2(-jnp.abs(z)))
        s_ref[at, :] = z - soft
        if diagonal:
            soft = jnp.where(visible(i), soft, 0.0)
        soft_ref[at, :] = soft.astype(bf16)
        return 0

    lax.fori_loop(0, ROWS // TILE, first, 0, unroll=2)
    for blk in range(2):
        r_ref[:, blk * WIDE : (blk + 1) * WIDE] = mm(
            soft_ref[:, blk * SPAN : (blk + 1) * SPAN], tri_ref[...]
        )

    def second(i, _):
        at = pl.ds(pl.multiple_of(i * TILE, TILE), TILE)
        fall1 = fall_ref[at, :]
        fall0 = fall1 + r_ref[at, WIDE + SPAN :]
        fall_ref[at, :] = fall0 + r_ref[at, SPAN:WIDE]
        behind = jnp.concatenate(
            [
                r_ref[at, :BLOCK] + fall0,
                r_ref[at, BLOCK:SPAN] + fall0,
                r_ref[at, WIDE : WIDE + BLOCK] + fall1,
                r_ref[at, WIDE + BLOCK : WIDE + SPAN] + fall1,
            ],
            axis=1,
        )
        w = jnp.exp2(s_ref[at, :] - behind)
        if diagonal:
            w = jnp.where(visible(i), w, 0.0)
        w_ref[at, :] = w.astype(bf16)
        return 0

    lax.fori_loop(0, ROWS // TILE, second, 0, unroll=2)
    acc_ref[...] += mm(w_ref[...], kv_ref[:ROWS, BLOCK:])


ATTEND_SCRATCH = [
    pltpu.VMEM((ROWS, ROWS), f32),
    pltpu.VMEM((ROWS, ROWS), bf16),
    pltpu.VMEM((ROWS, 2 * WIDE), f32),
    pltpu.VMEM((ROWS, ROWS), bf16),
    pltpu.VMEM((SPAN, WIDE), bf16),
]
PAIR = (shape((ROWS, BLOCK), f32), shape((ROWS, BLOCK), f32))
ATTEND_FLOPS = 8 * ROWS * ROWS * BLOCK


def zero(ref):
    ref[...] = jnp.zeros(ref.shape, ref.dtype)


def attend_own(q, kv):
    def body(kv_ref, q_ref, acc_ref, fall_ref, far_ref, *scr):
        zero(acc_ref)
        zero(fall_ref)
        zero(far_ref)
        chunk(q_ref, kv_ref, acc_ref, fall_ref, scr, True)

    return staged(body, (), [kv], ATTEND_SCRATCH, flops=ATTEND_FLOPS, vin=(q,), vout=PAIR + PAIR[:1])


def attend_step(q, acc, fall, far, up, down, k):
    def body(ready, send, up_ref, down_ref, q_ref, _a, _b, _c, acc_ref, fall_ref, far_ref, low_ref, part_ref, *scr):
        z = lax.axis_index("z")
        ready(0, 1)

        @pl.when(z >= k)
        def _():
            chunk(q_ref, up_ref, acc_ref, fall_ref, scr, False)

        @pl.when(z + k >= 8)
        def _():
            zero(low_ref)
            zero(part_ref)
            chunk(q_ref, down_ref, part_ref, low_ref, scr, False)
            far_ref[...] = part_ref[...] + jnp.exp2(-low_ref[...]) * far_ref[...]

    return staged(
        body,
        (),
        [up, down],
        [pltpu.VMEM((ROWS, BLOCK), f32)] * 2 + ATTEND_SCRATCH,
        flops=2 * ATTEND_FLOPS,
        lazy=True,
        free=(0, 1),
        vin=(q, acc, fall, far),
        vout=PAIR + PAIR[:1],
        alias=((1, 0), (2, 1), (3, 2)),
    )


def attend_last(q, acc, fall, far, ups, downs, y, ef, power, hop, init, c_map):
    def body(
        ready, send, up4, y_ref, ef_ref, pow_ref, hop_ref, init_ref, ct_ref, *refs,
    ):
        heads = refs[:6]
        refs = refs[6:]
        q_ref, acc_in, fall_in, far_ref, *parts = refs[:8]
        out_ref, acc_ref, fall_ref, g_ref, head_ref, head_sem = refs[8:14]
        scr = refs[14:]
        tails = [
            pltpu.make_async_copy(ref.at[pl.ds(ROWS + EXTRA, EXTRA)], head_ref.at[n], head_sem.at[n])
            for n, ref in enumerate(heads)
        ]
        for copy in tails:
            copy.start()
        acc_ref[...] = acc_in[...]
        fall_ref[...] = fall_in[...]
        ready(0)

        @pl.when(lax.axis_index("z") >= 4)
        def _():
            chunk(q_ref, up4, acc_ref, fall_ref, scr, False)

        for copy in tails:
            copy.wait()
        ready(1, 2, 3, 4, 5, 6)
        out_ref[:, BLOCK:] = (acc_ref[...] + jnp.exp2(-fall_ref[...]) * far_ref[...]).astype(bf16)

        def chunks(z):
            for n, k in enumerate((1, 2, 3)):
                yield head_ref[n], z + k >= 8
            yield up4[ROWS + EXTRA :, :], z >= 4
            for n, k in ((3, 3), (4, 2), (5, 1)):
                yield head_ref[n], z >= k

        out_ref[:, :BLOCK] = finish(chunks, y_ref, ef_ref, pow_ref, hop_ref, init_ref, ct_ref, g_ref)
        mine = lax.axis_index("y")
        for k, part in enumerate(parts):
            part[...] = out_ref[pl.ds(pl.multiple_of(((mine + k) % 4) * BLOCK, BLOCK), BLOCK), :]

    return staged(
        body,
        [],
        [ups[4], y, ef, power, hop, init, c_map, downs[1], downs[2], downs[3], ups[3], ups[2], ups[1]],
        [
            pltpu.VMEM((ROWS, 2 * BLOCK), bf16),
            pltpu.VMEM((ROWS, BLOCK), f32),
            pltpu.VMEM((ROWS, BLOCK), f32),
            pltpu.VMEM((ROWS, 2 * N), bf16),
            pltpu.VMEM((6, EXTRA, 256), bf16),
            pltpu.SemaphoreType.DMA((6,)),
        ]
        + ATTEND_SCRATCH,
        flops=2 * ATTEND_FLOPS,
        lazy=True,
        raw=range(7, 13),
        free=(0,) + tuple(range(7, 13)),
        vin=(q, acc, fall, far),
        vout=(shape((BLOCK, 2 * BLOCK), bf16),) * 4,
    )


N = 512


def cmul(ar, ai, br, bi):
    return ar * br - ai * bi, ar * bi + ai * br


def tables_body(
    in_ref, out_ref, lam_r_ref, lam_i_ref, step_ref, start_ref, skip_in,
    pow_ref, inv_ref, b_ref, ct_ref, init_ref, skip_ref,
):
    y = lax.axis_index("y")
    own = pl.ds(pl.multiple_of(y * 8, 8), 8)
    copy = (
        lax.broadcasted_iota(jnp.int32, (64, N), 1) % 64 == lax.broadcasted_iota(jnp.int32, (64, N), 0)
    ).astype(f32)

    def tiled(a, height):
        rows, width = a.shape
        r = lax.broadcasted_iota(jnp.int32, (rows, N), 0) // height
        k = lax.broadcasted_iota(jnp.int32, (rows, N), 1) // width
        spread = jnp.dot(a, copy, precision=lax.Precision.HIGHEST, preferred_element_type=f32)
        return jnp.where(r == k, spread, 0.0)

    def line(a):
        return jnp.sum(tiled(a, 1), axis=0, keepdims=True)

    lam_r, lam_i, step = line(lam_r_ref[own]), line(lam_i_ref[own]), jnp.exp(line(step_ref[own]))
    init_ref[0:1, :] = line(start_ref[0, 0, own])
    init_ref[1:2, :] = line(start_ref[1, 0, own])
    skip_ref[...] = skip_in[:, pl.ds(pl.multiple_of(y * BLOCK, BLOCK), BLOCK)]
    gain = lam_r * step
    turn = lam_i * step
    size = jnp.exp(gain)
    bar_r = size * jnp.cos(turn)
    bar_i = size * jnp.sin(turn)
    over = lam_r * lam_r + lam_i * lam_i
    less = bar_r - 1.0
    factor_r = (less * lam_r + bar_i * lam_i) / over
    factor_i = (bar_i * lam_r - less * lam_i) / over
    count = lax.broadcasted_iota(jnp.int32, (BLOCK, N), 0) + 1
    pr = jnp.ones((BLOCK, N), f32)
    pi = jnp.zeros((BLOCK, N), f32)
    sr, si = bar_r, bar_i
    for bit in range(8):
        on = ((count >> bit) & 1) == 1
        nr, ni = cmul(pr, pi, sr, si)
        pr, pi = jnp.where(on, nr, pr), jnp.where(on, ni, pi)
        if bit < 7:
            sr, si = cmul(sr, si, sr, si)
    back = jnp.exp(-2.0 * count.astype(f32) * gain)
    pow_ref[:BLOCK, :] = pr
    pow_ref[BLOCK:, :] = pi
    br, bi = cmul(pr * back, -pi * back, factor_r, factor_i)
    inv_ref[:BLOCK, :] = br
    inv_ref[BLOCK:, :] = bi
    for p in range(2):
        b_ref[:, p * N : (p + 1) * N] = tiled(in_ref[p, own].reshape(BLOCK, 64), 16).astype(bf16)
        sign = 1.0 if p == 0 else -1.0
        ct_ref[:, p * N : (p + 1) * N] = (sign * tiled(out_ref[p, own].reshape(BLOCK, 64), 16)).astype(bf16)


def scan_tables(*arrays):
    return staged(
        tables_body,
        (
            shape((2 * BLOCK, N), f32),
            shape((2 * BLOCK, N), f32),
            shape((BLOCK, 2 * N), bf16),
            shape((BLOCK, 2 * N), bf16),
            shape((2, N), f32),
            shape((1, BLOCK), f32),
        ),
        arrays,
        flops=10**9,
    )


DEEP = ROWS + 2 * EXTRA


def project_body(
    ready, send, mine, theirs, a0, a3, a1, a2, b0, b3, b1, b2, pow_ref, inv_ref, b_ref, ct_ref, skip_ref,
    kv_ref, y_ref, ef_ref, hop_ref, q_ref,
    rows, sems, more, u_ref, x_ref, st_ref, w_ref,
):
    c = lax.axis_index("c")
    x = lax.axis_index("x")
    copies = []
    for n, (step, ref) in enumerate(((0, a0), (3, a3), (1, a1), (2, a2), (0, b0), (3, b3), (1, b1), (2, b2))):
        at = pl.multiple_of(((x + step) % 4) * ROWS, ROWS)
        to = w_ref.at[pl.ds(at, ROWS), pl.ds(256 * (n // 4), 256)]
        copies.append(pltpu.make_async_copy(ref, to, sems.at[12 + n]))
    for b in range(4):
        for part, ref in enumerate((mine, theirs)):
            at = pl.multiple_of(b * BLOCK + ((c + part) % 2) * 64, 64)
            copies.append(
                pltpu.make_async_copy(ref.at[b, pl.ds(0, 64)], rows.at[pl.ds(at, 64)], sems.at[2 * b + part])
            )
    for b in range(4):
        copies.append(
            pltpu.make_async_copy(mine.at[b, pl.ds(64, MORE)], more.at[b], sems.at[8 + b])
        )
    for copy in copies[-4:] + copies[:-4]:
        copy.start()
    for copy in copies[-4:]:
        copy.wait()
    offs = [more[b].astype(f32)[1:2, :BLOCK] for b in range(4)]
    row0 = jnp.concatenate(offs[:2], axis=1)
    row1 = jnp.concatenate(offs[2:], axis=1)
    tail = jnp.concatenate([row0, row1, jnp.zeros((EXTRA - 2, 256), f32)], axis=0)
    kv_ref[ROWS : ROWS + EXTRA, :] = tail.astype(bf16)
    row = lax.broadcasted_iota(jnp.int32, (BLOCK, BLOCK), 0)
    col = lax.broadcasted_iota(jnp.int32, (BLOCK, BLOCK), 1)
    low = (col <= row).astype(bf16)
    low32 = (col <= row).astype(f32)
    even = lax.broadcasted_iota(jnp.int32, (1, BLOCK), 1) < 64
    keeps = []
    blocks = [slice(b * BLOCK, (b + 1) * BLOCK) for b in range(4)]
    for b, at in enumerate(blocks):
        part = more[b].astype(f32)
        part = part[0:1, : 8 * BLOCK] + part[0:1, 8 * BLOCK :]
        f = jnp.concatenate([part[:, g * BLOCK : (g + 1) * BLOCK] for g in range(8)], axis=0)
        f_all = jnp.concatenate([jnp.broadcast_to(f[g : g + 1], (16, BLOCK)) for g in range(8)], axis=0)
        cum_f = lax.dot_general(
            low32, f_all, (((1,), (1,)), ((), ())), precision=lax.Precision.HIGHEST, preferred_element_type=f32
        )
        ef_ref[at, :] = jnp.exp(cum_f)
        x_ref[at, :BLOCK] = jnp.exp(-cum_f)
        total = jnp.exp(jnp.broadcast_to(jnp.sum(f, axis=1, keepdims=True), (8, BLOCK)))
        keeps.append(
            jnp.concatenate(
                [jnp.where(even, total[2 * g : 2 * g + 1], total[2 * g + 1 : 2 * g + 2]) for g in range(4)],
                axis=1,
            )
        )
    for copy in copies[:-4]:
        copy.wait()
    both = mm(rows[...], w_ref[...])
    kv_ref[:ROWS, :] = both[:, :256].astype(bf16)
    q_ref[...] = both[:, 256:384].astype(bf16)
    u_ref[...] = both[:, 384:].astype(bf16)
    x_ref[:, :BLOCK] = x_ref[:, :BLOCK] * u_ref[...].astype(f32)
    ready(10, 11, 12, 13, 14)
    x_ref[...] = mm(x_ref[:, :BLOCK].astype(bf16), b_ref[...])
    carry_r = jnp.zeros((1, N), f32)
    carry_i = jnp.zeros((1, N), f32)
    hop_r = jnp.ones((1, N), f32)
    hop_i = jnp.zeros((1, N), f32)
    end_r, end_i = pow_ref[BLOCK - 1 : BLOCK, :], pow_ref[2 * BLOCK - 1 :, :]
    hops = []
    for at, keep in zip(blocks, keeps):
        dr, di = cmul(x_ref[at, :N], x_ref[at, N:], inv_ref[:BLOCK, :], inv_ref[BLOCK:, :])
        tr = mm(low, dr.astype(bf16)) + carry_r
        ti = mm(low, di.astype(bf16)) + carry_i
        st_r, st_i = cmul(pow_ref[:BLOCK, :], pow_ref[BLOCK:, :], tr, ti)
        st_ref[at, :N] = st_r.astype(bf16)
        st_ref[at, N:] = st_i.astype(bf16)
        carry_r, carry_i = keep * st_r[BLOCK - 1 :, :], keep * st_i[BLOCK - 1 :, :]
        hops += [hop_r, hop_i]
        nr, ni = cmul(hop_r, hop_i, end_r, end_i)
        hop_r, hop_i = keep * nr, keep * ni
    hop_ref[...] = jnp.concatenate(hops, axis=0)
    hi, lo = split2(jnp.concatenate([carry_r, carry_i, hop_r, hop_i], axis=0))
    hi, lo = hi.astype(f32), lo.astype(f32)
    kv_ref[ROWS + EXTRA :, :] = jnp.concatenate(
        [hi[:, :256], hi[:, 256:], lo[:, :256], lo[:, 256:]], axis=0
    ).astype(bf16)
    send(0)
    y_ref[...] = ef_ref[...] * mm_t(st_ref[...], ct_ref[...]) + skip_ref[...] * u_ref[...].astype(f32)


def project(*arrays):
    return staged(
        project_body,
        (
            shape((DEEP, 256), bf16),
            shape((ROWS, BLOCK), f32),
            shape((ROWS, BLOCK), f32),
            shape((8, N), f32),
        ),
        arrays,
        [
            pltpu.VMEM((ROWS, 2048), bf16),
            pltpu.SemaphoreType.DMA((20,)),
            pltpu.VMEM((4, MORE, 2048), bf16),
            pltpu.VMEM((ROWS, BLOCK), bf16),
            pltpu.VMEM((ROWS, 2 * N), f32),
            pltpu.VMEM((ROWS, 2 * N), bf16),
            pltpu.VMEM((2048, ROWS), bf16),
        ],
        flops=3 * 10**9,
        lazy=True,
        raw=range(10),
        free=range(10),
        vout=(shape((ROWS, BLOCK), bf16),),
        limit=32,
    )


def finish(chunks, y_ref, ef_ref, pow_ref, hop_ref, init_ref, ct_ref, g_ref):
    z = lax.axis_index("z")
    sr, si = init_ref[0:1, :], init_ref[1:2, :]
    for ref, active in chunks(z):
        part = ref.astype(f32)
        part = part[:8] + part[8:]
        part = jnp.concatenate([part[:4], part[4:]], axis=1)
        nr, ni = cmul(part[2:3], part[3:4], sr, si)
        sr = jnp.where(active, nr + part[0:1], sr)
        si = jnp.where(active, ni + part[1:2], si)
    for b in range(ROWS // BLOCK):
        at = slice(b * BLOCK, (b + 1) * BLOCK)
        er, ei = cmul(hop_ref[2 * b : 2 * b + 1, :], hop_ref[2 * b + 1 : 2 * b + 2, :], sr, si)
        gr, gi = cmul(pow_ref[:BLOCK, :], pow_ref[BLOCK:, :], er, ei)
        g_ref[at, :N] = gr.astype(bf16)
        g_ref[at, N:] = gi.astype(bf16)
    v = y_ref[...] + ef_ref[...] * mm_t(g_ref[...], ct_ref[...])
    inner = math.sqrt(2.0 / math.pi) * (v + 0.044715 * v * v * v)
    return (0.5 * v * (1.0 + jnp.tanh(inner))).astype(bf16)


def out_body(
    a0, a3, a1, a2, b0, b1, b3, b2, r0, r3, r1, r2, send_ref, keep_ref, lhs_ref, sum_ref
):
    x, y, c = lax.axis_index("x"), lax.axis_index("y"), lax.axis_index("c")
    for step, ref in ((0, r0), (3, r3), (1, r1), (2, r2)):
        at = pl.multiple_of(((y + step) % 4) * BLOCK, BLOCK)
        lhs_ref[:, pl.ds(at, BLOCK)] = ref[:, :BLOCK]
        lhs_ref[:, pl.ds(ROWS + at, BLOCK)] = ref[:, BLOCK:]
    for step, scan_w, attend_w in ((0, a0, b0), (3, a3, b3), (1, a1, b1), (2, a2, b2)):
        total = mm(lhs_ref[:, :ROWS], scan_w[...]) + mm(lhs_ref[:, ROWS:], attend_w[...])
        sum_ref[:, pl.ds(pl.multiple_of(((x + step) % 4) * ROWS, ROWS), ROWS)] = total
    keep_ref[...] = sum_ref[pl.ds(pl.multiple_of(c * 64, 64), 64), :]
    send_ref[...] = sum_ref[pl.ds(pl.multiple_of((1 - c) * 64, 64), 64), :].astype(bf16)


def project_out(recv, pieces):
    return staged(
        out_body,
        [shape((64, 2048), bf16)],
        [],
        [pltpu.VMEM((BLOCK, 1024), bf16), pltpu.VMEM((BLOCK, 2048), f32)],
        flops=BLOCK * 1024 * 2048 * 2,
        vin=tuple(pieces) + tuple(recv),
        vout=(shape((64, 2048), f32),),
    )


def shift(a, axis, by):
    n = lax.axis_size(axis)
    return lax.ppermute(a, axis, [(i, (i + by) % n) for i in range(n)])


def after(a, b):
    return lax.optimization_barrier((a, b))[0]


def on_device(
    tokens,
    norm_gain,
    drive_weight,
    query_weight,
    key_weight,
    value_weight,
    key_offset,
    log_step,
    lambda_real,
    lambda_imag,
    input_map,
    output_map,
    skip_gain,
    forget,
    initial_state,
    scan_out_weight,
    attend_out_weight,
):
    def exchange(a, axis):
        return lax.all_to_all(a, axis, split_axis=0, concat_axis=0, tiled=True)

    normed, w_a, w_b = normalize(
        tokens,
        norm_gain,
        forget[:, 0, :],
        key_offset[:, 0, :],
        key_weight,
        value_weight,
        query_weight,
        drive_weight,
    )
    a_up = shift(w_a, "x", 1)
    b_down = shift(w_b, "x", -1)
    b_up = shift(w_b, "x", 1)
    a_down = shift(w_a, "x", -1)
    a_far = shift(a_up, "x", 1)
    b_far = shift(b_down, "x", -1)
    weights = (w_a, a_up, a_down, a_far, w_b, b_up, b_down, b_far)
    mine = exchange(normed, "y")
    theirs = shift(mine, "c", 1)
    wide = jnp.broadcast_to(log_step[:, None], lambda_real.shape)
    tables = scan_tables(
        input_map.transpose(0, 1, 3, 2),
        output_map,
        lambda_real,
        lambda_imag,
        wide,
        initial_state,
        skip_gain.reshape(1, -1),
    )
    theirs, tables = lax.optimization_barrier((theirs, tables))
    power, inverse, b_map, c_map, init, skip = tables
    kv, y_local, ef, hop, q = project(
        mine, theirs, *weights, power, inverse, b_map, c_map, skip
    )
    ups, downs = [kv], [kv]
    for k in range(1, 5):
        ups.append(lax.ppermute(ups[-1], "z", [(i, i + 1) for i in range(k - 1, 7)]))
        if k < 4:
            downs.append(lax.ppermute(downs[-1], "z", [((j - k + 1) % 8, (j - k) % 8) for j in range(3)]))
    out_pieces = []
    for w, way in ((scan_out_weight, 1), (attend_out_weight, -1)):
        w = after(w, kv)
        first = shift(w, "x", way)
        second = shift(w, "x", -way)
        far_piece = shift(first, "x", way)
        out_pieces += [w, first, second, far_piece]
    acc, fall, far = attend_own(q, kv)
    for k in (1, 2, 3):
        acc, fall, far = attend_step(q, acc, fall, far, ups[k], downs[k], k)
    both = attend_last(q, acc, fall, far, ups, downs, y_local, ef, power, hop, init, c_map)
    got = [both[0]]
    for k in (1, 3, 2):
        got.append(shift(both[k], "y", k))
    send, keep = project_out(got, out_pieces)
    return (keep + shift(send, "c", 1).astype(f32)).astype(bf16)[None]


def solution(mesh):
    split = Mesh(
        mesh.devices.reshape(8, 4, mesh.shape["fs"], mesh.shape["tp"]), ("z", "y", "x", "c")
    )
    in_specs = (
        P("x", SP_TP, None),
        P(),
        P("x", "c"),
        P("x", "c"),
        P("x", "c"),
        P("x", "c"),
        P("c", "x", SP),
        P("c"),
        P("c", None),
        P("c", None),
        P(None, "c", None, None),
        P(None, "c", None, None),
        P("c"),
        P("c", "x", SP),
        P(None, "x", "c", None),
        P("c", "x"),
        P("c", "x"),
    )
    out_specs = P("x", SP_TP, None)

    return jax.shard_map(on_device, mesh=split, in_specs=in_specs, out_specs=out_specs, check_vma=False)
```

```python
import math

import jax
import jax.numpy as jnp
from jax import lax
from jax.experimental import pallas as pl
from jax.experimental.pallas import tpu as pltpu
from jax.sharding import Mesh
from jax.sharding import PartitionSpec as P


HEAD_DIM = 128
BLOCK = 128
ROWS = 512
EXTRA = 16
MORE = 8
SP = ("z", "y")
SP_TP = ("z", "y", "c")
LOG2E = 1.4426950408889634
SCORE = HEAD_DIM ** (-0.5) * LOG2E
epsilon = 1e-06
f32 = jnp.float32
bf16 = jnp.bfloat16
INTERPRET = False


def staged(body, outs, arrays, scratch=(), flops=0, limit=20, lazy=False, raw=(), free=(), vin=(), vout=(), alias=()):
    n, m = len(arrays), len(outs)
    kept = [i for i in range(n) if i not in raw]

    def kernel(*refs):
        nv, mv = len(vin), len(vout)
        src, near_in = refs[:n], refs[n : n + nv]
        refs = refs[n + nv :]
        dst, near_out = refs[:m], refs[m : m + mv]
        refs = refs[m + mv :]
        bufs = dict(zip(kept, refs[: len(kept)]))
        results = refs[len(kept) : len(kept) + m]
        sems, rest = refs[len(kept) + m], refs[len(kept) + m + 1 :]
        copies = {i: pltpu.make_async_copy(src[i], bufs[i], sems.at[i]) for i in kept}
        for i in kept:
            copies[i].start()
        leaving = {}

        def ready(*which):
            for i in which:
                copies[i].wait()

        def send(i):
            leaving[i] = pltpu.make_async_copy(results[i], dst[i], sems.at[n + i])
            leaving[i].start()

        ins = [bufs.get(i, src[i]) for i in range(n)]
        if lazy:
            body(ready, send, *ins, *near_in, *results, *near_out, *rest)
        else:
            ready(*kept)
            body(*ins, *near_in, *results, *near_out, *rest)
        for i in range(m):
            if i not in leaving:
                send(i)
        for i in range(m):
            leaving[i].wait()

    hbm = pl.BlockSpec(memory_space=pltpu.HBM)
    near = pl.BlockSpec(memory_space=pltpu.VMEM)
    got = pl.pallas_call(
        kernel,
        out_shape=tuple(pltpu.HBM(o.shape, o.dtype) for o in outs) + tuple(vout),
        in_specs=[hbm] * n + [near] * len(vin),
        out_specs=(hbm,) * m + (near,) * len(vout),
        input_output_aliases={n + i: m + o for i, o in alias},
        scratch_shapes=[pltpu.VMEM(arrays[i].shape, arrays[i].dtype) for i in kept]
        + [pltpu.VMEM(o.shape, o.dtype) for o in outs]
        + [pltpu.SemaphoreType.DMA((n + m,))]
        + list(scratch),
        cost_estimate=pl.CostEstimate(flops=flops, transcendentals=0, bytes_accessed=1 << 20),
        compiler_params=pltpu.CompilerParams(vmem_limit_bytes=limit << 20),
        interpret=INTERPRET,
    )(*(a if i in free else pltpu.with_memory_space_constraint(a, pltpu.HBM) for i, a in enumerate(arrays)), *vin)
    return got if len(got) > 1 else got[0]


def shape(dims, dtype):
    return jax.ShapeDtypeStruct(dims, dtype)


def split2(v):
    hi = v.astype(bf16)
    return hi, (v - hi.astype(f32)).astype(bf16)


def mm(a, b):
    return jnp.dot(a, b, preferred_element_type=f32)


def mm_t(a, b):
    return lax.dot_general(a, b, (((1,), (1,)), ((), ())), preferred_element_type=f32)


def norm_body(
    ready, send, tok_ref, gain_ref, forget_ref, off_ref, k_ref, v_ref, q_ref, d_ref, out_ref, a_ref, b_ref, sems
):
    at = pl.ds(pl.multiple_of(lax.axis_index("y") * BLOCK, BLOCK), BLOCK)
    copies = []
    for n, (ref, to, h) in enumerate(((k_ref, a_ref, 0), (v_ref, a_ref, 1), (q_ref, b_ref, 0), (d_ref, b_ref, 1))):
        copies.append(pltpu.make_async_copy(ref.at[:, at], to.at[:, pl.ds(h * BLOCK, BLOCK)], sems.at[n]))
    for copy in copies:
        copy.start()
    ready(0, 1, 2, 3)
    v = tok_ref[0].astype(f32)
    scale = lax.rsqrt(jnp.mean(v * v, axis=1, keepdims=True) + epsilon)
    normed = (v * scale * gain_ref[...]).astype(bf16)
    hi, lo = split2(forget_ref[...])
    hi, lo = hi.astype(f32), lo.astype(f32)
    off = off_ref[...].astype(f32)
    blank = jnp.zeros((6, BLOCK), f32)
    for k in range(4):
        out_ref[k, :64, :] = normed
        for j in range(16):
            row = hi[8 * k + j : 8 * k + j + 1] if j < 8 else lo[8 * k + j - 8 : 8 * k + j - 7]
            last = off[k : k + 1] if j == 0 else jnp.zeros((1, BLOCK), f32)
            tile = jnp.concatenate([row, last, blank], axis=0)
            out_ref[k, 64:, j * BLOCK : (j + 1) * BLOCK] = tile.astype(bf16)
    send(0)
    for copy in copies:
        copy.wait()


def normalize(tokens, gain, forget, offset, *weights):
    return staged(
        norm_body,
        [shape((4, 64 + MORE, 2048), bf16), shape((ROWS, 256), bf16), shape((ROWS, 256), bf16)],
        [tokens, gain.reshape(1, -1), forget, offset, *weights],
        [pltpu.SemaphoreType.DMA((4,))],
        flops=10**6,
        lazy=True,
        raw=(4, 5, 6, 7),
    )


SPAN = 256
TILE = 32
WIDE = SPAN + BLOCK


def chunk(q_ref, kv_ref, acc_ref, fall_ref, scr, diagonal):
    s_ref, soft_ref, r_ref, w_ref, tri_ref = scr
    j = lax.broadcasted_iota(jnp.int32, (SPAN, WIDE), 0)
    k = lax.broadcasted_iota(jnp.int32, (SPAN, WIDE), 1)
    tri_ref[...] = jnp.where((j > k) | (k >= SPAN), 1.0, 0.0).astype(bf16)
    offs = kv_ref[ROWS : ROWS + EXTRA, :].astype(f32)
    off = jnp.concatenate([offs[0:1], offs[1:2]], axis=1) * LOG2E
    s_ref[...] = mm_t(q_ref[...], kv_ref[:ROWS, :BLOCK])

    def visible(i):
        t = lax.broadcasted_iota(jnp.int32, (TILE, ROWS), 0) + i * TILE
        s = lax.broadcasted_iota(jnp.int32, (TILE, ROWS), 1)
        return s < t

    def first(i, _):
        at = pl.ds(pl.multiple_of(i * TILE, TILE), TILE)
        z = s_ref[at, :] * SCORE + off
        soft = jnp.maximum(z, 0.0) + jnp.log2(1.0 + jnp.exp2(-jnp.abs(z)))
        s_ref[at, :] = z - soft
        if diagonal:
            soft = jnp.where(visible(i), soft, 0.0)
        soft_ref[at, :] = soft.astype(bf16)
        return 0

    lax.fori_loop(0, ROWS // TILE, first, 0, unroll=2)
    for blk in range(2):
        r_ref[:, blk * WIDE : (blk + 1) * WIDE] = mm(
            soft_ref[:, blk * SPAN : (blk + 1) * SPAN], tri_ref[...]
        )

    def second(i, _):
        at = pl.ds(pl.multiple_of(i * TILE, TILE), TILE)
        fall1 = fall_ref[at, :]
        fall0 = fall1 + r_ref[at, WIDE + SPAN :]
        fall_ref[at, :] = fall0 + r_ref[at, SPAN:WIDE]
        behind = jnp.concatenate(
            [
                r_ref[at, :BLOCK] + fall0,
                r_ref[at, BLOCK:SPAN] + fall0,
                r_ref[at, WIDE : WIDE + BLOCK] + fall1,
                r_ref[at, WIDE + BLOCK : WIDE + SPAN] + fall1,
            ],
            axis=1,
        )
        w = jnp.exp2(s_ref[at, :] - behind)
        if diagonal:
            w = jnp.where(visible(i), w, 0.0)
        w_ref[at, :] = w.astype(bf16)
        return 0

    lax.fori_loop(0, ROWS // TILE, second, 0, unroll=2)
    acc_ref[...] += mm(w_ref[...], kv_ref[:ROWS, BLOCK:])


ATTEND_SCRATCH = [
    pltpu.VMEM((ROWS, ROWS), f32),
    pltpu.VMEM((ROWS, ROWS), bf16),
    pltpu.VMEM((ROWS, 2 * WIDE), f32),
    pltpu.VMEM((ROWS, ROWS), bf16),
    pltpu.VMEM((SPAN, WIDE), bf16),
]
PAIR = (shape((ROWS, BLOCK), f32), shape((ROWS, BLOCK), f32))
ATTEND_FLOPS = 8 * ROWS * ROWS * BLOCK


def zero(ref):
    ref[...] = jnp.zeros(ref.shape, ref.dtype)


def attend_own(q, kv):
    def body(kv_ref, q_ref, acc_ref, fall_ref, far_ref, *scr):
        zero(acc_ref)
        zero(fall_ref)
        zero(far_ref)
        chunk(q_ref, kv_ref, acc_ref, fall_ref, scr, True)

    return staged(body, (), [kv], ATTEND_SCRATCH, flops=ATTEND_FLOPS, vin=(q,), vout=PAIR + PAIR[:1])


def attend_step(q, acc, fall, far, up, down, k):
    def body(ready, send, up_ref, down_ref, q_ref, _a, _b, _c, acc_ref, fall_ref, far_ref, low_ref, part_ref, *scr):
        z = lax.axis_index("z")
        ready(0, 1)

        @pl.when(z >= k)
        def _():
            chunk(q_ref, up_ref, acc_ref, fall_ref, scr, False)

        @pl.when(z + k >= 8)
        def _():
            zero(low_ref)
            zero(part_ref)
            chunk(q_ref, down_ref, part_ref, low_ref, scr, False)
            far_ref[...] = part_ref[...] + jnp.exp2(-low_ref[...]) * far_ref[...]

    return staged(
        body,
        (),
        [up, down],
        [pltpu.VMEM((ROWS, BLOCK), f32)] * 2 + ATTEND_SCRATCH,
        flops=2 * ATTEND_FLOPS,
        lazy=True,
        free=(0, 1),
        vin=(q, acc, fall, far),
        vout=PAIR + PAIR[:1],
        alias=((1, 0), (2, 1), (3, 2)),
    )


def attend_last(q, acc, fall, far, ups, downs, y, ef, power, hop, init, c_map):
    def body(
        ready, send, up4, y_ref, ef_ref, pow_ref, hop_ref, init_ref, ct_ref, *refs,
    ):
        heads = refs[:6]
        refs = refs[6:]
        q_ref, acc_in, fall_in, far_ref, *parts = refs[:8]
        out_ref, acc_ref, fall_ref, g_ref, head_ref, head_sem = refs[8:14]
        scr = refs[14:]
        tails = [
            pltpu.make_async_copy(ref.at[pl.ds(ROWS + EXTRA, EXTRA)], head_ref.at[n], head_sem.at[n])
            for n, ref in enumerate(heads)
        ]
        for copy in tails:
            copy.start()
        acc_ref[...] = acc_in[...]
        fall_ref[...] = fall_in[...]
        ready(0)

        @pl.when(lax.axis_index("z") >= 4)
        def _():
            chunk(q_ref, up4, acc_ref, fall_ref, scr, False)

        for copy in tails:
            copy.wait()
        ready(1, 2, 3, 4, 5, 6)
        out_ref[:, BLOCK:] = (acc_ref[...] + jnp.exp2(-fall_ref[...]) * far_ref[...]).astype(bf16)

        def chunks(z):
            for n, k in enumerate((1, 2, 3)):
                yield head_ref[n], z + k >= 8
            yield up4[ROWS + EXTRA :, :], z >= 4
            for n, k in ((3, 3), (4, 2), (5, 1)):
                yield head_ref[n], z >= k

        out_ref[:, :BLOCK] = finish(chunks, y_ref, ef_ref, pow_ref, hop_ref, init_ref, ct_ref, g_ref)
        mine = lax.axis_index("y")
        for k, part in enumerate(parts):
            part[...] = out_ref[pl.ds(pl.multiple_of(((mine + k) % 4) * BLOCK, BLOCK), BLOCK), :]

    return staged(
        body,
        [],
        [ups[4], y, ef, power, hop, init, c_map, downs[1], downs[2], downs[3], ups[3], ups[2], ups[1]],
        [
            pltpu.VMEM((ROWS, 2 * BLOCK), bf16),
            pltpu.VMEM((ROWS, BLOCK), f32),
            pltpu.VMEM((ROWS, BLOCK), f32),
            pltpu.VMEM((ROWS, 2 * N), bf16),
            pltpu.VMEM((6, EXTRA, 256), bf16),
            pltpu.SemaphoreType.DMA((6,)),
        ]
        + ATTEND_SCRATCH,
        flops=2 * ATTEND_FLOPS,
        lazy=True,
        raw=range(7, 13),
        free=(0,) + tuple(range(7, 13)),
        vin=(q, acc, fall, far),
        vout=(shape((BLOCK, 2 * BLOCK), bf16),) * 4,
    )


N = 512


def cmul(ar, ai, br, bi):
    return ar * br - ai * bi, ar * bi + ai * br


def tables_body(
    in_ref, out_ref, lam_r_ref, lam_i_ref, step_ref, start_ref, skip_in,
    pow_ref, inv_ref, b_ref, ct_ref, init_ref, skip_ref,
):
    y = lax.axis_index("y")
    own = pl.ds(pl.multiple_of(y * 8, 8), 8)
    copy = (
        lax.broadcasted_iota(jnp.int32, (64, N), 1) % 64 == lax.broadcasted_iota(jnp.int32, (64, N), 0)
    ).astype(f32)

    def tiled(a, height):
        rows, width = a.shape
        r = lax.broadcasted_iota(jnp.int32, (rows, N), 0) // height
        k = lax.broadcasted_iota(jnp.int32, (rows, N), 1) // width
        spread = jnp.dot(a, copy, precision=lax.Precision.HIGHEST, preferred_element_type=f32)
        return jnp.where(r == k, spread, 0.0)

    def line(a):
        return jnp.sum(tiled(a, 1), axis=0, keepdims=True)

    lam_r, lam_i, step = line(lam_r_ref[own]), line(lam_i_ref[own]), jnp.exp(line(step_ref[own]))
    init_ref[0:1, :] = line(start_ref[0, 0, own])
    init_ref[1:2, :] = line(start_ref[1, 0, own])
    skip_ref[...] = skip_in[:, pl.ds(pl.multiple_of(y * BLOCK, BLOCK), BLOCK)]
    gain = lam_r * step
    turn = lam_i * step
    size = jnp.exp(gain)
    bar_r = size * jnp.cos(turn)
    bar_i = size * jnp.sin(turn)
    over = lam_r * lam_r + lam_i * lam_i
    less = bar_r - 1.0
    factor_r = (less * lam_r + bar_i * lam_i) / over
    factor_i = (bar_i * lam_r - less * lam_i) / over
    count = lax.broadcasted_iota(jnp.int32, (BLOCK, N), 0) + 1
    pr = jnp.ones((BLOCK, N), f32)
    pi = jnp.zeros((BLOCK, N), f32)
    sr, si = bar_r, bar_i
    for bit in range(8):
        on = ((count >> bit) & 1) == 1
        nr, ni = cmul(pr, pi, sr, si)
        pr, pi = jnp.where(on, nr, pr), jnp.where(on, ni, pi)
        if bit < 7:
            sr, si = cmul(sr, si, sr, si)
    back = jnp.exp(-2.0 * count.astype(f32) * gain)
    pow_ref[:BLOCK, :] = pr
    pow_ref[BLOCK:, :] = pi
    br, bi = cmul(pr * back, -pi * back, factor_r, factor_i)
    inv_ref[:BLOCK, :] = br
    inv_ref[BLOCK:, :] = bi
    for p in range(2):
        b_ref[:, p * N : (p + 1) * N] = tiled(in_ref[p, own].reshape(BLOCK, 64), 16).astype(bf16)
        sign = 1.0 if p == 0 else -1.0
        ct_ref[:, p * N : (p + 1) * N] = (sign * tiled(out_ref[p, own].reshape(BLOCK, 64), 16)).astype(bf16)


def scan_tables(*arrays):
    return staged(
        tables_body,
        (
            shape((2 * BLOCK, N), f32),
            shape((2 * BLOCK, N), f32),
            shape((BLOCK, 2 * N), bf16),
            shape((BLOCK, 2 * N), bf16),
            shape((2, N), f32),
            shape((1, BLOCK), f32),
        ),
        arrays,
        flops=10**9,
    )


DEEP = ROWS + 2 * EXTRA


def project_body(
    ready, send, mine, theirs, a0, a3, a1, a2, b0, b3, b1, b2, pow_ref, inv_ref, b_ref, ct_ref, skip_ref,
    kv_ref, y_ref, ef_ref, hop_ref, q_ref,
    rows, sems, more, u_ref, x_ref, st_ref, w_ref,
):
    c = lax.axis_index("c")
    x = lax.axis_index("x")
    copies = []
    arriving = []
    for n, (step, a_ref, b_ref2) in enumerate(((0, a0, b0), (3, a3, b3), (1, a1, b1), (2, a2, b2))):
        at = pl.multiple_of(((x + step) % 4) * ROWS, ROWS)
        pair = [
            pltpu.make_async_copy(ref, w_ref.at[n, :, pl.ds(256 * h, 256)], sems.at[12 + 2 * n + h])
            for h, ref in enumerate((a_ref, b_ref2))
        ]
        arriving.append((at, pair))
    for b in range(4):
        for part, ref in enumerate((mine, theirs)):
            at = pl.multiple_of(b * BLOCK + ((c + part) % 2) * 64, 64)
            copies.append(
                pltpu.make_async_copy(ref.at[b, pl.ds(0, 64)], rows.at[pl.ds(at, 64)], sems.at[2 * b + part])
            )
    for b in range(4):
        copies.append(
            pltpu.make_async_copy(mine.at[b, pl.ds(64, MORE)], more.at[b], sems.at[8 + b])
        )
    for copy in copies[-4:] + copies[:-4] + [copy for _, pair in arriving for copy in pair]:
        copy.start()
    for copy in copies[-4:]:
        copy.wait()
    offs = [more[b].astype(f32)[1:2, :BLOCK] for b in range(4)]
    row0 = jnp.concatenate(offs[:2], axis=1)
    row1 = jnp.concatenate(offs[2:], axis=1)
    tail = jnp.concatenate([row0, row1, jnp.zeros((EXTRA - 2, 256), f32)], axis=0)
    kv_ref[ROWS : ROWS + EXTRA, :] = tail.astype(bf16)
    row = lax.broadcasted_iota(jnp.int32, (BLOCK, BLOCK), 0)
    col = lax.broadcasted_iota(jnp.int32, (BLOCK, BLOCK), 1)
    low = (col <= row).astype(bf16)
    low32 = (col <= row).astype(f32)
    even = lax.broadcasted_iota(jnp.int32, (1, BLOCK), 1) < 64
    keeps = []
    blocks = [slice(b * BLOCK, (b + 1) * BLOCK) for b in range(4)]
    for b, at in enumerate(blocks):
        part = more[b].astype(f32)
        part = part[0:1, : 8 * BLOCK] + part[0:1, 8 * BLOCK :]
        f = jnp.concatenate([part[:, g * BLOCK : (g + 1) * BLOCK] for g in range(8)], axis=0)
        f_all = jnp.concatenate([jnp.broadcast_to(f[g : g + 1], (16, BLOCK)) for g in range(8)], axis=0)
        cum_f = lax.dot_general(
            low32, f_all, (((1,), (1,)), ((), ())), precision=lax.Precision.HIGHEST, preferred_element_type=f32
        )
        ef_ref[at, :] = jnp.exp(cum_f)
        x_ref[at, :BLOCK] = jnp.exp(-cum_f)
        total = jnp.exp(jnp.broadcast_to(jnp.sum(f, axis=1, keepdims=True), (8, BLOCK)))
        keeps.append(
            jnp.concatenate(
                [jnp.where(even, total[2 * g : 2 * g + 1], total[2 * g + 1 : 2 * g + 2]) for g in range(4)],
                axis=1,
            )
        )
    for copy in copies[:-4]:
        copy.wait()
    both = None
    for n, (at, pair) in enumerate(arriving):
        for copy in pair:
            copy.wait()
        part = mm(rows[:, pl.ds(at, ROWS)], w_ref[n])
        both = part if both is None else both + part
    kv_ref[:ROWS, :] = both[:, :256].astype(bf16)
    q_ref[...] = both[:, 256:384].astype(bf16)
    u_ref[...] = both[:, 384:].astype(bf16)
    x_ref[:, :BLOCK] = x_ref[:, :BLOCK] * u_ref[...].astype(f32)
    ready(10, 11, 12, 13, 14)
    x_ref[...] = mm(x_ref[:, :BLOCK].astype(bf16), b_ref[...])
    carry_r = jnp.zeros((1, N), f32)
    carry_i = jnp.zeros((1, N), f32)
    hop_r = jnp.ones((1, N), f32)
    hop_i = jnp.zeros((1, N), f32)
    end_r, end_i = pow_ref[BLOCK - 1 : BLOCK, :], pow_ref[2 * BLOCK - 1 :, :]
    hops = []
    for at, keep in zip(blocks, keeps):
        dr, di = cmul(x_ref[at, :N], x_ref[at, N:], inv_ref[:BLOCK, :], inv_ref[BLOCK:, :])
        tr = mm(low, dr.astype(bf16)) + carry_r
        ti = mm(low, di.astype(bf16)) + carry_i
        st_r, st_i = cmul(pow_ref[:BLOCK, :], pow_ref[BLOCK:, :], tr, ti)
        st_ref[at, :N] = st_r.astype(bf16)
        st_ref[at, N:] = st_i.astype(bf16)
        carry_r, carry_i = keep * st_r[BLOCK - 1 :, :], keep * st_i[BLOCK - 1 :, :]
        hops += [hop_r, hop_i]
        nr, ni = cmul(hop_r, hop_i, end_r, end_i)
        hop_r, hop_i = keep * nr, keep * ni
    hop_ref[...] = jnp.concatenate(hops, axis=0)
    hi, lo = split2(jnp.concatenate([carry_r, carry_i, hop_r, hop_i], axis=0))
    hi, lo = hi.astype(f32), lo.astype(f32)
    kv_ref[ROWS + EXTRA :, :] = jnp.concatenate(
        [hi[:, :256], hi[:, 256:], lo[:, :256], lo[:, 256:]], axis=0
    ).astype(bf16)
    send(0)
    y_ref[...] = ef_ref[...] * mm_t(st_ref[...], ct_ref[...]) + skip_ref[...] * u_ref[...].astype(f32)


def project(*arrays):
    return staged(
        project_body,
        (
            shape((DEEP, 256), bf16),
            shape((ROWS, BLOCK), f32),
            shape((ROWS, BLOCK), f32),
            shape((8, N), f32),
        ),
        arrays,
        [
            pltpu.VMEM((ROWS, 2048), bf16),
            pltpu.SemaphoreType.DMA((20,)),
            pltpu.VMEM((4, MORE, 2048), bf16),
            pltpu.VMEM((ROWS, BLOCK), bf16),
            pltpu.VMEM((ROWS, 2 * N), f32),
            pltpu.VMEM((ROWS, 2 * N), bf16),
            pltpu.VMEM((4, ROWS, ROWS), bf16),
        ],
        flops=3 * 10**9,
        lazy=True,
        raw=range(10),
        free=range(10),
        vout=(shape((ROWS, BLOCK), bf16),),
        limit=32,
    )


def finish(chunks, y_ref, ef_ref, pow_ref, hop_ref, init_ref, ct_ref, g_ref):
    z = lax.axis_index("z")
    sr, si = init_ref[0:1, :], init_ref[1:2, :]
    for ref, active in chunks(z):
        part = ref.astype(f32)
        part = part[:8] + part[8:]
        part = jnp.concatenate([part[:4], part[4:]], axis=1)
        nr, ni = cmul(part[2:3], part[3:4], sr, si)
        sr = jnp.where(active, nr + part[0:1], sr)
        si = jnp.where(active, ni + part[1:2], si)
    for b in range(ROWS // BLOCK):
        at = slice(b * BLOCK, (b + 1) * BLOCK)
        er, ei = cmul(hop_ref[2 * b : 2 * b + 1, :], hop_ref[2 * b + 1 : 2 * b + 2, :], sr, si)
        gr, gi = cmul(pow_ref[:BLOCK, :], pow_ref[BLOCK:, :], er, ei)
        g_ref[at, :N] = gr.astype(bf16)
        g_ref[at, N:] = gi.astype(bf16)
    v = y_ref[...] + ef_ref[...] * mm_t(g_ref[...], ct_ref[...])
    inner = math.sqrt(2.0 / math.pi) * (v + 0.044715 * v * v * v)
    return (0.5 * v * (1.0 + jnp.tanh(inner))).astype(bf16)


def out_body(
    a0, a3, a1, a2, b0, b1, b3, b2, r0, r3, r1, r2, send_ref, keep_ref, lhs_ref, sum_ref
):
    x, y, c = lax.axis_index("x"), lax.axis_index("y"), lax.axis_index("c")
    for step, ref in ((0, r0), (3, r3), (1, r1), (2, r2)):
        at = pl.multiple_of(((y + step) % 4) * BLOCK, BLOCK)
        lhs_ref[:, pl.ds(at, BLOCK)] = ref[:, :BLOCK]
        lhs_ref[:, pl.ds(ROWS + at, BLOCK)] = ref[:, BLOCK:]
    for step, scan_w, attend_w in ((0, a0, b0), (3, a3, b3), (1, a1, b1), (2, a2, b2)):
        total = mm(lhs_ref[:, :ROWS], scan_w[...]) + mm(lhs_ref[:, ROWS:], attend_w[...])
        sum_ref[:, pl.ds(pl.multiple_of(((x + step) % 4) * ROWS, ROWS), ROWS)] = total
    keep_ref[...] = sum_ref[pl.ds(pl.multiple_of(c * 64, 64), 64), :]
    send_ref[...] = sum_ref[pl.ds(pl.multiple_of((1 - c) * 64, 64), 64), :].astype(bf16)


def project_out(recv, pieces):
    return staged(
        out_body,
        [shape((64, 2048), bf16)],
        [],
        [pltpu.VMEM((BLOCK, 1024), bf16), pltpu.VMEM((BLOCK, 2048), f32)],
        flops=BLOCK * 1024 * 2048 * 2,
        vin=tuple(pieces) + tuple(recv),
        vout=(shape((64, 2048), f32),),
    )


def shift(a, axis, by):
    n = lax.axis_size(axis)
    return lax.ppermute(a, axis, [(i, (i + by) % n) for i in range(n)])


def after(a, b):
    return lax.optimization_barrier((a, b))[0]


def on_device(
    tokens,
    norm_gain,
    drive_weight,
    query_weight,
    key_weight,
    value_weight,
    key_offset,
    log_step,
    lambda_real,
    lambda_imag,
    input_map,
    output_map,
    skip_gain,
    forget,
    initial_state,
    scan_out_weight,
    attend_out_weight,
):
    def exchange(a, axis):
        return lax.all_to_all(a, axis, split_axis=0, concat_axis=0, tiled=True)

    normed, w_a, w_b = normalize(
        tokens,
        norm_gain,
        forget[:, 0, :],
        key_offset[:, 0, :],
        key_weight,
        value_weight,
        query_weight,
        drive_weight,
    )
    a_up = shift(w_a, "x", 1)
    b_down = shift(w_b, "x", -1)
    b_up = shift(w_b, "x", 1)
    a_down = shift(w_a, "x", -1)
    a_far = shift(a_up, "x", 1)
    b_far = shift(b_down, "x", -1)
    weights = (w_a, a_up, a_down, a_far, w_b, b_up, b_down, b_far)
    mine = exchange(normed, "y")
    theirs = shift(mine, "c", 1)
    wide = jnp.broadcast_to(log_step[:, None], lambda_real.shape)
    tables = scan_tables(
        input_map.transpose(0, 1, 3, 2),
        output_map,
        lambda_real,
        lambda_imag,
        wide,
        initial_state,
        skip_gain.reshape(1, -1),
    )
    theirs, tables = lax.optimization_barrier((theirs, tables))
    power, inverse, b_map, c_map, init, skip = tables
    kv, y_local, ef, hop, q = project(
        mine, theirs, *weights, power, inverse, b_map, c_map, skip
    )
    ups, downs = [kv], [kv]
    for k in range(1, 5):
        ups.append(shift(ups[-1], "z", 1))
        if k < 4:
            downs.append(shift(downs[-1], "z", -1))
    out_pieces = []
    for w, way in ((scan_out_weight, 1), (attend_out_weight, -1)):
        w = after(w, kv)
        first = shift(w, "x", way)
        second = shift(w, "x", -way)
        far_piece = shift(first, "x", way)
        out_pieces += [w, first, second, far_piece]
    acc, fall, far = attend_own(q, kv)
    for k in (1, 2, 3):
        acc, fall, far = attend_step(q, acc, fall, far, ups[k], downs[k], k)
    both = attend_last(q, acc, fall, far, ups, downs, y_local, ef, power, hop, init, c_map)
    got = [both[0]]
    for k in (1, 3, 2):
        got.append(shift(both[k], "y", k))
    send, keep = project_out(got, out_pieces)
    return (keep + shift(send, "c", 1).astype(f32)).astype(bf16)[None]


def solution(mesh):
    split = Mesh(
        mesh.devices.reshape(8, 4, mesh.shape["fs"], mesh.shape["tp"]), ("z", "y", "x", "c")
    )
    in_specs = (
        P("x", SP_TP, None),
        P(),
        P("x", "c"),
        P("x", "c"),
        P("x", "c"),
        P("x", "c"),
        P("c", "x", SP),
        P("c"),
        P("c", None),
        P("c", None),
        P(None, "c", None, None),
        P(None, "c", None, None),
        P("c"),
        P("c", "x", SP),
        P(None, "x", "c", None),
        P("c", "x"),
        P("c", "x"),
    )
    out_specs = P("x", SP_TP, None)

    return jax.shard_map(on_device, mesh=split, in_specs=in_specs, out_specs=out_specs, check_vma=False)
```

```python
import math

import jax
import jax.numpy as jnp
from jax import lax
from jax.experimental import pallas as pl
from jax.experimental.pallas import tpu as pltpu
from jax.sharding import Mesh
from jax.sharding import PartitionSpec as P


HEAD_DIM = 128
BLOCK = 128
ROWS = 512
EXTRA = 16
MORE = 8
SP = ("z", "y")
SP_TP = ("z", "y", "c")
LOG2E = 1.4426950408889634
SCORE = HEAD_DIM ** (-0.5) * LOG2E
epsilon = 1e-06
f32 = jnp.float32
bf16 = jnp.bfloat16
INTERPRET = False


def staged(body, outs, arrays, scratch=(), flops=0, limit=20, lazy=False, raw=(), free=(), vin=(), vout=(), alias=()):
    n, m = len(arrays), len(outs)
    kept = [i for i in range(n) if i not in raw]

    def kernel(*refs):
        nv, mv = len(vin), len(vout)
        src, near_in = refs[:n], refs[n : n + nv]
        refs = refs[n + nv :]
        dst, near_out = refs[:m], refs[m : m + mv]
        refs = refs[m + mv :]
        bufs = dict(zip(kept, refs[: len(kept)]))
        results = refs[len(kept) : len(kept) + m]
        sems, rest = refs[len(kept) + m], refs[len(kept) + m + 1 :]
        copies = {i: pltpu.make_async_copy(src[i], bufs[i], sems.at[i]) for i in kept}
        for i in kept:
            copies[i].start()
        leaving = {}

        def ready(*which):
            for i in which:
                copies[i].wait()

        def send(i):
            leaving[i] = pltpu.make_async_copy(results[i], dst[i], sems.at[n + i])
            leaving[i].start()

        ins = [bufs.get(i, src[i]) for i in range(n)]
        if lazy:
            body(ready, send, *ins, *near_in, *results, *near_out, *rest)
        else:
            ready(*kept)
            body(*ins, *near_in, *results, *near_out, *rest)
        for i in range(m):
            if i not in leaving:
                send(i)
        for i in range(m):
            leaving[i].wait()

    hbm = pl.BlockSpec(memory_space=pltpu.HBM)
    near = pl.BlockSpec(memory_space=pltpu.VMEM)
    got = pl.pallas_call(
        kernel,
        out_shape=tuple(pltpu.HBM(o.shape, o.dtype) for o in outs) + tuple(vout),
        in_specs=[hbm] * n + [near] * len(vin),
        out_specs=(hbm,) * m + (near,) * len(vout),
        input_output_aliases={n + i: m + o for i, o in alias},
        scratch_shapes=[pltpu.VMEM(arrays[i].shape, arrays[i].dtype) for i in kept]
        + [pltpu.VMEM(o.shape, o.dtype) for o in outs]
        + [pltpu.SemaphoreType.DMA((n + m,))]
        + list(scratch),
        cost_estimate=pl.CostEstimate(flops=flops, transcendentals=0, bytes_accessed=1 << 20),
        compiler_params=pltpu.CompilerParams(vmem_limit_bytes=limit << 20),
        interpret=INTERPRET,
    )(*(a if i in free else pltpu.with_memory_space_constraint(a, pltpu.HBM) for i, a in enumerate(arrays)), *vin)
    return got if len(got) > 1 else got[0]


def shape(dims, dtype):
    return jax.ShapeDtypeStruct(dims, dtype)


def split2(v):
    hi = v.astype(bf16)
    return hi, (v - hi.astype(f32)).astype(bf16)


def mm(a, b):
    return jnp.dot(a, b, preferred_element_type=f32)


def mm_t(a, b):
    return lax.dot_general(a, b, (((1,), (1,)), ((), ())), preferred_element_type=f32)


def norm_body(
    ready, send, tok_ref, gain_ref, forget_ref, off_ref, k_ref, v_ref, q_ref, d_ref, out_ref, a_ref, b_ref, sems
):
    at = pl.ds(pl.multiple_of(lax.axis_index("y") * BLOCK, BLOCK), BLOCK)
    copies = []
    for n, (ref, to, h) in enumerate(((k_ref, a_ref, 0), (v_ref, a_ref, 1), (q_ref, b_ref, 0), (d_ref, b_ref, 1))):
        copies.append(pltpu.make_async_copy(ref.at[:, at], to.at[:, pl.ds(h * BLOCK, BLOCK)], sems.at[n]))
    for copy in copies:
        copy.start()
    ready(0, 1, 2, 3)
    v = tok_ref[0].astype(f32)
    scale = lax.rsqrt(jnp.mean(v * v, axis=1, keepdims=True) + epsilon)
    normed = (v * scale * gain_ref[...]).astype(bf16)
    hi, lo = split2(forget_ref[...])
    hi, lo = hi.astype(f32), lo.astype(f32)
    off = off_ref[...].astype(f32)
    blank = jnp.zeros((6, BLOCK), f32)
    for k in range(4):
        out_ref[k, :64, :] = normed
        for j in range(16):
            row = hi[8 * k + j : 8 * k + j + 1] if j < 8 else lo[8 * k + j - 8 : 8 * k + j - 7]
            last = off[k : k + 1] if j == 0 else jnp.zeros((1, BLOCK), f32)
            tile = jnp.concatenate([row, last, blank], axis=0)
            out_ref[k, 64:, j * BLOCK : (j + 1) * BLOCK] = tile.astype(bf16)
    send(0)
    for copy in copies:
        copy.wait()


def normalize(tokens, gain, forget, offset, *weights):
    return staged(
        norm_body,
        [shape((4, 64 + MORE, 2048), bf16), shape((ROWS, 256), bf16), shape((ROWS, 256), bf16)],
        [tokens, gain.reshape(1, -1), forget, offset, *weights],
        [pltpu.SemaphoreType.DMA((4,))],
        flops=10**6,
        lazy=True,
        raw=(4, 5, 6, 7),
    )


SPAN = 256
TILE = 32
WIDE = SPAN + BLOCK


def chunk(q_ref, kv_ref, acc_ref, fall_ref, scr, diagonal):
    s_ref, soft_ref, r_ref, w_ref, tri_ref = scr
    j = lax.broadcasted_iota(jnp.int32, (SPAN, WIDE), 0)
    k = lax.broadcasted_iota(jnp.int32, (SPAN, WIDE), 1)
    tri_ref[...] = jnp.where((j > k) | (k >= SPAN), 1.0, 0.0).astype(bf16)
    offs = kv_ref[ROWS : ROWS + EXTRA, :].astype(f32)
    off = jnp.concatenate([offs[0:1], offs[1:2]], axis=1) * LOG2E
    s_ref[...] = mm_t(q_ref[...], kv_ref[:ROWS, :BLOCK])

    def visible(i):
        t = lax.broadcasted_iota(jnp.int32, (TILE, ROWS), 0) + i * TILE
        s = lax.broadcasted_iota(jnp.int32, (TILE, ROWS), 1)
        return s < t

    def first(i, _):
        at = pl.ds(pl.multiple_of(i * TILE, TILE), TILE)
        z = s_ref[at, :] * SCORE + off
        soft = jnp.maximum(z, 0.0) + jnp.log2(1.0 + jnp.exp2(-jnp.abs(z)))
        s_ref[at, :] = z - soft
        if diagonal:
            soft = jnp.where(visible(i), soft, 0.0)
        soft_ref[at, :] = soft.astype(bf16)
        return 0

    lax.fori_loop(0, ROWS // TILE, first, 0, unroll=2)
    for blk in range(2):
        r_ref[:, blk * WIDE : (blk + 1) * WIDE] = mm(
            soft_ref[:, blk * SPAN : (blk + 1) * SPAN], tri_ref[...]
        )

    def second(i, _):
        at = pl.ds(pl.multiple_of(i * TILE, TILE), TILE)
        fall1 = fall_ref[at, :]
        fall0 = fall1 + r_ref[at, WIDE + SPAN :]
        fall_ref[at, :] = fall0 + r_ref[at, SPAN:WIDE]
        behind = jnp.concatenate(
            [
                r_ref[at, :BLOCK] + fall0,
                r_ref[at, BLOCK:SPAN] + fall0,
                r_ref[at, WIDE : WIDE + BLOCK] + fall1,
                r_ref[at, WIDE + BLOCK : WIDE + SPAN] + fall1,
            ],
            axis=1,
        )
        w = jnp.exp2(s_ref[at, :] - behind)
        if diagonal:
            w = jnp.where(visible(i), w, 0.0)
        w_ref[at, :] = w.astype(bf16)
        return 0

    lax.fori_loop(0, ROWS // TILE, second, 0, unroll=2)
    acc_ref[...] += mm(w_ref[...], kv_ref[:ROWS, BLOCK:])


ATTEND_SCRATCH = [
    pltpu.VMEM((ROWS, ROWS), f32),
    pltpu.VMEM((ROWS, ROWS), bf16),
    pltpu.VMEM((ROWS, 2 * WIDE), f32),
    pltpu.VMEM((ROWS, ROWS), bf16),
    pltpu.VMEM((SPAN, WIDE), bf16),
]
PAIR = (shape((ROWS, BLOCK), f32), shape((ROWS, BLOCK), f32))
ATTEND_FLOPS = 8 * ROWS * ROWS * BLOCK


def zero(ref):
    ref[...] = jnp.zeros(ref.shape, ref.dtype)


def attend_own(q, kv):
    def body(kv_ref, q_ref, acc_ref, fall_ref, far_ref, *scr):
        zero(acc_ref)
        zero(fall_ref)
        zero(far_ref)
        chunk(q_ref, kv_ref, acc_ref, fall_ref, scr, True)

    return staged(body, (), [kv], ATTEND_SCRATCH, flops=ATTEND_FLOPS, vin=(q,), vout=PAIR + PAIR[:1])


def attend_step(q, acc, fall, far, up, down, k):
    def body(ready, send, up_ref, down_ref, q_ref, _a, _b, _c, acc_ref, fall_ref, far_ref, low_ref, part_ref, *scr):
        z = lax.axis_index("z")
        ready(0, 1)

        @pl.when(z >= k)
        def _():
            chunk(q_ref, up_ref, acc_ref, fall_ref, scr, False)

        @pl.when(z + k >= 8)
        def _():
            zero(low_ref)
            zero(part_ref)
            chunk(q_ref, down_ref, part_ref, low_ref, scr, False)
            far_ref[...] = part_ref[...] + jnp.exp2(-low_ref[...]) * far_ref[...]

    return staged(
        body,
        (),
        [up, down],
        [pltpu.VMEM((ROWS, BLOCK), f32)] * 2 + ATTEND_SCRATCH,
        flops=2 * ATTEND_FLOPS,
        lazy=True,
        free=(0, 1),
        vin=(q, acc, fall, far),
        vout=PAIR + PAIR[:1],
        alias=((1, 0), (2, 1), (3, 2)),
    )


def attend_last(q, acc, fall, far, ups, downs, y, ef, power, hop, init, c_map):
    def body(
        ready, send, up4, y_ref, ef_ref, pow_ref, hop_ref, init_ref, ct_ref, *refs,
    ):
        heads = refs[:6]
        refs = refs[6:]
        q_ref, acc_in, fall_in, far_ref, *parts = refs[:8]
        out_ref, acc_ref, fall_ref, g_ref, head_ref, head_sem = refs[8:14]
        scr = refs[14:]
        tails = [
            pltpu.make_async_copy(ref.at[pl.ds(ROWS + EXTRA, EXTRA)], head_ref.at[n], head_sem.at[n])
            for n, ref in enumerate(heads)
        ]
        for copy in tails:
            copy.start()
        acc_ref[...] = acc_in[...]
        fall_ref[...] = fall_in[...]
        ready(0)

        @pl.when(lax.axis_index("z") >= 4)
        def _():
            chunk(q_ref, up4, acc_ref, fall_ref, scr, False)

        for copy in tails:
            copy.wait()
        ready(1, 2, 3, 4, 5, 6)
        out_ref[:, BLOCK:] = (acc_ref[...] + jnp.exp2(-fall_ref[...]) * far_ref[...]).astype(bf16)

        def chunks(z):
            for n, k in enumerate((1, 2, 3)):
                yield head_ref[n], z + k >= 8
            yield up4[ROWS + EXTRA :, :], z >= 4
            for n, k in ((3, 3), (4, 2), (5, 1)):
                yield head_ref[n], z >= k

        out_ref[:, :BLOCK] = finish(chunks, y_ref, ef_ref, pow_ref, hop_ref, init_ref, ct_ref, g_ref)
        mine = lax.axis_index("y")
        for k, part in enumerate(parts):
            part[...] = out_ref[pl.ds(pl.multiple_of(((mine + k) % 4) * BLOCK, BLOCK), BLOCK), :]

    return staged(
        body,
        [],
        [ups[4], y, ef, power, hop, init, c_map, downs[1], downs[2], downs[3], ups[3], ups[2], ups[1]],
        [
            pltpu.VMEM((ROWS, 2 * BLOCK), bf16),
            pltpu.VMEM((ROWS, BLOCK), f32),
            pltpu.VMEM((ROWS, BLOCK), f32),
            pltpu.VMEM((ROWS, 2 * N), bf16),
            pltpu.VMEM((6, EXTRA, 256), bf16),
            pltpu.SemaphoreType.DMA((6,)),
        ]
        + ATTEND_SCRATCH,
        flops=2 * ATTEND_FLOPS,
        lazy=True,
        raw=range(7, 13),
        free=(0,) + tuple(range(7, 13)),
        vin=(q, acc, fall, far),
        vout=(shape((BLOCK, 2 * BLOCK), bf16),) * 4,
    )


N = 512


def cmul(ar, ai, br, bi):
    return ar * br - ai * bi, ar * bi + ai * br


def tables_body(
    in_ref, out_ref, lam_r_ref, lam_i_ref, step_ref, start_ref, skip_in,
    pow_ref, inv_ref, b_ref, ct_ref, init_ref, skip_ref,
):
    y = lax.axis_index("y")
    own = pl.ds(pl.multiple_of(y * 8, 8), 8)
    copy = (
        lax.broadcasted_iota(jnp.int32, (64, N), 1) % 64 == lax.broadcasted_iota(jnp.int32, (64, N), 0)
    ).astype(f32)

    def tiled(a, height):
        rows, width = a.shape
        r = lax.broadcasted_iota(jnp.int32, (rows, N), 0) // height
        k = lax.broadcasted_iota(jnp.int32, (rows, N), 1) // width
        spread = jnp.dot(a, copy, precision=lax.Precision.HIGHEST, preferred_element_type=f32)
        return jnp.where(r == k, spread, 0.0)

    def line(a):
        return jnp.sum(tiled(a, 1), axis=0, keepdims=True)

    lam_r, lam_i, step = line(lam_r_ref[own]), line(lam_i_ref[own]), jnp.exp(line(step_ref[own]))
    init_ref[0:1, :] = line(start_ref[0, 0, own])
    init_ref[1:2, :] = line(start_ref[1, 0, own])
    skip_ref[...] = skip_in[:, pl.ds(pl.multiple_of(y * BLOCK, BLOCK), BLOCK)]
    gain = lam_r * step
    turn = lam_i * step
    size = jnp.exp(gain)
    bar_r = size * jnp.cos(turn)
    bar_i = size * jnp.sin(turn)
    over = lam_r * lam_r + lam_i * lam_i
    less = bar_r - 1.0
    factor_r = (less * lam_r + bar_i * lam_i) / over
    factor_i = (bar_i * lam_r - less * lam_i) / over
    count = lax.broadcasted_iota(jnp.int32, (BLOCK, N), 0) + 1
    pr = jnp.ones((BLOCK, N), f32)
    pi = jnp.zeros((BLOCK, N), f32)
    sr, si = bar_r, bar_i
    for bit in range(8):
        on = ((count >> bit) & 1) == 1
        nr, ni = cmul(pr, pi, sr, si)
        pr, pi = jnp.where(on, nr, pr), jnp.where(on, ni, pi)
        if bit < 7:
            sr, si = cmul(sr, si, sr, si)
    back = jnp.exp(-2.0 * count.astype(f32) * gain)
    pow_ref[:BLOCK, :] = pr
    pow_ref[BLOCK:, :] = pi
    br, bi = cmul(pr * back, -pi * back, factor_r, factor_i)
    inv_ref[:BLOCK, :] = br
    inv_ref[BLOCK:, :] = bi
    for p in range(2):
        b_ref[:, p * N : (p + 1) * N] = tiled(in_ref[p, own].reshape(BLOCK, 64), 16).astype(bf16)
        sign = 1.0 if p == 0 else -1.0
        ct_ref[:, p * N : (p + 1) * N] = (sign * tiled(out_ref[p, own].reshape(BLOCK, 64), 16)).astype(bf16)


def scan_tables(*arrays):
    return staged(
        tables_body,
        (
            shape((2 * BLOCK, N), f32),
            shape((2 * BLOCK, N), f32),
            shape((BLOCK, 2 * N), bf16),
            shape((BLOCK, 2 * N), bf16),
            shape((2, N), f32),
            shape((1, BLOCK), f32),
        ),
        arrays,
        flops=10**9,
    )


DEEP = ROWS + 2 * EXTRA


def project_body(
    ready, send, mine, theirs, a0, a3, a1, a2, b0, b3, b1, b2, pow_ref, inv_ref, b_ref, ct_ref, skip_ref,
    kv_ref, y_ref, ef_ref, hop_ref, q_ref,
    rows, sems, more, u_ref, f_ref, x_ref, st_ref, w_ref,
):
    c = lax.axis_index("c")
    x = lax.axis_index("x")
    copies = []
    both = None
    for n, (step, ref) in enumerate(((0, a0), (3, a3), (1, a1), (2, a2), (0, b0), (3, b3), (1, b1), (2, b2))):
        at = pl.multiple_of(((x + step) % 4) * ROWS, ROWS)
        to = w_ref.at[pl.ds(at, ROWS), pl.ds(256 * (n // 4), 256)]
        copies.append(pltpu.make_async_copy(ref, to, sems.at[12 + n]))
    for b in range(4):
        for part, ref in enumerate((mine, theirs)):
            at = pl.multiple_of(b * BLOCK + ((c + part) % 2) * 64, 64)
            copies.append(
                pltpu.make_async_copy(ref.at[b, pl.ds(0, 64)], rows.at[pl.ds(at, 64)], sems.at[2 * b + part])
            )
    for b in range(4):
        copies.append(
            pltpu.make_async_copy(mine.at[b, pl.ds(64, MORE)], more.at[b], sems.at[8 + b])
        )
    for copy in copies:
        copy.start()
    for copy in copies:
        copy.wait()
    both = mm(rows[...], w_ref[...])
    kv_ref[:ROWS, :] = both[:, :256].astype(bf16)
    q_ref[...] = both[:, 256:384].astype(bf16)
    u_ref[...] = both[:, 384:].astype(bf16)
    offs = [more[b].astype(f32)[1:2, :BLOCK] for b in range(4)]
    row0 = jnp.concatenate(offs[:2], axis=1)
    row1 = jnp.concatenate(offs[2:], axis=1)
    tail = jnp.concatenate([row0, row1, jnp.zeros((EXTRA - 2, 256), f32)], axis=0)
    kv_ref[ROWS : ROWS + EXTRA, :] = tail.astype(bf16)
    for b in range(4):
        part = more[b].astype(f32)
        part = part[0:1, : 8 * BLOCK] + part[0:1, 8 * BLOCK :]
        f_ref[:, b * BLOCK : (b + 1) * BLOCK] = jnp.concatenate(
            [part[:, g * BLOCK : (g + 1) * BLOCK] for g in range(8)], axis=0
        )
    ready(10, 11, 12, 13, 14)
    row = lax.broadcasted_iota(jnp.int32, (BLOCK, BLOCK), 0)
    col = lax.broadcasted_iota(jnp.int32, (BLOCK, BLOCK), 1)
    low = (col <= row).astype(bf16)
    low32 = (col <= row).astype(f32)
    even = lax.broadcasted_iota(jnp.int32, (1, BLOCK), 1) < 64
    keeps = []
    blocks = [slice(b * BLOCK, (b + 1) * BLOCK) for b in range(4)]
    for at in blocks:
        f = f_ref[:, at]
        f_all = jnp.concatenate([jnp.broadcast_to(f[g : g + 1], (16, BLOCK)) for g in range(8)], axis=0)
        cum_f = lax.dot_general(
            low32, f_all, (((1,), (1,)), ((), ())), precision=lax.Precision.HIGHEST, preferred_element_type=f32
        )
        ef_ref[at, :] = jnp.exp(cum_f)
        x_ref[at, :BLOCK] = u_ref[at, :].astype(f32) * jnp.exp(-cum_f)
        total = jnp.exp(jnp.broadcast_to(jnp.sum(f, axis=1, keepdims=True), (8, BLOCK)))
        keeps.append(
            jnp.concatenate(
                [jnp.where(even, total[2 * g : 2 * g + 1], total[2 * g + 1 : 2 * g + 2]) for g in range(4)],
                axis=1,
            )
        )
    x_ref[...] = mm(x_ref[:, :BLOCK].astype(bf16), b_ref[...])
    carry_r = jnp.zeros((1, N), f32)
    carry_i = jnp.zeros((1, N), f32)
    hop_r = jnp.ones((1, N), f32)
    hop_i = jnp.zeros((1, N), f32)
    end_r, end_i = pow_ref[BLOCK - 1 : BLOCK, :], pow_ref[2 * BLOCK - 1 :, :]
    hops = []
    for at, keep in zip(blocks, keeps):
        dr, di = cmul(x_ref[at, :N], x_ref[at, N:], inv_ref[:BLOCK, :], inv_ref[BLOCK:, :])
        tr = mm(low, dr.astype(bf16)) + carry_r
        ti = mm(low, di.astype(bf16)) + carry_i
        st_r, st_i = cmul(pow_ref[:BLOCK, :], pow_ref[BLOCK:, :], tr, ti)
        st_ref[at, :N] = st_r.astype(bf16)
        st_ref[at, N:] = st_i.astype(bf16)
        carry_r, carry_i = keep * st_r[BLOCK - 1 :, :], keep * st_i[BLOCK - 1 :, :]
        hops += [hop_r, hop_i]
        nr, ni = cmul(hop_r, hop_i, end_r, end_i)
        hop_r, hop_i = keep * nr, keep * ni
    hop_ref[...] = jnp.concatenate(hops, axis=0)
    hi, lo = split2(jnp.concatenate([carry_r, carry_i, hop_r, hop_i], axis=0))
    hi, lo = hi.astype(f32), lo.astype(f32)
    kv_ref[ROWS + EXTRA :, :] = jnp.concatenate(
        [hi[:, :256], hi[:, 256:], lo[:, :256], lo[:, 256:]], axis=0
    ).astype(bf16)
    send(0)
    y_ref[...] = ef_ref[...] * mm_t(st_ref[...], ct_ref[...]) + skip_ref[...] * u_ref[...].astype(f32)


def project(*arrays):
    return staged(
        project_body,
        (
            shape((DEEP, 256), bf16),
            shape((ROWS, BLOCK), f32),
            shape((ROWS, BLOCK), f32),
            shape((8, N), f32),
        ),
        arrays,
        [
            pltpu.VMEM((ROWS, 2048), bf16),
            pltpu.SemaphoreType.DMA((20,)),
            pltpu.VMEM((4, MORE, 2048), bf16),
            pltpu.VMEM((ROWS, BLOCK), bf16),
            pltpu.VMEM((8, ROWS), f32),
            pltpu.VMEM((ROWS, 2 * N), f32),
            pltpu.VMEM((ROWS, 2 * N), bf16),
            pltpu.VMEM((2048, ROWS), bf16),
        ],
        flops=3 * 10**9,
        lazy=True,
        raw=range(10),
        free=range(10),
        vout=(shape((ROWS, BLOCK), bf16),),
        limit=32,
    )


def finish(chunks, y_ref, ef_ref, pow_ref, hop_ref, init_ref, ct_ref, g_ref):
    z = lax.axis_index("z")
    sr, si = init_ref[0:1, :], init_ref[1:2, :]
    for ref, active in chunks(z):
        part = ref.astype(f32)
        part = part[:8] + part[8:]
        part = jnp.concatenate([part[:4], part[4:]], axis=1)
        nr, ni = cmul(part[2:3], part[3:4], sr, si)
        sr = jnp.where(active, nr + part[0:1], sr)
        si = jnp.where(active, ni + part[1:2], si)
    for b in range(ROWS // BLOCK):
        at = slice(b * BLOCK, (b + 1) * BLOCK)
        er, ei = cmul(hop_ref[2 * b : 2 * b + 1, :], hop_ref[2 * b + 1 : 2 * b + 2, :], sr, si)
        gr, gi = cmul(pow_ref[:BLOCK, :], pow_ref[BLOCK:, :], er, ei)
        g_ref[at, :N] = gr.astype(bf16)
        g_ref[at, N:] = gi.astype(bf16)
    v = y_ref[...] + ef_ref[...] * mm_t(g_ref[...], ct_ref[...])
    inner = math.sqrt(2.0 / math.pi) * (v + 0.044715 * v * v * v)
    return (0.5 * v * (1.0 + jnp.tanh(inner))).astype(bf16)


def out_body(
    a0, a3, a1, a2, b0, b1, b3, b2, r0, r3, r1, r2, send_ref, keep_ref, lhs_ref, sum_ref
):
    x, y, c = lax.axis_index("x"), lax.axis_index("y"), lax.axis_index("c")
    for step, ref in ((0, r0), (3, r3), (1, r1), (2, r2)):
        at = pl.multiple_of(((y + step) % 4) * BLOCK, BLOCK)
        lhs_ref[:, pl.ds(at, BLOCK)] = ref[:, :BLOCK]
        lhs_ref[:, pl.ds(ROWS + at, BLOCK)] = ref[:, BLOCK:]
    for step, scan_w, attend_w in ((0, a0, b0), (3, a3, b3), (1, a1, b1), (2, a2, b2)):
        total = mm(lhs_ref[:, :ROWS], scan_w[...]) + mm(lhs_ref[:, ROWS:], attend_w[...])
        sum_ref[:, pl.ds(pl.multiple_of(((x + step) % 4) * ROWS, ROWS), ROWS)] = total
    keep_ref[...] = sum_ref[pl.ds(pl.multiple_of(c * 64, 64), 64), :]
    send_ref[...] = sum_ref[pl.ds(pl.multiple_of((1 - c) * 64, 64), 64), :].astype(bf16)


def project_out(recv, pieces):
    return staged(
        out_body,
        [shape((64, 2048), bf16)],
        [],
        [pltpu.VMEM((BLOCK, 1024), bf16), pltpu.VMEM((BLOCK, 2048), f32)],
        flops=BLOCK * 1024 * 2048 * 2,
        vin=tuple(pieces) + tuple(recv),
        vout=(shape((64, 2048), f32),),
    )


def shift(a, axis, by):
    n = lax.axis_size(axis)
    return lax.ppermute(a, axis, [(i, (i + by) % n) for i in range(n)])


def after(a, b):
    return lax.optimization_barrier((a, b))[0]


def on_device(
    tokens,
    norm_gain,
    drive_weight,
    query_weight,
    key_weight,
    value_weight,
    key_offset,
    log_step,
    lambda_real,
    lambda_imag,
    input_map,
    output_map,
    skip_gain,
    forget,
    initial_state,
    scan_out_weight,
    attend_out_weight,
):
    def exchange(a, axis):
        return lax.all_to_all(a, axis, split_axis=0, concat_axis=0, tiled=True)

    normed, w_a, w_b = normalize(
        tokens,
        norm_gain,
        forget[:, 0, :],
        key_offset[:, 0, :],
        key_weight,
        value_weight,
        query_weight,
        drive_weight,
    )
    a_up = shift(w_a, "x", 1)
    b_down = shift(w_b, "x", -1)
    b_up = shift(w_b, "x", 1)
    a_down = shift(w_a, "x", -1)
    a_far = shift(a_up, "x", 1)
    b_far = shift(b_down, "x", -1)
    weights = (w_a, a_up, a_down, a_far, w_b, b_up, b_down, b_far)
    mine = exchange(normed, "y")
    theirs = shift(mine, "c", 1)
    wide = jnp.broadcast_to(log_step[:, None], lambda_real.shape)
    tables = scan_tables(
        input_map.transpose(0, 1, 3, 2),
        output_map,
        lambda_real,
        lambda_imag,
        wide,
        initial_state,
        skip_gain.reshape(1, -1),
    )
    theirs, tables = lax.optimization_barrier((theirs, tables))
    power, inverse, b_map, c_map, init, skip = tables
    kv, y_local, ef, hop, q = project(
        mine, theirs, *weights, power, inverse, b_map, c_map, skip
    )
    ups, downs = [kv], [kv]
    for k in range(1, 5):
        ups.append(shift(ups[-1], "z", 1))
        if k < 4:
            downs.append(shift(downs[-1], "z", -1))
    out_pieces = []
    for w, way in ((scan_out_weight, 1), (attend_out_weight, -1)):
        w = after(w, kv)
        first = shift(w, "x", way)
        second = shift(w, "x", -way)
        far_piece = shift(first, "x", way)
        out_pieces += [w, first, second, far_piece]
    acc, fall, far = attend_own(q, kv)
    for k in (1, 2, 3):
        acc, fall, far = attend_step(q, acc, fall, far, ups[k], downs[k], k)
    both = attend_last(q, acc, fall, far, ups, downs, y_local, ef, power, hop, init, c_map)
    got = [both[0]]
    for k in (1, 3, 2):
        got.append(shift(both[k], "y", k))
    send, keep = project_out(got, out_pieces)
    return (keep + shift(send, "c", 1).astype(f32)).astype(bf16)[None]


def solution(mesh):
    split = Mesh(
        mesh.devices.reshape(8, 4, mesh.shape["fs"], mesh.shape["tp"]), ("z", "y", "x", "c")
    )
    in_specs = (
        P("x", SP_TP, None),
        P(),
        P("x", "c"),
        P("x", "c"),
        P("x", "c"),
        P("x", "c"),
        P("c", "x", SP),
        P("c"),
        P("c", None),
        P("c", None),
        P(None, "c", None, None),
        P(None, "c", None, None),
        P("c"),
        P("c", "x", SP),
        P(None, "x", "c", None),
        P("c", "x"),
        P("c", "x"),
    )
    out_specs = P("x", SP_TP, None)

    return jax.shard_map(on_device, mesh=split, in_specs=in_specs, out_specs=out_specs, check_vma=False)
```
